512 devices in a mesh: sp: 32 (over z, core), tp: 16 (over y, x).
Axes of the slice: x: 4, y: 4, z: 16, core: 2. Of those that a mesh axis runs over, the one named last changes fastest.
Arguments:
- moe_input: bfloat16 [10240, 2048], P('sp', 'tp'), may hold values from -6 to 6
- out_cotangent: bfloat16 [10240, 2048], P('sp', 'tp'), may hold values from -0.59765625 to 0.59765625
- routes: int32 [10240, 2], P('sp'), may hold values from 0 to 31, all different within a row; in each aligned block of 320 rows (0 to 319, 320 to 639, ...) at most 30 rows name the same one
- route_weight: float32 [10240, 2], P('sp'), may hold values from 0.1 to 0.9
- gate_weight: bfloat16 [32, 1024, 2048], P('sp', 'tp'), may hold values from -0.125 to 0.125
- up_weight: bfloat16 [32, 1024, 2048], P('sp', 'tp'), may hold values from -0.125 to 0.125
- down_weight: bfloat16 [32, 1024, 2048], P('sp', 'tp'), may hold values from -0.1875 to 0.1875
- glu_value: bfloat16 [10240, 1024], P('sp', 'tp'), may hold values from -6 to 6
- glu_gate: bfloat16 [10240, 1024], P('sp', 'tp'), may hold values from -8 to 8
- conv_result: bfloat16 [10240, 1024], P('sp', 'tp'), may hold values from -12 to 12
- conv_taps: float32 [31, 1024], P(None, 'tp'), may hold values from -1 to 1
- norm_gain: float32 [1024], P('tp'), may hold values from 0.1 to 1.9
- proj_weight: bfloat16 [1024, 2048], P('tp'), may hold values from -0.1875 to 0.1875
Outputs:
- grad_gate: float32 [32, 1024, 2048], P('sp', 'tp')
- grad_up: float32 [32, 1024, 2048], P('sp', 'tp')
- grad_down: float32 [32, 1024, 2048], P('sp', 'tp')
- grad_proj: float32 [2048, 1024], P('sp', 'tp')
- grad_value: bfloat16 [10240, 1024], P('sp', 'tp')
- grad_glu_gate: bfloat16 [10240, 1024], P('sp', 'tp')
The draws below stay inside these ranges and needn't reach their ends.
Inputs may be any that keep to these rules, and one draw needn't show every extreme that they name: `routes`: each row names two different experts. In the aligned blocks of 320 rows (the rows of one index of sp) no expert is named by more than 30 rows, and that bound is reached.
All inputs are finite; a program needn't handle non-finite values.
Results may differ from the reference program's by a relative error of at most 0.025.
Values may be sent and summed in bfloat16 or wider, within the bound.
No kernel may reach another device: no remote copies, remote signals or barrier semaphores. Data moves between devices by JAX's collectives and lax.ppermute only.
A program may use at most 64 MiB of HBM per device.

```python
import math
import jax
import jax.numpy as jnp
import numpy as np
from jax import lax

D = 2048
C = 1024
F = 1024
K = 31
TOK_DEV = 320
TOKENS = 10240
EXPERTS = 32
CAP = 30
SLOTS = 960
FT = 64
N_SP = 32
N_TP = 16


def draw_conv_result(key, part):
    first, second, third = jax.random.split(key, 3)
    position = jnp.arange(C, dtype=jnp.float32) / C
    chan_scale = (0.5 + 2.5 * position) * jax.random.uniform(first, (C,), jnp.float32, 0.7, 1.4)
    offset = jax.random.uniform(second, (C,), jnp.float32, -1.0, 1.0)
    base = jax.random.normal(third, (TOKENS, C), jnp.float32)
    values = base * chan_scale[None, :] + offset[None, :]
    return jnp.clip(values, -12.0, 12.0).astype(jnp.bfloat16)


def raised(values, rng, source, target, parts, factor):
    def block_of(dim):
        return (jnp.arange(values.shape[dim]) // (values.shape[dim] // parts)).reshape((-1,) + (1,) * (values.ndim - 1 - dim))

    one_side = jax.random.permutation(rng, parts)[block_of(target)]
    second = (block_of(target) + parts // 2) % parts
    return jnp.where((block_of(source) == one_side) | (block_of(source) == second), factor * values, values)


def level_of(key, dims, cuts, least, high):
    loudness = 1.0
    for dim, blocks in cuts:
        steps = jax.random.uniform(jax.random.fold_in(jax.random.fold_in(key, 6), dim), (blocks,), jnp.float32, least / len(cuts), high / len(cuts))
        loudness = loudness * jnp.repeat(jnp.exp(steps), dims[dim] // blocks).reshape((-1,) + (1,) * (len(dims) - 1 - dim))
    return loudness


def assign_block(stream_key, own, number, rows, number_of, top, reach, skew):
    ranking = jax.random.permutation(stream_key, number_of)
    crowded, common = load_shares(number_of, rows * top, reach, skew, True), load_shares(number_of, rows * top, reach, skew, False)
    places = jnp.arange(number_of)

    def named(sizes, rotation):
        used = int((sizes > 0).sum())
        fixed = max(1, used // 4)
        passed = fixed + (places - fixed + rotation * (used - fixed)) % max(1, number_of - fixed)
        return jnp.zeros((number_of,), jnp.int32).at[ranking[jnp.where(places < fixed, places, passed)]].set(jnp.asarray(sizes, jnp.int32))

    sizes = jnp.where(number % 4 == 0, named(crowded, number // 4), named(common, number - number // 4 - 1))
    mixed = jax.random.permutation(jax.random.fold_in(own, 3), number_of)
    source_of, sink = mixed[0:number_of // 2 * 2:2], mixed[1:number_of // 2 * 2:2]
    room = jnp.minimum(sizes[source_of] - 1, reach - sizes[sink]) // 2
    room = jnp.where((source_of == ranking[0]) | (sink == ranking[0]) | (sizes[sink] == 0), 0, jnp.maximum(room, 0))
    passed = jax.random.randint(jax.random.fold_in(own, 4), (number_of // 2,), 0, 1 << 20) % (room + 1)
    sizes = sizes.at[source_of].add(-passed).at[sink].add(passed)
    labels = jnp.searchsorted(jnp.cumsum(sizes), jnp.arange(rows * top), side="right").astype(jnp.int32)
    grid = labels.reshape(top, rows).T
    grid = grid[jax.random.permutation(jax.random.fold_in(own, 1), rows)]
    rotation = jax.random.randint(jax.random.fold_in(own, 2), (rows, 1), 0, top)
    return jnp.take_along_axis(grid, (jnp.arange(top)[None, :] + rotation) % top, axis=1)


def load_shares(count, total, most, slope, full):
    weights = [(1 << 20) // math.isqrt(standing ** slope) + 1 for standing in range(1, count + 1)]
    largest = most if full else min(most, max(-(-total // count), total * weights[0] // sum(weights)))
    least = 1 if total - largest >= count - 1 else 0
    counts, surplus = [largest] + [least] * (count - 1), total - largest - least * (count - 1)
    while surplus > 0:
        free = [i for i in range(1, count) if counts[i] < largest] or [i for i in range(1, count) if counts[i] < most]
        whole, remaining = sum([weights[i] for i in free]), surplus
        for i in free:
            extra = min(most - counts[i], max(1, remaining * weights[i] // whole), surplus)
            counts[i] = counts[i] + extra
            surplus = surplus - extra
    return np.array(counts)


def noise(key, shape, deviation, reach, shards=(), kind=jnp.bfloat16):
    level = level_of(key, shape, shards, -0.22, 0.18) if shards else 1.0
    values = jax.random.normal(key, shape, jnp.float32) * deviation * level
    return jnp.minimum(jnp.maximum(values, -reach), reach).astype(kind)


def heavy_noise(key, shape, width, bound, cuts, heavy, kind=jnp.bfloat16):
    values = width * jax.random.normal(key, shape, jnp.float32)
    if cuts:
        values = values * level_of(key, shape, cuts, -0.22, 0.18)
    return jnp.clip(raised(values, jax.random.fold_in(key, 3), *heavy), -bound, bound).astype(kind)


def setup_inputs(seed: int = 0) -> dict:
    arg_keys = jax.random.split(jax.random.key(seed), 14)
    moe_input = noise(arg_keys[0], (TOKENS, D), 1.0, 6.0, ((0, 32), (1, 16)))
    out_cotangent = heavy_noise(arg_keys[1], (TOKENS, D), 0.1, 0.59765625, ((0, 32), (1, 16)), (0, 1, 32, 2.75))
    routes_keys = jax.random.split(jax.random.fold_in(arg_keys[2], 1), TOKENS // TOK_DEV)
    routes_turns = jax.random.permutation(jax.random.fold_in(arg_keys[2], 3), TOKENS // TOK_DEV)
    routes = jax.vmap(lambda own, number: assign_block(jax.random.fold_in(arg_keys[2], 2), own, number, TOK_DEV, EXPERTS, 2, CAP, 2))(routes_keys, routes_turns).reshape((TOKENS, 2))
    route_weight = jnp.clip(0.1 + 0.79999997 * jax.random.uniform(arg_keys[3], (TOKENS, 2), jnp.float32) ** level_of(arg_keys[3], (TOKENS, 2), ((0, 32),), -0.2, 0.2), 0.1, 0.9)
    gate_weight = noise(arg_keys[4], (EXPERTS, F, D), D ** -0.5, 0.125, ((0, 32), (1, 16)))
    up_weight = noise(arg_keys[5], (EXPERTS, F, D), D ** -0.5, 0.125, ((0, 32), (1, 16)))
    down_weight = noise(arg_keys[6], (EXPERTS, F, D), F ** -0.5, 0.1875, ((0, 32), (1, 16)))
    glu_value = noise(arg_keys[7], (TOKENS, C), 1.0, 6.0, ((0, 32), (1, 16)))
    glu_gate = noise(arg_keys[8], (TOKENS, C), 1.5, 8.0, ((0, 32), (1, 16)))
    conv_result = draw_conv_result(jax.random.fold_in(arg_keys[13], 71), 0)
    conv_taps = noise(arg_keys[10], (K, C), K ** -0.5, 1.0, ((1, 16),), jnp.float32)
    norm_gain = jnp.clip(1.0 + 0.18 * jax.random.normal(arg_keys[11], (C,), jnp.float32), 0.1, 1.9)
    proj_weight = noise(arg_keys[12], (C, D), C ** -0.5, 0.1875, ((0, 16),))
    return {"moe_input": moe_input, "out_cotangent": out_cotangent, "routes": routes, "route_weight": route_weight, "gate_weight": gate_weight, "up_weight": up_weight, "down_weight": down_weight, "glu_value": glu_value, "glu_gate": glu_gate, "conv_result": conv_result, "conv_taps": conv_taps, "norm_gain": norm_gain, "proj_weight": proj_weight}


NORM_EPS = 0.25

def pair_places(routes):
    blocks = routes.reshape(N_SP, TOK_DEV * 2).astype(jnp.int32)
    onehot = (blocks[:, :, None] == jnp.arange(EXPERTS, dtype=jnp.int32)[None, None, :]).astype(jnp.int32)
    earlier = jnp.cumsum(onehot, axis=1) - onehot
    slot_rank = lax.optimization_barrier(jnp.sum(earlier * onehot, axis=2))
    source = jnp.arange(N_SP, dtype=jnp.int32)[:, None]
    places = (source * CAP + slot_rank).reshape(-1).astype(jnp.int32)
    return (routes.reshape(-1).astype(jnp.int32), places)

def contract_rows(left, right):
    return lax.dot_general(left, right, (((0,), (0,)), ((), ())), preferred_element_type=jnp.float32)

def contract_cols(left, right):
    return lax.dot_general(left, right, (((1,), (1,)), ((), ())), preferred_element_type=jnp.float32)

def expert_backward(packed):
    token_rows, cot_rows, gate_matrix, up_matrix, down_matrix = packed
    gate_pre = contract_cols(token_rows, gate_matrix)
    up_pre = contract_cols(token_rows, up_matrix)
    gate_sigmoid = jax.nn.sigmoid(gate_pre)
    activation = gate_pre * gate_sigmoid
    hidden = (activation * up_pre).astype(jnp.bfloat16)
    grad_down = contract_rows(hidden, cot_rows)
    hidden_cot = contract_cols(cot_rows, down_matrix)
    up_cot = (hidden_cot * activation).astype(jnp.bfloat16)
    gate_cot = (hidden_cot * up_pre * gate_sigmoid * (1.0 + gate_pre * (1.0 - gate_sigmoid))).astype(jnp.bfloat16)
    grad_gate = contract_rows(gate_cot, token_rows)
    grad_up = contract_rows(up_cot, token_rows)
    gate_blocks = gate_cot.astype(jnp.float32).reshape(SLOTS, N_TP, FT)
    up_blocks = up_cot.astype(jnp.float32).reshape(SLOTS, N_TP, FT)
    gate_wblocks = gate_matrix.astype(jnp.float32).reshape(N_TP, FT, D)
    up_wblocks = up_matrix.astype(jnp.float32).reshape(N_TP, FT, D)
    partial_value = jnp.einsum('rtf,tfd->trd', gate_blocks, gate_wblocks) + jnp.einsum('rtf,tfd->trd', up_blocks, up_wblocks)
    rounded = lax.optimization_barrier(partial_value.astype(jnp.bfloat16))
    returned = lax.optimization_barrier(jnp.sum(rounded.astype(jnp.float32), axis=0)).astype(jnp.bfloat16)
    return (grad_gate, grad_up, grad_down, returned)

def reference(moe_input, out_cotangent, routes, route_weight, gate_weight, up_weight, down_weight, glu_value, glu_gate, conv_result, conv_taps, norm_gain, proj_weight):
    expert_ids, places = pair_places(routes)
    pair_rows = jnp.repeat(moe_input, 2, axis=0)
    scaled = (route_weight.reshape(-1, 1) * jnp.repeat(out_cotangent, 2, axis=0).astype(jnp.float32)).astype(jnp.bfloat16)
    expert_rows = jnp.zeros((EXPERTS, SLOTS, D), jnp.bfloat16).at[expert_ids, places].set(pair_rows)
    expert_cot = jnp.zeros((EXPERTS, SLOTS, D), jnp.bfloat16).at[expert_ids, places].set(scaled)
    grad_gate, grad_up, grad_down, returned = lax.map(expert_backward, (expert_rows, expert_cot, gate_weight, up_weight, down_weight))
    picked = returned[expert_ids, places].astype(jnp.float32)
    moe_grad = lax.optimization_barrier(jnp.sum(picked.reshape(TOKENS, 2, D), axis=1))
    total_cot = (out_cotangent.astype(jnp.float32) + moe_grad).astype(jnp.bfloat16)
    conv_values = conv_result.astype(jnp.float32)
    row_mean = lax.optimization_barrier(jnp.mean(conv_values, axis=1, keepdims=True))
    centered = conv_values - row_mean
    inv_scale = lax.rsqrt(lax.optimization_barrier(jnp.mean(centered * centered, axis=1, keepdims=True)) + NORM_EPS)
    normed = centered * inv_scale
    linear = normed * norm_gain[None, :]
    lin_sigmoid = jax.nn.sigmoid(linear)
    act_out = (linear * lin_sigmoid).astype(jnp.bfloat16)
    grad_proj = contract_rows(total_cot, act_out)
    act_cot = contract_cols(total_cot, proj_weight)
    norm_cot = act_cot * lin_sigmoid * (1.0 + linear * (1.0 - lin_sigmoid)) * norm_gain[None, :]
    conv_cot = inv_scale * (norm_cot - lax.optimization_barrier(jnp.mean(norm_cot, axis=1, keepdims=True)) - normed * lax.optimization_barrier(jnp.mean(norm_cot * normed, axis=1, keepdims=True)))
    padded = jnp.pad(conv_cot, ((0, K - 1), (0, 0)))
    glu_cot = lax.conv_general_dilated(padded[None], jnp.flip(conv_taps, 0)[:, None, :], (1,), 'VALID', dimension_numbers=('NWC', 'WIO', 'NWC'), feature_group_count=C, precision=lax.Precision.HIGHEST)[0]
    gate_sigmoid = jax.nn.sigmoid(glu_gate.astype(jnp.float32))
    grad_value = (glu_cot * gate_sigmoid).astype(jnp.bfloat16)
    grad_glu_gate = (glu_cot * glu_value.astype(jnp.float32) * gate_sigmoid * (1.0 - gate_sigmoid)).astype(jnp.bfloat16)
    return (grad_gate, grad_up, grad_down, grad_proj, grad_value, grad_glu_gate)
```

```python
import jax
import jax.numpy as jnp
from jax import lax
from jax.experimental import pallas as pl
from jax.experimental.pallas import tpu as pltpu
from jax.sharding import Mesh
from jax.sharding import PartitionSpec as P

NORM_EPS = 0.25
SP = ("z", "c")
TP = ("y", "x")
PLANE = ("c", "y", "x")
SIDE = 4
SLOT = 32
BF = jnp.bfloat16
F32 = jnp.float32
VM = pltpu.VMEM

NT = (((1,), (1,)), ((), ()))
TN = (((0,), (0,)), ((), ()))
NN = (((1,), (0,)), ((), ()))


def place(core, row, col):
    return core * SIDE * SIDE + row * SIDE + col


def plane_groups():
    r = range(SIDE)
    down = [[[place(k, y, x) for y in r] for x in r] for k in (0, 1)]
    across = [[[place(k, y, x) for x in r] for y in r] for k in (0, 1)]
    return down[0] + across[1], across[0] + down[1]


def mm(a, b, dims):
    return lax.dot_general(a, b, dims, preferred_element_type=F32)


def exchange(v, groups):
    return lax.all_to_all(v, PLANE, 0, 0, axis_index_groups=groups, tiled=True)


def cost(flops, nbytes):
    return pl.CostEstimate(flops=flops, bytes_accessed=nbytes, transcendentals=0)


def route_kernel(rt_ref, w_ref, x_ref, c_ref, s_ref, p_ref):
    tokens = rt_ref.shape[1]
    experts = s_ref.shape[0] // SLOT
    first, second = rt_ref[0:1, :], rt_ref[1:2, :]
    ids = lax.broadcasted_iota(jnp.int32, (experts, tokens), 0)
    o0, o1 = ids == first, ids == second
    both = jnp.where(o0 | o1, 1.0, 0.0).astype(BF)
    before = lax.broadcasted_iota(jnp.int32, (tokens, tokens), 0) < lax.broadcasted_iota(
        jnp.int32, (tokens, tokens), 1
    )
    earlier = mm(both, jnp.where(before, 1.0, 0.0).astype(BF), NN)
    rank0 = jnp.sum(jnp.where(o0, earlier, 0.0), axis=0, keepdims=True)
    rank1 = jnp.sum(jnp.where(o1, earlier, 0.0), axis=0, keepdims=True)
    t0 = first * SLOT + rank0.astype(jnp.int32)
    t1 = second * SLOT + rank1.astype(jnp.int32)
    w0, w1 = w_ref[0:1, :], w_ref[1:2, :]
    x, c = x_ref[...], c_ref[...]
    size = 128
    for k in range(s_ref.shape[0] // size):
        slots = lax.broadcasted_iota(jnp.int32, (size, tokens), 0) + k * size
        m0, m1 = slots == t0, slots == t1
        pick = jnp.where(m0 | m1, 1.0, 0.0).astype(BF)
        weight = jnp.sum(
            jnp.where(m0, w0, 0.0) + jnp.where(m1, w1, 0.0), axis=1, keepdims=True
        )
        rows = pl.ds(k * size, size)
        p_ref[rows, :] = pick
        s_ref[rows, 0:128] = mm(pick, x, NN).astype(BF)
        s_ref[rows, 128:256] = (weight * mm(pick, c, NN)).astype(BF)


def split_kernel(core_ref, g_ref, u_ref, d_ref, o_ref):
    core = core_ref[0]
    for b in range(SIDE):
        for a in range(SIDE):
            at = jnp.where(core == 0, a * SIDE + b, b * SIDE + a)
            cols = pl.ds(pl.multiple_of(at * 128, 128), 128)
            for q, ref in enumerate((g_ref, u_ref, d_ref)):
                o_ref[b, q * 64 : q * 64 + 64, a * 128 : a * 128 + 128] = ref[:, cols]


def merge_kernel(core_ref, s_ref, g_ref, u_ref, d_ref):
    core = core_ref[0]
    for b in range(SIDE):
        for a in range(SIDE):
            at = jnp.where(core == 0, a * SIDE + b, b * SIDE + a)
            cols = pl.ds(pl.multiple_of(at * 128, 128), 128)
            for q, ref in enumerate((g_ref, u_ref, d_ref)):
                ref[:, cols] = s_ref[
                    b, q * 64 : q * 64 + 64, a * 128 : a * 128 + 128
                ].astype(F32)


def pre_kernel(a_ref, w_ref, o_ref):
    x = jnp.concatenate([a_ref[i, :, 0:128] for i in range(SIDE)], axis=1)
    c = jnp.concatenate([a_ref[i, :, 128:256] for i in range(SIDE)], axis=1)
    for b in range(SIDE):
        o_ref[b, 0:128, :] = mm(w_ref[b, 0:128, :], x, NT).astype(BF)
        o_ref[b, 128:192, :] = mm(w_ref[b, 128:192, :], c, NT).astype(BF)


def gate_kernel(p_ref, o_ref):
    total = p_ref[0].astype(F32)
    for b in range(1, SIDE):
        total = total + p_ref[b].astype(F32)
    gate, up, cot = total[0:64], total[64:128], total[128:192]
    s = jax.nn.sigmoid(gate)
    act = gate * s
    hidden = (act * up).astype(BF)
    up_cot = (cot * act).astype(BF)
    gate_cot = (cot * up * s * (1.0 + gate * (1.0 - s))).astype(BF)
    for b in range(SIDE):
        o_ref[b, 0:64, :] = gate_cot
        o_ref[b, 64:128, :] = up_cot
        o_ref[b, 128:192, :] = hidden


def partial_kernel(h_ref, w_ref, o_ref):
    h = jnp.concatenate([h_ref[b, 0:128, :] for b in range(SIDE)], axis=0)
    w = jnp.concatenate([w_ref[b, 0:128, :] for b in range(SIDE)], axis=0)
    total = mm(h, w, TN)
    for a in range(SIDE):
        o_ref[a] = total[:, a * 128 : a * 128 + 128].astype(BF)


def grads_kernel(h_ref, a_ref, o_ref):
    x, c = a_ref[0, :, 0:128], a_ref[0, :, 128:256]
    for b in range(SIDE):
        o_ref[b, 0:128, :] = mm(h_ref[b, 0:128, :], x, NN).astype(BF)
        o_ref[b, 128:192, :] = mm(h_ref[b, 128:192, :], c, NN).astype(BF)


def combine_kernel(p_ref, r_ref, c_ref, o_ref):
    moe = mm(p_ref[...], r_ref[...], TN)
    total = (c_ref[...].astype(F32) + moe).astype(BF)
    for b in range(o_ref.shape[0]):
        o_ref[b] = total


def normed_of(conv, sums, channels):
    mean = sums[0:1, :] / channels
    var = sums[1:2, :] / channels - mean * mean
    inv = lax.rsqrt(var + NORM_EPS)
    return (conv.astype(F32) - mean) * inv, inv


def proj_kernel(f_ref, conv_ref, sums_ref, gain_ref, o_ref):
    channels = 16 * conv_ref.shape[0]
    normed, _ = normed_of(conv_ref[...], sums_ref[...], channels)
    linear = normed * gain_ref[...]
    act = (linear * jax.nn.sigmoid(linear)).astype(BF)
    low = lax.broadcasted_iota(jnp.int32, (32, 128), 1) < 64
    for b in range(f_ref.shape[0]):
        g = mm(act, f_ref[b], NN)
        turned = pltpu.roll(g, 64, 1)
        o_ref[2 * b] = jnp.where(low, g[0:32], turned[32:64]).astype(BF)
        o_ref[2 * b + 1] = jnp.where(low, turned[0:32], g[32:64]).astype(BF)


def norm_kernel(f_ref, proj_ref, conv_ref, sums_ref, gain_ref, n_ref, t_ref):
    channels = 16 * conv_ref.shape[0]
    total = mm(proj_ref[:, 0:128], f_ref[0], NT)
    for b in range(1, f_ref.shape[0]):
        total = total + mm(proj_ref[:, b * 128 : b * 128 + 128], f_ref[b], NT)
    normed, _ = normed_of(conv_ref[...], sums_ref[...], channels)
    gain = gain_ref[...]
    linear = normed * gain
    s = jax.nn.sigmoid(linear)
    cot = total * s * (1.0 + linear * (1.0 - s)) * gain
    n_ref[...] = cot
    t_ref[0:1, :] = jnp.sum(cot, axis=0, keepdims=True)
    t_ref[1:2, :] = jnp.sum(cot * normed, axis=0, keepdims=True)


def head_kernel(n_ref, t_ref, conv_ref, sums_ref, o_ref, h_ref):
    channels = 16 * conv_ref.shape[0]
    normed, inv = normed_of(conv_ref[...], sums_ref[...], channels)
    t = t_ref[...]
    cot = inv * (n_ref[...] - t[0:1, :] / channels - normed * (t[1:2, :] / channels))
    o_ref[...] = cot
    h_ref[...] = cot[:, 0:128]


def conv_kernel(cot_ref, next_ref, taps_ref, gate_ref, value_ref, v_ref, g_ref, buf):
    rows, tokens = cot_ref.shape
    wide = buf.shape[1]
    reach = taps_ref.shape[1] - 1
    buf[:, 0:128] = next_ref[...]
    buf[:, 128:wide] = jnp.zeros((rows, wide - 128), F32)
    after = pltpu.roll(buf[...], tokens, 1)
    buf[:, 0:tokens] = cot_ref[...]
    lane = lax.broadcasted_iota(jnp.int32, (rows, wide), 1)
    whole = jnp.where(lane < tokens, buf[...], after)
    taps = taps_ref[...]
    total = whole * taps[:, reach : reach + 1]
    for s in range(1, reach + 1):
        total = total + pltpu.roll(whole, wide - s, 1) * taps[:, reach - s : reach - s + 1]
    cot = total[:, 0:tokens]
    s = jax.nn.sigmoid(gate_ref[...].astype(F32))
    v_ref[...] = (cot * s).astype(BF)
    g_ref[...] = (cot * value_ref[...].astype(F32) * s * (1.0 - s)).astype(BF)


def whole(shape, dtype):
    return jax.ShapeDtypeStruct(shape, dtype)


def body(
    moe_input,
    out_cotangent,
    routes,
    route_weight,
    gate_weight,
    up_weight,
    down_weight,
    glu_value,
    glu_gate,
    conv_result,
    conv_taps,
    norm_gain,
    proj_weight,
):
    sp_count = lax.axis_size(SP)
    tp_count = lax.axis_size(TP)
    tokens = moe_input.shape[0]
    slots = sp_count * SLOT
    feature_groups, unit_groups = plane_groups()
    core = lax.axis_index("c").reshape(1).astype(jnp.int32)
    smem = pl.BlockSpec(memory_space=pltpu.SMEM)
    vmem = pl.BlockSpec(memory_space=VM)

    split = pl.pallas_call(
        split_kernel,
        out_shape=whole((SIDE, 192, 512), BF),
        in_specs=[smem, vmem, vmem, vmem],
        out_specs=vmem,
        cost_estimate=cost(1000000, 1600000),
        name="split_weights",
    )(core, gate_weight[0], up_weight[0], down_weight[0])
    weights = exchange(split, unit_groups)

    sent, pick = pl.pallas_call(
        route_kernel,
        out_shape=(whole((slots, 256), BF), whole((slots, tokens), BF)),
        in_specs=[vmem] * 4,
        out_specs=(vmem, vmem),
        cost_estimate=cost(400000000, 2000000),
        name="route",
    )(routes.T, route_weight.T, moe_input, out_cotangent)
    weights, sent = lax.optimization_barrier((weights, sent))
    got = lax.all_to_all(sent.reshape(sp_count, SLOT, 256), SP, 0, 0, tiled=True)
    got = got.reshape(slots, 256)

    conv_t = conv_result.T
    conv_f = conv_t.astype(F32)
    sums = jnp.stack([jnp.sum(conv_f, axis=0), jnp.sum(conv_f * conv_f, axis=0)])
    sums = lax.psum(lax.psum(sums, "y"), "x")
    got, sums = lax.optimization_barrier((got, sums))
    gain = norm_gain.reshape(-1, 1)
    taps_t = conv_taps.T

    rows = exchange(jnp.broadcast_to(got[None], (SIDE, slots, 256)), feature_groups)
    step = 256
    pre = pl.pallas_call(
        pre_kernel,
        grid=(slots // step,),
        out_shape=whole((SIDE, 192, slots), BF),
        in_specs=[
            pl.BlockSpec((SIDE, step, 256), lambda i: (0, i, 0)),
            pl.BlockSpec((SIDE, 192, 512), lambda i: (0, 0, 0)),
        ],
        out_specs=pl.BlockSpec((SIDE, 192, step), lambda i: (0, 0, i)),
        cost_estimate=cost(800000000, 4400000),
        name="pre",
    )(rows, weights)
    pre = exchange(pre, unit_groups)
    hidden = pl.pallas_call(
        gate_kernel,
        grid=(slots // step,),
        out_shape=whole((SIDE, 192, slots), BF),
        in_specs=[pl.BlockSpec((SIDE, 192, step), lambda i: (0, 0, i))],
        out_specs=pl.BlockSpec((SIDE, 192, step), lambda i: (0, 0, i)),
        cost_estimate=cost(3000000, 3200000),
        name="gates",
    )(pre)
    hidden = exchange(hidden, unit_groups)
    part = pl.pallas_call(
        partial_kernel,
        grid=(slots // step,),
        out_shape=whole((SIDE, slots, 128), BF),
        in_specs=[
            pl.BlockSpec((SIDE, 192, step), lambda i: (0, 0, i)),
            pl.BlockSpec((SIDE, 192, 512), lambda i: (0, 0, 0)),
        ],
        out_specs=pl.BlockSpec((SIDE, step, 128), lambda i: (0, i, 0)),
        cost_estimate=cost(540000000, 3400000),
        name="partial",
    )(hidden, weights)
    part = exchange(part, feature_groups)
    back = jnp.sum(part.astype(F32), axis=0).astype(BF).reshape(sp_count, SLOT, 128)
    returned = lax.all_to_all(back, SP, 0, 0, tiled=True).reshape(slots, 128)

    grads = pl.pallas_call(
        grads_kernel,
        grid=(SIDE,),
        out_shape=whole((SIDE, 192, 512), BF),
        in_specs=[
            pl.BlockSpec((SIDE, 192, slots), lambda i: (0, 0, 0)),
            pl.BlockSpec((1, slots, 256), lambda i: (i, 0, 0)),
        ],
        out_specs=pl.BlockSpec((SIDE, 192, 128), lambda i: (0, 0, i)),
        cost_estimate=cost(800000000, 4400000),
        name="grads",
    )(hidden, rows)

    spread = pl.pallas_call(
        combine_kernel,
        out_shape=whole((tp_count, tokens, 128), BF),
        in_specs=[vmem] * 3,
        out_specs=vmem,
        cost_estimate=cost(80000000, 2500000),
        name="combine",
    )(pick, returned, out_cotangent)
    full = lax.all_to_all(spread, TP, 0, 0, tiled=True)

    proj_part = pl.pallas_call(
        proj_kernel,
        out_shape=whole((sp_count, 32, 128), BF),
        in_specs=[vmem] * 4,
        out_specs=vmem,
        cost_estimate=cost(84000000, 1600000),
        name="proj_grad",
    )(full, conv_t, sums, gain)
    norm_cot, cot_sums = pl.pallas_call(
        norm_kernel,
        out_shape=(whole((64, tokens), F32), whole((2, tokens), F32)),
        in_specs=[vmem] * 5,
        out_specs=(vmem, vmem),
        cost_estimate=cost(84000000, 1600000),
        name="norm_cot",
    )(full, proj_weight, conv_t, sums, gain)
    proj_part = lax.all_to_all(proj_part, SP, 0, 0, tiled=True)
    grads = exchange(grads, unit_groups)

    cot_sums = lax.psum(lax.psum(cot_sums, "y"), "x")
    conv_cot, head = pl.pallas_call(
        head_kernel,
        out_shape=(whole((64, tokens), F32), whole((64, 128), F32)),
        in_specs=[vmem] * 4,
        out_specs=(vmem, vmem),
        cost_estimate=cost(1000000, 200000),
        name="conv_cot",
    )(norm_cot, cot_sums, conv_t, sums)
    behind = [(i + 1, i) for i in range(sp_count - 1)]
    after = lax.ppermute(head, SP, behind)
    value, gate = pl.pallas_call(
        conv_kernel,
        out_shape=(whole((64, tokens), BF), whole((64, tokens), BF)),
        in_specs=[vmem] * 5,
        out_specs=(vmem, vmem),
        scratch_shapes=[VM((64, 384), F32)],
        cost_estimate=cost(4000000, 400000),
        name="conv",
    )(conv_cot, after, taps_t, glu_gate.T, glu_value.T)

    total = jnp.sum(proj_part.astype(F32), axis=0)
    grad_proj = jnp.concatenate([total[:, 0:64], total[:, 64:128]], axis=0).T

    grad_gate, grad_up, grad_down = pl.pallas_call(
        merge_kernel,
        out_shape=(whole((64, 2048), F32),) * 3,
        in_specs=[smem, vmem],
        out_specs=(vmem,) * 3,
        cost_estimate=cost(1000000, 2400000),
        name="merge_grads",
    )(core, grads)
    return (
        grad_gate[None],
        grad_up[None],
        grad_down[None],
        grad_proj,
        value.T,
        gate.T,
    )


def solution(mesh):
    split = Mesh(mesh.devices.reshape(16, 2, SIDE, SIDE), ("z", "c", "y", "x"))
    placed = (
        P(SP, TP),
        P(SP, TP),
        P(SP, None),
        P(SP, None),
        P(SP, TP, None),
        P(SP, TP, None),
        P(SP, TP, None),
        P(SP, TP),
        P(SP, TP),
        P(SP, TP),
        P(None, TP),
        P(TP),
        P(TP, None),
    )
    return jax.shard_map(
        body,
        mesh=split,
        in_specs=placed,
        out_specs=(
            P(SP, TP, None),
            P(SP, TP, None),
            P(SP, TP, None),
            P(SP, TP),
            P(SP, TP),
            P(SP, TP),
        ),
        check_vma=False,
    )
```

```python
import jax
import jax.numpy as jnp
import numpy as np
from jax import lax
from jax.experimental import pallas as pl
from jax.experimental.pallas import tpu as pltpu
from jax.sharding import Mesh
from jax.sharding import PartitionSpec as P

NORM_EPS = 0.25
SP = ("z", "c")
TP = ("y", "x")
PLANE = ("c", "y", "x")
SIDE = 4
SLOT = 32
ROOM = 24 << 20
BF = jnp.bfloat16
F32 = jnp.float32
VM = pltpu.VMEM

NT = (((1,), (1,)), ((), ()))
TN = (((0,), (0,)), ((), ()))
NN = (((1,), (0,)), ((), ()))


def place(core, row, col):
    return core * SIDE * SIDE + row * SIDE + col


def plane_groups():
    r = range(SIDE)
    down = [[[place(k, y, x) for y in r] for x in r] for k in (0, 1)]
    across = [[[place(k, y, x) for x in r] for y in r] for k in (0, 1)]
    return down[0] + across[1], across[0] + down[1]


def step_tables():
    features, units = plane_groups()
    of_features = {p: g for g in features for p in g}
    table = np.zeros((2 * SIDE * SIDE, 64), np.int32)
    for group in units:
        for me, p in enumerate(group):
            table[p, 0] = me
            for k in range(SIDE):
                ahead = of_features[group[(me + k) % SIDE]]
                back = of_features[group[(me - k) % SIDE]]
                for a in range(SIDE):
                    table[p, 16 + k * SIDE + a] = ahead[a] % (SIDE * SIDE)
                    table[p, 32 + k * SIDE + a] = back[a] % (SIDE * SIDE)
    return table


def steps_ahead(groups, k):
    return [(g[i], g[(i + k) % SIDE]) for g in groups for i in range(SIDE)]


def pass_on(parts, groups):
    return (parts[0],) + tuple(
        lax.ppermute(parts[k], PLANE, steps_ahead(groups, k)) for k in range(1, SIDE)
    )


def mm(a, b, dims):
    return lax.dot_general(a, b, dims, preferred_element_type=F32)


def exchange(v, groups):
    return lax.all_to_all(v, PLANE, 0, 0, axis_index_groups=groups, tiled=True)


def cost(flops, nbytes):
    return pl.CostEstimate(flops=flops, bytes_accessed=nbytes, transcendentals=0)


def route_kernel(rt_ref, w_ref, x_ref, c_ref, s_ref, t_ref):
    tokens = rt_ref.shape[1]
    experts = s_ref.shape[0] // SLOT
    first, second = rt_ref[0:1, :], rt_ref[1:2, :]
    ids = lax.broadcasted_iota(jnp.int32, (experts, tokens), 0)
    o0, o1 = ids == first, ids == second
    both = jnp.where(o0 | o1, 1.0, 0.0).astype(BF)
    before = lax.broadcasted_iota(jnp.int32, (tokens, tokens), 0) < lax.broadcasted_iota(
        jnp.int32, (tokens, tokens), 1
    )
    earlier = mm(both, jnp.where(before, 1.0, 0.0).astype(BF), NN)
    rank0 = jnp.sum(jnp.where(o0, earlier, 0.0), axis=0, keepdims=True)
    rank1 = jnp.sum(jnp.where(o1, earlier, 0.0), axis=0, keepdims=True)
    t0 = first * SLOT + rank0.astype(jnp.int32)
    t1 = second * SLOT + rank1.astype(jnp.int32)
    t_ref[0:1, :] = t0
    t_ref[1:2, :] = t1
    w0, w1 = w_ref[0:1, :], w_ref[1:2, :]
    x, c = x_ref[...], c_ref[...]
    size = 128
    for k in range(s_ref.shape[0] // size):
        slots = lax.broadcasted_iota(jnp.int32, (size, tokens), 0) + k * size
        m0, m1 = slots == t0, slots == t1
        pick = jnp.where(m0 | m1, 1.0, 0.0).astype(BF)
        weight = jnp.sum(
            jnp.where(m0, w0, 0.0) + jnp.where(m1, w1, 0.0), axis=1, keepdims=True
        )
        rows = pl.ds(k * size, size)
        s_ref[rows, 0:128] = mm(pick, x, NN).astype(BF)
        s_ref[rows, 128:256] = (weight * mm(pick, c, NN)).astype(BF)


def pick_kernel(t_ref, p_ref):
    slots = lax.broadcasted_iota(jnp.int32, p_ref.shape, 0)
    held = (slots == t_ref[0:1, :]) | (slots == t_ref[1:2, :])
    p_ref[...] = jnp.where(held, 1.0, 0.0).astype(BF)


def split_kernel(at_ref, g_ref, u_ref, d_ref, *outs):
    for k, out in enumerate(outs):
        for a in range(SIDE):
            at = at_ref[16 + k * SIDE + a]
            cols = pl.ds(pl.multiple_of(at * 128, 128), 128)
            for q, ref in enumerate((g_ref, u_ref, d_ref)):
                out[q * 64 : q * 64 + 64, a * 128 : a * 128 + 128] = ref[:, cols]


def merge_kernel(at_ref, s0, s1, s2, s3, g_ref, u_ref, d_ref):
    for k, s_ref in enumerate((s0, s1, s2, s3)):
        for a in range(SIDE):
            at = at_ref[32 + k * SIDE + a]
            cols = pl.ds(pl.multiple_of(at * 128, 128), 128)
            for q, ref in enumerate((g_ref, u_ref, d_ref)):
                ref[:, cols] = s_ref[
                    q * 64 : q * 64 + 64, a * 128 : a * 128 + 128
                ].astype(F32)


def behind_of(at_ref, k):
    return lax.rem(at_ref[0] + (SIDE - k), SIDE)


def ahead_of(at_ref, k):
    return lax.rem(at_ref[0] + k, SIDE)


def pre_kernel(at_ref, a_ref, w0, w1, w2, w3, o_ref):
    x = jnp.concatenate([a_ref[i, :, 0:128] for i in range(SIDE)], axis=1)
    c = jnp.concatenate([a_ref[i, :, 128:256] for i in range(SIDE)], axis=1)
    for k, w_ref in enumerate((w0, w1, w2, w3)):
        b = behind_of(at_ref, k)
        o_ref[b, 0:128, :] = mm(w_ref[0:128, :], x, NT).astype(BF)
        o_ref[b, 128:192, :] = mm(w_ref[128:192, :], c, NT).astype(BF)


def gate_kernel(p_ref, o_ref):
    total = p_ref[0].astype(F32)
    for b in range(1, SIDE):
        total = total + p_ref[b].astype(F32)
    gate, up, cot = total[0:64], total[64:128], total[128:192]
    s = jax.nn.sigmoid(gate)
    act = gate * s
    hidden = (act * up).astype(BF)
    up_cot = (cot * act).astype(BF)
    gate_cot = (cot * up * s * (1.0 + gate * (1.0 - s))).astype(BF)
    for b in range(SIDE):
        o_ref[b, 0:64, :] = gate_cot
        o_ref[b, 64:128, :] = up_cot
        o_ref[b, 128:192, :] = hidden


def partial_kernel(at_ref, h_ref, w0, w1, w2, w3, o_ref):
    ws = (w0, w1, w2, w3)
    h = jnp.concatenate([h_ref[behind_of(at_ref, k), 0:128, :] for k in range(SIDE)], axis=0)
    w = jnp.concatenate([w_ref[0:128, :] for w_ref in ws], axis=0)
    total = mm(h, w, TN)
    for a in range(SIDE):
        o_ref[a] = total[:, a * 128 : a * 128 + 128].astype(BF)


def grads_kernel(at_ref, h_ref, a_ref, *outs):
    x, c = a_ref[0, :, 0:128], a_ref[0, :, 128:256]
    for k, out in enumerate(outs):
        b = ahead_of(at_ref, k)
        out[0:128, :] = mm(h_ref[b, 0:128, :], x, NN).astype(BF)
        out[128:192, :] = mm(h_ref[b, 128:192, :], c, NN).astype(BF)


def combine_kernel(p_ref, r_ref, c_ref, o_ref):
    moe = mm(p_ref[...], r_ref[...], TN)
    total = (c_ref[...].astype(F32) + moe).astype(BF)
    for b in range(o_ref.shape[0]):
        o_ref[b] = total


def normed_of(conv, sums, channels):
    mean = sums[0:1, :] / channels
    var = sums[1:2, :] / channels - mean * mean
    inv = lax.rsqrt(var + NORM_EPS)
    return (conv.astype(F32) - mean) * inv, inv


def proj_kernel(f_ref, conv_ref, sums_ref, gain_ref, o_ref):
    channels = 16 * conv_ref.shape[0]
    normed, _ = normed_of(conv_ref[...], sums_ref[...], channels)
    linear = normed * gain_ref[...]
    act = (linear * jax.nn.sigmoid(linear)).astype(BF)
    low = lax.broadcasted_iota(jnp.int32, (32, 128), 1) < 64
    for b in range(f_ref.shape[0]):
        g = mm(act, f_ref[b], NN)
        turned = pltpu.roll(g, 64, 1)
        o_ref[2 * b] = jnp.where(low, g[0:32], turned[32:64]).astype(BF)
        o_ref[2 * b + 1] = jnp.where(low, turned[0:32], g[32:64]).astype(BF)


def norm_kernel(f_ref, proj_ref, conv_ref, sums_ref, gain_ref, n_ref, t_ref):
    channels = 16 * conv_ref.shape[0]
    total = mm(proj_ref[:, 0:128], f_ref[0], NT)
    for b in range(1, f_ref.shape[0]):
        total = total + mm(proj_ref[:, b * 128 : b * 128 + 128], f_ref[b], NT)
    normed, _ = normed_of(conv_ref[...], sums_ref[...], channels)
    gain = gain_ref[...]
    linear = normed * gain
    s = jax.nn.sigmoid(linear)
    cot = total * s * (1.0 + linear * (1.0 - s)) * gain
    n_ref[...] = cot
    t_ref[0:1, :] = jnp.sum(cot, axis=0, keepdims=True)
    t_ref[1:2, :] = jnp.sum(cot * normed, axis=0, keepdims=True)


def head_kernel(n_ref, t_ref, conv_ref, sums_ref, o_ref, h_ref):
    channels = 16 * conv_ref.shape[0]
    normed, inv = normed_of(conv_ref[...], sums_ref[...], channels)
    t = t_ref[...]
    cot = inv * (n_ref[...] - t[0:1, :] / channels - normed * (t[1:2, :] / channels))
    o_ref[...] = cot
    h_ref[...] = cot[:, 0:128]


def conv_kernel(cot_ref, next_ref, taps_ref, gate_ref, value_ref, v_ref, g_ref, buf):
    rows, tokens = cot_ref.shape
    wide = buf.shape[1]
    reach = taps_ref.shape[1] - 1
    buf[:, 0:128] = next_ref[...]
    buf[:, 128:wide] = jnp.zeros((rows, wide - 128), F32)
    after = pltpu.roll(buf[...], tokens, 1)
    buf[:, 0:tokens] = cot_ref[...]
    lane = lax.broadcasted_iota(jnp.int32, (rows, wide), 1)
    whole = jnp.where(lane < tokens, buf[...], after)
    taps = taps_ref[...]
    total = whole * taps[:, reach : reach + 1]
    for s in range(1, reach + 1):
        total = total + pltpu.roll(whole, wide - s, 1) * taps[:, reach - s : reach - s + 1]
    cot = total[:, 0:tokens]
    s = jax.nn.sigmoid(gate_ref[...].astype(F32))
    v_ref[...] = (cot * s).astype(BF)
    g_ref[...] = (cot * value_ref[...].astype(F32) * s * (1.0 - s)).astype(BF)


def whole(shape, dtype):
    return jax.ShapeDtypeStruct(shape, dtype)


def body(
    moe_input,
    out_cotangent,
    routes,
    route_weight,
    gate_weight,
    up_weight,
    down_weight,
    glu_value,
    glu_gate,
    conv_result,
    conv_taps,
    norm_gain,
    proj_weight,
):
    sp_count = lax.axis_size(SP)
    tp_count = lax.axis_size(TP)
    tokens = moe_input.shape[0]
    slots = sp_count * SLOT
    feature_groups, unit_groups = plane_groups()
    smem = pl.BlockSpec(memory_space=pltpu.SMEM)
    vmem = pl.BlockSpec(memory_space=VM)
    room = pltpu.CompilerParams(vmem_limit_bytes=ROOM)

    sent, target = pl.pallas_call(
        route_kernel,
        out_shape=(whole((slots, 256), BF), whole((2, tokens), jnp.int32)),
        in_specs=[vmem] * 4,
        out_specs=(vmem, vmem),
        cost_estimate=cost(400000000, 2000000),
        name="route",
    )(routes.T, route_weight.T, moe_input, out_cotangent)
    sent, target, table, gate_weight, conv_result = lax.optimization_barrier(
        (sent, target, jnp.asarray(step_tables()), gate_weight, conv_result)
    )
    at = table[lax.axis_index(PLANE)]
    pick = pl.pallas_call(
        pick_kernel,
        out_shape=whole((slots, tokens), BF),
        in_specs=[vmem],
        out_specs=vmem,
        compiler_params=room,
        cost_estimate=cost(1000000, 700000),
        name="pick",
    )(target)
    split = pl.pallas_call(
        split_kernel,
        out_shape=(whole((192, 512), BF),) * SIDE,
        in_specs=[smem, vmem, vmem, vmem],
        out_specs=(vmem,) * SIDE,
        compiler_params=room,
        cost_estimate=cost(1000000, 1600000),
        name="split_weights",
    )(at, gate_weight[0], up_weight[0], down_weight[0])
    weights = pass_on(split, unit_groups)

    got = lax.all_to_all(sent.reshape(sp_count, SLOT, 256), SP, 0, 0, tiled=True)
    got = got.reshape(slots, 256)

    conv_t = conv_result.T
    conv_f = conv_t.astype(F32)
    sums = jnp.stack([jnp.sum(conv_f, axis=0), jnp.sum(conv_f * conv_f, axis=0)])
    sums = lax.psum(lax.psum(sums, "y"), "x")
    got, sums, weights = lax.optimization_barrier((got, sums, weights))
    gain = norm_gain.reshape(-1, 1)
    taps_t = conv_taps.T

    rows = exchange(jnp.broadcast_to(got[None], (SIDE, slots, 256)), feature_groups)
    step = 256
    pre = pl.pallas_call(
        pre_kernel,
        grid=(slots // step,),
        out_shape=whole((SIDE, 192, slots), BF),
        in_specs=[smem, pl.BlockSpec((SIDE, step, 256), lambda i: (0, i, 0))]
        + [pl.BlockSpec((192, 512), lambda i: (0, 0))] * SIDE,
        out_specs=pl.BlockSpec((SIDE, 192, step), lambda i: (0, 0, i)),
        compiler_params=room,
        cost_estimate=cost(800000000, 4400000),
        name="pre",
    )(at, rows, *weights)
    pre = exchange(pre, unit_groups)
    hidden = pl.pallas_call(
        gate_kernel,
        grid=(slots // step,),
        out_shape=whole((SIDE, 192, slots), BF),
        in_specs=[pl.BlockSpec((SIDE, 192, step), lambda i: (0, 0, i))],
        out_specs=pl.BlockSpec((SIDE, 192, step), lambda i: (0, 0, i)),
        compiler_params=room,
        cost_estimate=cost(3000000, 3200000),
        name="gates",
    )(pre)
    hidden = exchange(hidden, unit_groups)
    part = pl.pallas_call(
        partial_kernel,
        grid=(slots // step,),
        out_shape=whole((SIDE, slots, 128), BF),
        in_specs=[smem, pl.BlockSpec((SIDE, 192, step), lambda i: (0, 0, i))]
        + [pl.BlockSpec((192, 512), lambda i: (0, 0))] * SIDE,
        out_specs=pl.BlockSpec((SIDE, step, 128), lambda i: (0, i, 0)),
        compiler_params=room,
        cost_estimate=cost(540000000, 3400000),
        name="partial",
    )(at, hidden, *weights)
    part = exchange(part, feature_groups)
    back = jnp.sum(part.astype(F32), axis=0).astype(BF).reshape(sp_count, SLOT, 128)
    returned = lax.all_to_all(back, SP, 0, 0, tiled=True).reshape(slots, 128)

    grads = pl.pallas_call(
        grads_kernel,
        grid=(SIDE,),
        out_shape=(whole((192, 512), BF),) * SIDE,
        in_specs=[
            smem,
            pl.BlockSpec((SIDE, 192, slots), lambda i: (0, 0, 0)),
            pl.BlockSpec((1, slots, 256), lambda i: (i, 0, 0)),
        ],
        out_specs=(pl.BlockSpec((192, 128), lambda i: (0, i)),) * SIDE,
        compiler_params=room,
        cost_estimate=cost(800000000, 4400000),
        name="grads",
    )(at, hidden, rows)
    grads = pass_on(grads, unit_groups)
    returned, grads = lax.optimization_barrier((returned, grads))

    spread = pl.pallas_call(
        combine_kernel,
        out_shape=whole((tp_count, tokens, 128), BF),
        in_specs=[vmem] * 3,
        out_specs=vmem,
        compiler_params=room,
        cost_estimate=cost(80000000, 2500000),
        name="combine",
    )(pick, returned, out_cotangent)
    full = lax.all_to_all(spread, TP, 0, 0, tiled=True)

    proj_part = pl.pallas_call(
        proj_kernel,
        out_shape=whole((sp_count, 32, 128), BF),
        in_specs=[vmem] * 4,
        out_specs=vmem,
        compiler_params=room,
        cost_estimate=cost(84000000, 1600000),
        name="proj_grad",
    )(full, conv_t, sums, gain)
    norm_cot, cot_sums = pl.pallas_call(
        norm_kernel,
        out_shape=(whole((64, tokens), F32), whole((2, tokens), F32)),
        in_specs=[vmem] * 5,
        out_specs=(vmem, vmem),
        compiler_params=room,
        cost_estimate=cost(84000000, 1600000),
        name="norm_cot",
    )(full, proj_weight, conv_t, sums, gain)
    proj_part = lax.all_to_all(proj_part, SP, 0, 0, tiled=True)
    cot_sums = lax.psum(lax.psum(cot_sums, "y"), "x")
    conv_cot, head = pl.pallas_call(
        head_kernel,
        out_shape=(whole((64, tokens), F32), whole((64, 128), F32)),
        in_specs=[vmem] * 4,
        out_specs=(vmem, vmem),
        compiler_params=room,
        cost_estimate=cost(1000000, 200000),
        name="conv_cot",
    )(norm_cot, cot_sums, conv_t, sums)
    behind = [(i + 1, i) for i in range(sp_count - 1)]
    after = lax.ppermute(head, SP, behind)
    value, gate = pl.pallas_call(
        conv_kernel,
        out_shape=(whole((64, tokens), BF), whole((64, tokens), BF)),
        in_specs=[vmem] * 5,
        out_specs=(vmem, vmem),
        scratch_shapes=[VM((64, 384), F32)],
        compiler_params=room,
        cost_estimate=cost(4000000, 400000),
        name="conv",
    )(conv_cot, after, taps_t, glu_gate.T, glu_value.T)

    total = jnp.sum(proj_part.astype(F32), axis=0)
    grad_proj = jnp.concatenate([total[:, 0:64], total[:, 64:128]], axis=0).T

    grad_gate, grad_up, grad_down = pl.pallas_call(
        merge_kernel,
        out_shape=(whole((64, 2048), F32),) * 3,
        in_specs=[smem] + [vmem] * SIDE,
        out_specs=(vmem,) * 3,
        compiler_params=room,
        cost_estimate=cost(1000000, 2400000),
        name="merge_grads",
    )(at, *grads)
    return (
        grad_gate[None],
        grad_up[None],
        grad_down[None],
        grad_proj,
        value.T,
        gate.T,
    )


def solution(mesh):
    split = Mesh(mesh.devices.reshape(16, 2, SIDE, SIDE), ("z", "c", "y", "x"))
    placed = (
        P(SP, TP),
        P(SP, TP),
        P(SP, None),
        P(SP, None),
        P(SP, TP, None),
        P(SP, TP, None),
        P(SP, TP, None),
        P(SP, TP),
        P(SP, TP),
        P(SP, TP),
        P(None, TP),
        P(TP),
        P(TP, None),
    )
    return jax.shard_map(
        body,
        mesh=split,
        in_specs=placed,
        out_specs=(
            P(SP, TP, None),
            P(SP, TP, None),
            P(SP, TP, None),
            P(SP, TP),
            P(SP, TP),
            P(SP, TP),
        ),
        check_vma=False,
    )
```

```python
import jax
import jax.numpy as jnp
import numpy as np
from jax import lax
from jax.experimental import pallas as pl
from jax.experimental.pallas import tpu as pltpu
from jax.sharding import Mesh
from jax.sharding import PartitionSpec as P

NORM_EPS = 0.25
SP = ("z", "c")
TP = ("y", "x")
PLANE = ("c", "y", "x")
SIDE = 4
SLOT = 32
ROOM = 12 << 20
BF = jnp.bfloat16
F32 = jnp.float32
VM = pltpu.VMEM

NT = (((1,), (1,)), ((), ()))
TN = (((0,), (0,)), ((), ()))
NN = (((1,), (0,)), ((), ()))


def place(core, row, col):
    return core * SIDE * SIDE + row * SIDE + col


def plane_groups():
    r = range(SIDE)
    down = [[[place(k, y, x) for y in r] for x in r] for k in (0, 1)]
    across = [[[place(k, y, x) for x in r] for y in r] for k in (0, 1)]
    return down[0] + across[1], across[0] + down[1]


def step_tables():
    features, units = plane_groups()
    of_features = {p: g for g in features for p in g}
    table = np.zeros((2 * SIDE * SIDE, 64), np.int32)
    for group in units:
        for me, p in enumerate(group):
            table[p, 0] = me
            table[p, 1] = of_features[p].index(p)
            table[p, 2] = p // (SIDE * SIDE)
            for k in range(SIDE):
                ahead = of_features[group[(me + k) % SIDE]]
                back = of_features[group[(me - k) % SIDE]]
                for a in range(SIDE):
                    table[p, 16 + k * SIDE + a] = ahead[a] % (SIDE * SIDE)
                    table[p, 32 + k * SIDE + a] = back[a] % (SIDE * SIDE)
    of_units = {p: g for g in units for p in g}
    for p in range(2 * SIDE * SIDE):
        group = of_features[p]
        for j in range(SIDE):
            source = group[(group.index(p) - j) % SIDE]
            their = of_units[source]
            for k in range(SIDE):
                first = their[(their.index(source) - k) % SIDE]
                table[p, 48 + j * SIDE + k] = first % (SIDE * SIDE)
    return table


def steps_ahead(groups, k):
    return [(g[i], g[(i + k) % SIDE]) for g in groups for i in range(SIDE)]


def pass_on(parts, groups):
    return (parts[0],) + tuple(
        lax.ppermute(parts[k], PLANE, steps_ahead(groups, k)) for k in range(1, SIDE)
    )


def mm(a, b, dims):
    return lax.dot_general(a, b, dims, preferred_element_type=F32)


def exchange(v, groups):
    return lax.all_to_all(v, PLANE, 0, 0, axis_index_groups=groups, tiled=True)


def cost(flops, nbytes):
    return pl.CostEstimate(flops=flops, bytes_accessed=nbytes, transcendentals=0)


def route_kernel(rt_ref, w_ref, x_ref, c_ref, s_ref, t_ref):
    tokens = rt_ref.shape[1]
    experts = s_ref.shape[0] // SLOT
    first, second = rt_ref[0:1, :], rt_ref[1:2, :]
    ids = lax.broadcasted_iota(jnp.int32, (experts, tokens), 0)
    o0, o1 = ids == first, ids == second
    both = jnp.where(o0 | o1, 1.0, 0.0).astype(BF)
    before = lax.broadcasted_iota(jnp.int32, (tokens, tokens), 0) < lax.broadcasted_iota(
        jnp.int32, (tokens, tokens), 1
    )
    earlier = mm(both, jnp.where(before, 1.0, 0.0).astype(BF), NN)
    rank0 = jnp.sum(jnp.where(o0, earlier, 0.0), axis=0, keepdims=True)
    rank1 = jnp.sum(jnp.where(o1, earlier, 0.0), axis=0, keepdims=True)
    t0 = first * SLOT + rank0.astype(jnp.int32)
    t1 = second * SLOT + rank1.astype(jnp.int32)
    t_ref[0:1, :] = t0
    t_ref[1:2, :] = t1
    w0, w1 = w_ref[0:1, :], w_ref[1:2, :]
    x, c = x_ref[...], c_ref[...]
    size = 128
    for k in range(s_ref.shape[0] // size):
        slots = lax.broadcasted_iota(jnp.int32, (size, tokens), 0) + k * size
        m0, m1 = slots == t0, slots == t1
        pick = jnp.where(m0 | m1, 1.0, 0.0).astype(BF)
        weight = jnp.sum(
            jnp.where(m0, w0, 0.0) + jnp.where(m1, w1, 0.0), axis=1, keepdims=True
        )
        rows = pl.ds(k * size, size)
        s_ref[rows, 0:128] = mm(pick, x, NN).astype(BF)
        s_ref[rows, 128:256] = (weight * mm(pick, c, NN)).astype(BF)


def pick_kernel(t_ref, p_ref):
    slots = lax.broadcasted_iota(jnp.int32, p_ref.shape, 0)
    held = (slots == t_ref[0:1, :]) | (slots == t_ref[1:2, :])
    p_ref[...] = jnp.where(held, 1.0, 0.0).astype(BF)


def split_kernel(at_ref, g_ref, u_ref, d_ref, p_ref, c_ref, *outs):
    for k, out in enumerate(outs):
        for a in range(SIDE):
            at = at_ref[16 + k * SIDE + a]
            cols = pl.ds(pl.multiple_of(at * 128, 128), 128)
            for q, ref in enumerate((g_ref, u_ref, d_ref, p_ref)):
                out[q * 64 : q * 64 + 64, a * 128 : a * 128 + 128] = ref[:, cols]
        out[256:320, :] = c_ref[...]


def relay_kernel(at_ref, r0, r1, r2, r3, *outs):
    for j, out in enumerate(outs):
        a = lax.rem(at_ref[1] + j, SIDE)
        cols = pl.ds(pl.multiple_of(a * 128, 128), 128)
        for k, r_ref in enumerate((r0, r1, r2, r3)):
            out[k * 64 : k * 64 + 64, 0:128] = r_ref[192:256, cols]
            out[k * 64 : k * 64 + 64, 128:512] = r_ref[256:320, 128:512]


def prep_kernel(q0, q1, q2, q3, act_ref, h_ref, n_ref, stats_ref):
    qs = (q0, q1, q2, q3)
    tokens = stats_ref.shape[1]
    channels = SIDE * q0.shape[0]
    conv = [q[:, 128 : 128 + tokens].astype(F32) for q in qs]
    mean = sum(jnp.sum(v, axis=0, keepdims=True) for v in conv) / channels
    off = [v - mean for v in conv]
    var = sum(jnp.sum(v * v, axis=0, keepdims=True) for v in off) / channels
    inv = lax.rsqrt(var + NORM_EPS)
    stats_ref[0:1, :] = mean
    stats_ref[1:2, :] = inv
    lane = lax.broadcasted_iota(jnp.int32, (q0.shape[0], 128), 1)
    for j, q in enumerate(qs):
        pieces = jnp.where((lane >= 64) & (lane < 67), q[:, 384:512].astype(F32), 0.0)
        gain = jnp.sum(pieces, axis=1, keepdims=True)
        normed = off[j] * inv
        linear = normed * gain
        s = jax.nn.sigmoid(linear)
        slope = s * (1.0 + linear * (1.0 - s)) * gain
        act_ref[j] = (linear * s).astype(BF)
        h_ref[j] = slope.astype(BF)
        n_ref[j] = (slope * normed).astype(BF)


def merge_kernel(at_ref, s0, s1, s2, s3, g_ref, u_ref, d_ref):
    for k, s_ref in enumerate((s0, s1, s2, s3)):
        for a in range(SIDE):
            at = at_ref[32 + k * SIDE + a]
            cols = pl.ds(pl.multiple_of(at * 128, 128), 128)
            for q, ref in enumerate((g_ref, u_ref, d_ref)):
                ref[:, cols] = s_ref[
                    q * 64 : q * 64 + 64, a * 128 : a * 128 + 128
                ].astype(F32)


def behind_of(at_ref, k):
    return lax.rem(at_ref[0] + (SIDE - k), SIDE)


def ahead_of(at_ref, k):
    return lax.rem(at_ref[0] + k, SIDE)


def pre_kernel(at_ref, a_ref, w0, w1, w2, w3, o_ref):
    x = jnp.concatenate([a_ref[i, :, 0:128] for i in range(SIDE)], axis=1)
    c = jnp.concatenate([a_ref[i, :, 128:256] for i in range(SIDE)], axis=1)
    for k, w_ref in enumerate((w0, w1, w2, w3)):
        b = behind_of(at_ref, k)
        o_ref[b, 0:128, :] = mm(w_ref[0:128, :], x, NT).astype(BF)
        o_ref[b, 128:192, :] = mm(w_ref[128:192, :], c, NT).astype(BF)


def gate_kernel(p_ref, o_ref):
    total = p_ref[0].astype(F32)
    for b in range(1, SIDE):
        total = total + p_ref[b].astype(F32)
    gate, up, cot = total[0:64], total[64:128], total[128:192]
    s = jax.nn.sigmoid(gate)
    act = gate * s
    hidden = (act * up).astype(BF)
    up_cot = (cot * act).astype(BF)
    gate_cot = (cot * up * s * (1.0 + gate * (1.0 - s))).astype(BF)
    for b in range(SIDE):
        o_ref[b, 0:64, :] = gate_cot
        o_ref[b, 64:128, :] = up_cot
        o_ref[b, 128:192, :] = hidden


def partial_kernel(at_ref, h_ref, w0, w1, w2, w3, o_ref):
    ws = (w0, w1, w2, w3)
    h = jnp.concatenate([h_ref[behind_of(at_ref, k), 0:128, :] for k in range(SIDE)], axis=0)
    w = jnp.concatenate([w_ref[0:128, :] for w_ref in ws], axis=0)
    total = mm(h, w, TN)
    for a in range(SIDE):
        o_ref[a] = total[:, a * 128 : a * 128 + 128].astype(BF)


def grads_kernel(at_ref, h_ref, a_ref, *outs):
    x, c = a_ref[0, :, 0:128], a_ref[0, :, 128:256]
    for k, out in enumerate(outs):
        b = ahead_of(at_ref, k)
        out[0:128, :] = mm(h_ref[b, 0:128, :], x, NN).astype(BF)
        out[128:192, :] = mm(h_ref[b, 128:192, :], c, NN).astype(BF)


def tail_kernel(
    at_ref, p_ref, r_ref, c_ref, q0, q1, q2, q3, act_ref, h_ref, n_ref, o_ref, mine_ref, other_ref
):
    moe = mm(p_ref[...], r_ref[...], TN)
    total = (c_ref[...].astype(F32) + moe).astype(BF)
    tokens = total.shape[0]
    first = jnp.zeros((1, tokens), F32)
    second = jnp.zeros((1, tokens), F32)
    own = jnp.full((32, 128), at_ref[2], jnp.int32) == 0
    low = lax.broadcasted_iota(jnp.int32, (32, 128), 1) < 64
    for j, q in enumerate((q0, q1, q2, q3)):
        cot = mm(q[:, 0:128], total, NT)
        first = first + jnp.sum(cot * h_ref[j].astype(F32), axis=0, keepdims=True)
        second = second + jnp.sum(cot * n_ref[j].astype(F32), axis=0, keepdims=True)
        grad = mm(act_ref[j], total, NN)
        turned = pltpu.roll(grad, 64, 1)
        for k in range(SIDE):
            b = at_ref[48 + j * SIDE + k]
            o_ref[b, 0:64, :] = cot[k * 64 : k * 64 + 64].astype(BF)
            up, down = slice(k * 64, k * 64 + 32), slice(k * 64 + 32, k * 64 + 64)
            left = jnp.where(low, grad[up], turned[down])
            right = jnp.where(low, turned[up], grad[down])
            mine_ref[b] = jnp.where(own, left, right).astype(BF)
            other_ref[b] = jnp.where(own, right, left).astype(BF)
    row = lax.broadcasted_iota(jnp.int32, (16, tokens), 0)
    sums = jnp.zeros((16, tokens), F32)
    for i, v in enumerate((first, second)):
        head = v.astype(BF).astype(F32)
        sums = jnp.where(row == 2 * i, head, jnp.where(row == 2 * i + 1, v - head, sums))
    for b in range(o_ref.shape[0]):
        o_ref[b, 64:80, :] = sums.astype(BF)


def head_kernel(r_ref, conv_ref, stats_ref, gain_ref, o_ref, h_ref):
    total = r_ref[0].astype(F32)
    for b in range(1, r_ref.shape[0]):
        total = total + r_ref[b].astype(F32)
    channels = 16 * conv_ref.shape[0]
    first = (total[64:65] + total[65:66]) / channels
    second = (total[66:67] + total[67:68]) / channels
    inv = stats_ref[1:2, :]
    normed = (conv_ref[...].astype(F32) - stats_ref[0:1, :]) * inv
    gain = gain_ref[...]
    linear = normed * gain
    s = jax.nn.sigmoid(linear)
    cot = total[0:64] * s * (1.0 + linear * (1.0 - s)) * gain
    cot = inv * (cot - first - normed * second)
    o_ref[...] = cot
    h_ref[...] = cot[:, 0:128]


def add_kernel(a_ref, b_ref, o_ref):
    o_ref[...] = (a_ref[...].astype(F32) + b_ref[...].astype(F32)).astype(BF)


def conv_kernel(cot_ref, next_ref, taps_ref, gate_ref, value_ref, v_ref, g_ref, buf):
    rows, tokens = cot_ref.shape
    wide = buf.shape[1]
    reach = taps_ref.shape[1] - 1
    buf[:, 0:128] = next_ref[...]
    buf[:, 128:wide] = jnp.zeros((rows, wide - 128), F32)
    after = pltpu.roll(buf[...], tokens, 1)
    buf[:, 0:tokens] = cot_ref[...]
    lane = lax.broadcasted_iota(jnp.int32, (rows, wide), 1)
    whole = jnp.where(lane < tokens, buf[...], after)
    taps = taps_ref[...]
    total = whole * taps[:, reach : reach + 1]
    for s in range(1, reach + 1):
        total = total + pltpu.roll(whole, wide - s, 1) * taps[:, reach - s : reach - s + 1]
    cot = total[:, 0:tokens]
    s = jax.nn.sigmoid(gate_ref[...].astype(F32))
    v_ref[...] = (cot * s).astype(BF)
    g_ref[...] = (cot * value_ref[...].astype(F32) * s * (1.0 - s)).astype(BF)


def whole(shape, dtype):
    return jax.ShapeDtypeStruct(shape, dtype)


def body(
    moe_input,
    out_cotangent,
    routes,
    route_weight,
    gate_weight,
    up_weight,
    down_weight,
    glu_value,
    glu_gate,
    conv_result,
    conv_taps,
    norm_gain,
    proj_weight,
):
    sp_count = lax.axis_size(SP)
    tp_count = lax.axis_size(TP)
    tokens = moe_input.shape[0]
    slots = sp_count * SLOT
    feature_groups, unit_groups = plane_groups()
    smem = pl.BlockSpec(memory_space=pltpu.SMEM)
    vmem = pl.BlockSpec(memory_space=VM)
    room = pltpu.CompilerParams(vmem_limit_bytes=ROOM)

    sent, target = pl.pallas_call(
        route_kernel,
        out_shape=(whole((slots, 256), BF), whole((2, tokens), jnp.int32)),
        in_specs=[vmem] * 4,
        out_specs=(vmem, vmem),
        cost_estimate=cost(400000000, 2000000),
        name="route",
    )(routes.T, route_weight.T, moe_input, out_cotangent)
    sent, target, table, gate_weight, conv_result, norm_gain = lax.optimization_barrier(
        (sent, target, jnp.asarray(step_tables()), gate_weight, conv_result, norm_gain)
    )
    at = table[lax.axis_index(PLANE)]
    pick = pl.pallas_call(
        pick_kernel,
        out_shape=whole((slots, tokens), BF),
        in_specs=[vmem],
        out_specs=vmem,
        compiler_params=room,
        cost_estimate=cost(1000000, 700000),
        name="pick",
    )(target)
    conv_t = conv_result.T
    gain = norm_gain.reshape(-1, 1)
    high = lax.reduce_precision(gain, 8, 7)
    middle = lax.reduce_precision(gain - high, 8, 7)
    pieces = jnp.concatenate([high, middle, gain - high - middle], axis=1).astype(BF)
    channel_part = jnp.concatenate(
        [jnp.zeros((64, 128), BF), conv_t, pieces, jnp.zeros((64, 61), BF)], axis=1
    )
    split = pl.pallas_call(
        split_kernel,
        out_shape=(whole((320, 512), BF),) * SIDE,
        in_specs=[smem] + [vmem] * 5,
        out_specs=(vmem,) * SIDE,
        compiler_params=room,
        cost_estimate=cost(1000000, 2600000),
        name="split_weights",
    )(at, gate_weight[0], up_weight[0], down_weight[0], proj_weight, channel_part)
    weights = pass_on(split, unit_groups)
    relay = pl.pallas_call(
        relay_kernel,
        out_shape=(whole((256, 512), BF),) * SIDE,
        in_specs=[smem] + [vmem] * SIDE,
        out_specs=(vmem,) * SIDE,
        compiler_params=room,
        cost_estimate=cost(1000000, 2000000),
        name="relay",
    )(at, *weights)
    relay = pass_on(relay, feature_groups)

    got = lax.all_to_all(sent.reshape(sp_count, SLOT, 256), SP, 0, 0, tiled=True)
    got = got.reshape(slots, 256)
    got, weights, relay = lax.optimization_barrier((got, weights, relay))
    taps_t = conv_taps.T

    rows = exchange(jnp.broadcast_to(got[None], (SIDE, slots, 256)), feature_groups)
    step = 256
    pre = pl.pallas_call(
        pre_kernel,
        grid=(slots // step,),
        out_shape=whole((SIDE, 192, slots), BF),
        in_specs=[smem, pl.BlockSpec((SIDE, step, 256), lambda i: (0, i, 0))]
        + [pl.BlockSpec((192, 512), lambda i: (0, 0))] * SIDE,
        out_specs=pl.BlockSpec((SIDE, 192, step), lambda i: (0, 0, i)),
        compiler_params=room,
        cost_estimate=cost(800000000, 4400000),
        name="pre",
    )(at, rows, *weights)
    pre = exchange(pre, unit_groups)
    act, slope, slope_normed, stats = pl.pallas_call(
        prep_kernel,
        out_shape=(whole((SIDE, 256, tokens), BF),) * 3 + (whole((2, tokens), F32),),
        in_specs=[vmem] * SIDE,
        out_specs=(vmem,) * 4,
        compiler_params=room,
        cost_estimate=cost(20000000, 3000000),
        name="prep",
    )(*relay)
    pre, act, slope, slope_normed, stats = lax.optimization_barrier(
        (pre, act, slope, slope_normed, stats)
    )
    hidden = pl.pallas_call(
        gate_kernel,
        grid=(slots // step,),
        out_shape=whole((SIDE, 192, slots), BF),
        in_specs=[pl.BlockSpec((SIDE, 192, step), lambda i: (0, 0, i))],
        out_specs=pl.BlockSpec((SIDE, 192, step), lambda i: (0, 0, i)),
        compiler_params=room,
        cost_estimate=cost(3000000, 3200000),
        name="gates",
    )(pre)
    hidden = exchange(hidden, unit_groups)
    part = pl.pallas_call(
        partial_kernel,
        grid=(slots // step,),
        out_shape=whole((SIDE, slots, 128), BF),
        in_specs=[smem, pl.BlockSpec((SIDE, 192, step), lambda i: (0, 0, i))]
        + [pl.BlockSpec((192, 512), lambda i: (0, 0))] * SIDE,
        out_specs=pl.BlockSpec((SIDE, step, 128), lambda i: (0, i, 0)),
        compiler_params=room,
        cost_estimate=cost(540000000, 3400000),
        name="partial",
    )(at, hidden, *weights)
    part = exchange(part, feature_groups)
    back = jnp.sum(part.astype(F32), axis=0).astype(BF).reshape(sp_count, SLOT, 128)
    returned = lax.all_to_all(back, SP, 0, 0, tiled=True).reshape(slots, 128)

    grads = pl.pallas_call(
        grads_kernel,
        grid=(SIDE,),
        out_shape=(whole((192, 512), BF),) * SIDE,
        in_specs=[
            smem,
            pl.BlockSpec((SIDE, 192, slots), lambda i: (0, 0, 0)),
            pl.BlockSpec((1, slots, 256), lambda i: (i, 0, 0)),
        ],
        out_specs=(pl.BlockSpec((192, 128), lambda i: (0, i)),) * SIDE,
        compiler_params=room,
        cost_estimate=cost(800000000, 4400000),
        name="grads",
    )(at, hidden, rows)
    grads = pass_on(grads, unit_groups)
    returned, grads = lax.optimization_barrier((returned, grads))

    act_part, mine, other = pl.pallas_call(
        tail_kernel,
        out_shape=(
            whole((tp_count, 80, tokens), BF),
            whole((tp_count, 32, 128), BF),
            whole((tp_count, 32, 128), BF),
        ),
        in_specs=[smem] + [vmem] * 10,
        out_specs=(vmem,) * 3,
        compiler_params=room,
        cost_estimate=cost(250000000, 4500000),
        name="tail",
    )(at, pick, returned, out_cotangent, *relay, act, slope, slope_normed)
    act_part = lax.all_to_all(act_part, TP, 0, 0, tiled=True)
    other = lax.ppermute(other, "c", [(0, 1), (1, 0)])
    proj_part = pl.pallas_call(
        add_kernel,
        out_shape=whole((tp_count, 32, 128), BF),
        in_specs=[vmem] * 2,
        out_specs=vmem,
        compiler_params=room,
        cost_estimate=cost(100000, 400000),
        name="add_core",
    )(mine, other)
    side = SIDE * SIDE
    swap = [
        (z * 2 * side + c * side + t, t * 2 * side + c * side + z)
        for z in range(side)
        for c in range(2)
        for t in range(side)
    ]
    proj_part = lax.ppermute(proj_part, ("z",) + PLANE, swap)
    act_part, proj_part = lax.optimization_barrier((act_part, proj_part))
    proj_part = lax.all_to_all(proj_part, TP, 0, 0, tiled=True)

    conv_cot, head = pl.pallas_call(
        head_kernel,
        out_shape=(whole((64, tokens), F32), whole((64, 128), F32)),
        in_specs=[vmem] * 4,
        out_specs=(vmem, vmem),
        compiler_params=room,
        cost_estimate=cost(3000000, 1200000),
        name="conv_cot",
    )(act_part, conv_t, stats, gain)
    behind = [(i + 1, i) for i in range(sp_count - 1)]
    after = lax.ppermute(head, SP, behind)
    value, gate = pl.pallas_call(
        conv_kernel,
        out_shape=(whole((64, tokens), BF), whole((64, tokens), BF)),
        in_specs=[vmem] * 5,
        out_specs=(vmem, vmem),
        scratch_shapes=[VM((64, 384), F32)],
        compiler_params=room,
        cost_estimate=cost(4000000, 400000),
        name="conv",
    )(conv_cot, after, taps_t, glu_gate.T, glu_value.T)

    total = jnp.sum(proj_part.astype(F32), axis=0)
    grad_proj = jnp.concatenate([total[:, 0:64], total[:, 64:128]], axis=0).T

    grad_gate, grad_up, grad_down = pl.pallas_call(
        merge_kernel,
        out_shape=(whole((64, 2048), F32),) * 3,
        in_specs=[smem] + [vmem] * SIDE,
        out_specs=(vmem,) * 3,
        compiler_params=room,
        cost_estimate=cost(1000000, 2400000),
        name="merge_grads",
    )(at, *grads)
    return (
        grad_gate[None],
        grad_up[None],
        grad_down[None],
        grad_proj,
        value.T,
        gate.T,
    )


def solution(mesh):
    split = Mesh(mesh.devices.reshape(16, 2, SIDE, SIDE), ("z", "c", "y", "x"))
    placed = (
        P(SP, TP),
        P(SP, TP),
        P(SP, None),
        P(SP, None),
        P(SP, TP, None),
        P(SP, TP, None),
        P(SP, TP, None),
        P(SP, TP),
        P(SP, TP),
        P(SP, TP),
        P(None, TP),
        P(TP),
        P(TP, None),
    )
    return jax.shard_map(
        body,
        mesh=split,
        in_specs=placed,
        out_specs=(
            P(SP, TP, None),
            P(SP, TP, None),
            P(SP, TP, None),
            P(SP, TP),
            P(SP, TP),
            P(SP, TP),
        ),
        check_vma=False,
    )
```

```python
import jax
import jax.numpy as jnp
import numpy as np
from jax import lax
from jax.experimental import pallas as pl
from jax.experimental.pallas import tpu as pltpu
from jax.sharding import Mesh
from jax.sharding import PartitionSpec as P

NORM_EPS = 0.25
SP = ("z", "c")
TP = ("y", "x")
PLANE = ("c", "y", "x")
SIDE = 4
SLOT = 32
ROOM = 12 << 20
BF = jnp.bfloat16
F32 = jnp.float32
VM = pltpu.VMEM

NT = (((1,), (1,)), ((), ()))
TN = (((0,), (0,)), ((), ()))
NN = (((1,), (0,)), ((), ()))


def place(core, row, col):
    return core * SIDE * SIDE + row * SIDE + col


def plane_groups():
    r = range(SIDE)
    down = [[[place(k, y, x) for y in r] for x in r] for k in (0, 1)]
    across = [[[place(k, y, x) for x in r] for y in r] for k in (0, 1)]
    return down[0] + across[1], across[0] + down[1]


def step_tables():
    features, units = plane_groups()
    of_features = {p: g for g in features for p in g}
    table = np.zeros((2 * SIDE * SIDE, 64), np.int32)
    for group in units:
        for me, p in enumerate(group):
            table[p, 0] = me
            table[p, 1] = of_features[p].index(p)
            table[p, 2] = p // (SIDE * SIDE)
            for k in range(SIDE):
                ahead = of_features[group[(me + k) % SIDE]]
                back = of_features[group[(me - k) % SIDE]]
                for a in range(SIDE):
                    table[p, 16 + k * SIDE + a] = ahead[a] % (SIDE * SIDE)
                    table[p, 32 + k * SIDE + a] = back[a] % (SIDE * SIDE)
    of_units = {p: g for g in units for p in g}
    for p in range(2 * SIDE * SIDE):
        group = of_features[p]
        for j in range(SIDE):
            source = group[(group.index(p) - j) % SIDE]
            their = of_units[source]
            for k in range(SIDE):
                first = their[(their.index(source) - k) % SIDE]
                table[p, 48 + j * SIDE + k] = first % (SIDE * SIDE)
    return table


def steps_ahead(groups, k):
    return [(g[i], g[(i + k) % SIDE]) for g in groups for i in range(SIDE)]


def pass_on(parts, groups):
    return (parts[0],) + tuple(
        lax.ppermute(parts[k], PLANE, steps_ahead(groups, k)) for k in range(1, SIDE)
    )


def mm(a, b, dims):
    return lax.dot_general(a, b, dims, preferred_element_type=F32)


def exchange(v, groups):
    return lax.all_to_all(v, PLANE, 0, 0, axis_index_groups=groups, tiled=True)


def cost(flops, nbytes):
    return pl.CostEstimate(flops=flops, bytes_accessed=nbytes, transcendentals=0)


def route_kernel(rt_ref, w_ref, x_ref, c_ref, s_ref, t_ref):
    tokens = rt_ref.shape[1]
    experts = s_ref.shape[0] // SLOT
    first, second = rt_ref[0:1, :], rt_ref[1:2, :]
    ids = lax.broadcasted_iota(jnp.int32, (experts, tokens), 0)
    o0, o1 = ids == first, ids == second
    both = jnp.where(o0 | o1, 1.0, 0.0).astype(BF)
    before = lax.broadcasted_iota(jnp.int32, (tokens, tokens), 0) < lax.broadcasted_iota(
        jnp.int32, (tokens, tokens), 1
    )
    earlier = mm(both, jnp.where(before, 1.0, 0.0).astype(BF), NN)
    rank0 = jnp.sum(jnp.where(o0, earlier, 0.0), axis=0, keepdims=True)
    rank1 = jnp.sum(jnp.where(o1, earlier, 0.0), axis=0, keepdims=True)
    t0 = first * SLOT + rank0.astype(jnp.int32)
    t1 = second * SLOT + rank1.astype(jnp.int32)
    t_ref[0:1, :] = t0
    t_ref[1:2, :] = t1
    w0, w1 = w_ref[0:1, :], w_ref[1:2, :]
    x, c = x_ref[...], c_ref[...]
    size = 128
    for k in range(s_ref.shape[0] // size):
        slots = lax.broadcasted_iota(jnp.int32, (size, tokens), 0) + k * size
        m0, m1 = slots == t0, slots == t1
        pick = jnp.where(m0 | m1, 1.0, 0.0).astype(BF)
        weight = jnp.sum(
            jnp.where(m0, w0, 0.0) + jnp.where(m1, w1, 0.0), axis=1, keepdims=True
        )
        rows = pl.ds(k * size, size)
        s_ref[rows, 0:128] = mm(pick, x, NN).astype(BF)
        s_ref[rows, 128:256] = (weight * mm(pick, c, NN)).astype(BF)


def pick_kernel(t_ref, p_ref):
    slots = lax.broadcasted_iota(jnp.int32, p_ref.shape, 0)
    held = (slots == t_ref[0:1, :]) | (slots == t_ref[1:2, :])
    p_ref[...] = jnp.where(held, 1.0, 0.0).astype(BF)


def split_kernel(at_ref, g_ref, u_ref, d_ref, p_ref, c_ref, *outs):
    for k, out in enumerate(outs):
        for a in range(SIDE):
            at = at_ref[16 + k * SIDE + a]
            cols = pl.ds(pl.multiple_of(at * 128, 128), 128)
            for q, ref in enumerate((g_ref, u_ref, d_ref, p_ref)):
                out[q * 64 : q * 64 + 64, a * 128 : a * 128 + 128] = ref[:, cols]
        out[256:320, :] = c_ref[...]


def relay_kernel(at_ref, r0, r1, r2, r3, *outs):
    for j, out in enumerate(outs):
        a = lax.rem(at_ref[1] + j, SIDE)
        cols = pl.ds(pl.multiple_of(a * 128, 128), 128)
        for k, r_ref in enumerate((r0, r1, r2, r3)):
            out[k * 64 : k * 64 + 64, 0:128] = r_ref[192:256, cols]
            out[k * 64 : k * 64 + 64, 128:512] = r_ref[256:320, 128:512]


def merge_kernel(at_ref, s0, s1, s2, s3, g_ref, u_ref, d_ref):
    for k, s_ref in enumerate((s0, s1, s2, s3)):
        for a in range(SIDE):
            at = at_ref[32 + k * SIDE + a]
            cols = pl.ds(pl.multiple_of(at * 128, 128), 128)
            for q, ref in enumerate((g_ref, u_ref, d_ref)):
                ref[:, cols] = s_ref[
                    q * 64 : q * 64 + 64, a * 128 : a * 128 + 128
                ].astype(F32)


def behind_of(at_ref, k):
    return lax.rem(at_ref[0] + (SIDE - k), SIDE)


def ahead_of(at_ref, k):
    return lax.rem(at_ref[0] + k, SIDE)


def pre_kernel(at_ref, a_ref, w0, w1, w2, w3, o_ref):
    x = jnp.concatenate([a_ref[i, :, 0:128] for i in range(SIDE)], axis=1)
    c = jnp.concatenate([a_ref[i, :, 128:256] for i in range(SIDE)], axis=1)
    for k, w_ref in enumerate((w0, w1, w2, w3)):
        b = behind_of(at_ref, k)
        o_ref[b, 0:128, :] = mm(w_ref[0:128, :], x, NT).astype(BF)
        o_ref[b, 128:192, :] = mm(w_ref[128:192, :], c, NT).astype(BF)


def gate_kernel(p_ref, o_ref):
    total = p_ref[0].astype(F32)
    for b in range(1, SIDE):
        total = total + p_ref[b].astype(F32)
    gate, up, cot = total[0:64], total[64:128], total[128:192]
    s = jax.nn.sigmoid(gate)
    act = gate * s
    hidden = (act * up).astype(BF)
    up_cot = (cot * act).astype(BF)
    gate_cot = (cot * up * s * (1.0 + gate * (1.0 - s))).astype(BF)
    for b in range(SIDE):
        o_ref[b, 0:64, :] = gate_cot
        o_ref[b, 64:128, :] = up_cot
        o_ref[b, 128:192, :] = hidden


def partial_kernel(at_ref, h_ref, w0, w1, w2, w3, o_ref):
    ws = (w0, w1, w2, w3)
    h = jnp.concatenate([h_ref[behind_of(at_ref, k), 0:128, :] for k in range(SIDE)], axis=0)
    w = jnp.concatenate([w_ref[0:128, :] for w_ref in ws], axis=0)
    total = mm(h, w, TN)
    for a in range(SIDE):
        o_ref[a] = total[:, a * 128 : a * 128 + 128].astype(BF)


def grads_kernel(at_ref, h_ref, a_ref, *outs):
    x, c = a_ref[0, :, 0:128], a_ref[0, :, 128:256]
    for k, out in enumerate(outs):
        b = ahead_of(at_ref, k)
        out[0:128, :] = mm(h_ref[b, 0:128, :], x, NN).astype(BF)
        out[128:192, :] = mm(h_ref[b, 128:192, :], c, NN).astype(BF)


def tail_kernel(
    at_ref, p_ref, r_ref, c_ref, q0, q1, q2, q3, o_ref, mine_ref, other_ref, stats_ref, held, sem
):
    copies = [
        pltpu.make_async_copy(q, held.at[j], sem.at[j]) for j, q in enumerate((q0, q1, q2, q3))
    ]
    for copy in copies:
        copy.start()
    moe = mm(p_ref[...], r_ref[...], TN)
    total = (c_ref[...].astype(F32) + moe).astype(BF)
    tokens = total.shape[0]
    size = held.shape[1]
    channels = SIDE * size
    for copy in copies:
        copy.wait()
    mean = jnp.zeros((1, tokens), F32)
    for j in range(SIDE):
        conv = held[j, :, 128 : 128 + tokens].astype(F32)
        mean = mean + jnp.sum(conv, axis=0, keepdims=True)
    mean = mean / channels
    var = jnp.zeros((1, tokens), F32)
    for j in range(SIDE):
        off = held[j, :, 128 : 128 + tokens].astype(F32) - mean
        var = var + jnp.sum(off * off, axis=0, keepdims=True)
    inv = lax.rsqrt(var / channels + NORM_EPS)
    stats_ref[0:1, :] = mean
    stats_ref[1:2, :] = inv
    first = jnp.zeros((1, tokens), F32)
    second = jnp.zeros((1, tokens), F32)
    own = jnp.full((32, 128), at_ref[2], jnp.int32) == 0
    low = lax.broadcasted_iota(jnp.int32, (32, 128), 1) < 64
    lane = lax.broadcasted_iota(jnp.int32, (size, 128), 1)
    for j in range(SIDE):
        pieces = jnp.where((lane >= 64) & (lane < 67), held[j, :, 384:512].astype(F32), 0.0)
        gain = jnp.sum(pieces, axis=1, keepdims=True)
        normed = (held[j, :, 128 : 128 + tokens].astype(F32) - mean) * inv
        linear = normed * gain
        s = jax.nn.sigmoid(linear)
        act = (linear * s).astype(BF)
        cot = mm(held[j, :, 0:128], total, NT)
        sloped = cot * (s * (1.0 + linear * (1.0 - s)) * gain)
        first = first + jnp.sum(sloped, axis=0, keepdims=True)
        second = second + jnp.sum(sloped * normed, axis=0, keepdims=True)
        grad = mm(act, total, NN)
        turned = pltpu.roll(grad, 64, 1)
        for k in range(SIDE):
            b = at_ref[48 + j * SIDE + k]
            o_ref[b, 0:64, :] = cot[k * 64 : k * 64 + 64].astype(BF)
            up, down = slice(k * 64, k * 64 + 32), slice(k * 64 + 32, k * 64 + 64)
            left = jnp.where(low, grad[up], turned[down])
            right = jnp.where(low, turned[up], grad[down])
            mine_ref[b] = jnp.where(own, left, right).astype(BF)
            other_ref[b] = jnp.where(own, right, left).astype(BF)
    row = lax.broadcasted_iota(jnp.int32, (16, tokens), 0)
    sums = jnp.zeros((16, tokens), F32)
    for i, v in enumerate((first, second)):
        head = v.astype(BF).astype(F32)
        sums = jnp.where(row == 2 * i, head, jnp.where(row == 2 * i + 1, v - head, sums))
    for b in range(o_ref.shape[0]):
        o_ref[b, 64:80, :] = sums.astype(BF)


def head_kernel(r_ref, conv_ref, stats_ref, gain_ref, o_ref, h_ref):
    total = r_ref[0].astype(F32)
    for b in range(1, r_ref.shape[0]):
        total = total + r_ref[b].astype(F32)
    channels = 16 * conv_ref.shape[0]
    first = (total[64:65] + total[65:66]) / channels
    second = (total[66:67] + total[67:68]) / channels
    inv = stats_ref[1:2, :]
    normed = (conv_ref[...].astype(F32) - stats_ref[0:1, :]) * inv
    gain = gain_ref[...]
    linear = normed * gain
    s = jax.nn.sigmoid(linear)
    cot = total[0:64] * s * (1.0 + linear * (1.0 - s)) * gain
    cot = inv * (cot - first - normed * second)
    o_ref[...] = cot
    h_ref[...] = cot[:, 0:128]


def sum_kernel(a_ref, o_ref):
    total = a_ref[0].astype(F32)
    for b in range(1, a_ref.shape[0]):
        total = total + a_ref[b].astype(F32)
    turned = pltpu.roll(total, 64, 1)
    block = jnp.concatenate([total, turned], axis=0)
    o_ref[...] = block.T[0:64, :].astype(BF)


def add_kernel(a_ref, b_ref, o_ref):
    o_ref[...] = (a_ref[...].astype(F32) + b_ref[...].astype(F32)).astype(BF)


def conv_kernel(cot_ref, next_ref, taps_ref, gate_ref, value_ref, v_ref, g_ref, buf):
    rows, tokens = cot_ref.shape
    wide = buf.shape[1]
    reach = taps_ref.shape[1] - 1
    buf[:, 0:128] = next_ref[...]
    buf[:, 128:wide] = jnp.zeros((rows, wide - 128), F32)
    after = pltpu.roll(buf[...], tokens, 1)
    buf[:, 0:tokens] = cot_ref[...]
    lane = lax.broadcasted_iota(jnp.int32, (rows, wide), 1)
    whole = jnp.where(lane < tokens, buf[...], after)
    taps = taps_ref[...]
    total = whole * taps[:, reach : reach + 1]
    for s in range(1, reach + 1):
        total = total + pltpu.roll(whole, wide - s, 1) * taps[:, reach - s : reach - s + 1]
    cot = total[:, 0:tokens]
    s = jax.nn.sigmoid(gate_ref[...].astype(F32))
    v_ref[...] = (cot * s).astype(BF)
    g_ref[...] = (cot * value_ref[...].astype(F32) * s * (1.0 - s)).astype(BF)


def whole(shape, dtype):
    return jax.ShapeDtypeStruct(shape, dtype)


def body(
    moe_input,
    out_cotangent,
    routes,
    route_weight,
    gate_weight,
    up_weight,
    down_weight,
    glu_value,
    glu_gate,
    conv_result,
    conv_taps,
    norm_gain,
    proj_weight,
):
    sp_count = lax.axis_size(SP)
    tp_count = lax.axis_size(TP)
    tokens = moe_input.shape[0]
    slots = sp_count * SLOT
    feature_groups, unit_groups = plane_groups()
    smem = pl.BlockSpec(memory_space=pltpu.SMEM)
    vmem = pl.BlockSpec(memory_space=VM)
    room = pltpu.CompilerParams(vmem_limit_bytes=ROOM)

    sent, target = pl.pallas_call(
        route_kernel,
        out_shape=(whole((slots, 256), BF), whole((2, tokens), jnp.int32)),
        in_specs=[vmem] * 4,
        out_specs=(vmem, vmem),
        cost_estimate=cost(400000000, 2000000),
        name="route",
    )(routes.T, route_weight.T, moe_input, out_cotangent)
    sent, target, table, gate_weight, conv_result, norm_gain = lax.optimization_barrier(
        (sent, target, jnp.asarray(step_tables()), gate_weight, conv_result, norm_gain)
    )
    at = table[lax.axis_index(PLANE)]
    pick = pl.pallas_call(
        pick_kernel,
        out_shape=whole((slots, tokens), BF),
        in_specs=[vmem],
        out_specs=vmem,
        compiler_params=room,
        cost_estimate=cost(1000000, 700000),
        name="pick",
    )(target)
    conv_t = conv_result.T
    gain = norm_gain.reshape(-1, 1)
    high = lax.reduce_precision(gain, 8, 7)
    middle = lax.reduce_precision(gain - high, 8, 7)
    pieces = jnp.concatenate([high, middle, gain - high - middle], axis=1).astype(BF)
    channel_part = jnp.concatenate(
        [jnp.zeros((64, 128), BF), conv_t, pieces, jnp.zeros((64, 61), BF)], axis=1
    )
    split = pl.pallas_call(
        split_kernel,
        out_shape=(whole((320, 512), BF),) * SIDE,
        in_specs=[smem] + [vmem] * 5,
        out_specs=(vmem,) * SIDE,
        compiler_params=room,
        cost_estimate=cost(1000000, 2600000),
        name="split_weights",
    )(at, gate_weight[0], up_weight[0], down_weight[0], proj_weight, channel_part)
    weights = pass_on(split, unit_groups)
    got = lax.all_to_all(sent.reshape(sp_count, SLOT, 256), SP, 0, 0, tiled=True)
    got = got.reshape(slots, 256)
    got, weights = lax.optimization_barrier((got, weights))
    taps_t = conv_taps.T

    rows = exchange(jnp.broadcast_to(got[None], (SIDE, slots, 256)), feature_groups)
    step = 256
    pre = pl.pallas_call(
        pre_kernel,
        grid=(slots // step,),
        out_shape=whole((SIDE, 192, slots), BF),
        in_specs=[smem, pl.BlockSpec((SIDE, step, 256), lambda i: (0, i, 0))]
        + [pl.BlockSpec((192, 512), lambda i: (0, 0))] * SIDE,
        out_specs=pl.BlockSpec((SIDE, 192, step), lambda i: (0, 0, i)),
        compiler_params=room,
        cost_estimate=cost(800000000, 4400000),
        name="pre",
    )(at, rows, *weights)
    pre = exchange(pre, unit_groups)
    hidden = pl.pallas_call(
        gate_kernel,
        grid=(slots // step,),
        out_shape=whole((SIDE, 192, slots), BF),
        in_specs=[pl.BlockSpec((SIDE, 192, step), lambda i: (0, 0, i))],
        out_specs=pl.BlockSpec((SIDE, 192, step), lambda i: (0, 0, i)),
        compiler_params=room,
        cost_estimate=cost(3000000, 3200000),
        name="gates",
    )(pre)
    hidden = exchange(hidden, unit_groups)
    part = pl.pallas_call(
        partial_kernel,
        grid=(slots // step,),
        out_shape=whole((SIDE, slots, 128), BF),
        in_specs=[smem, pl.BlockSpec((SIDE, 192, step), lambda i: (0, 0, i))]
        + [pl.BlockSpec((192, 512), lambda i: (0, 0))] * SIDE,
        out_specs=pl.BlockSpec((SIDE, step, 128), lambda i: (0, i, 0)),
        compiler_params=room,
        cost_estimate=cost(540000000, 3400000),
        name="partial",
    )(at, hidden, *weights)
    part = exchange(part, feature_groups)
    back = jnp.sum(part.astype(F32), axis=0).astype(BF).reshape(sp_count, SLOT, 128)
    back, weights = lax.optimization_barrier((back, weights))
    relay = pl.pallas_call(
        relay_kernel,
        out_shape=(whole((256, 512), BF),) * SIDE,
        in_specs=[smem] + [vmem] * SIDE,
        out_specs=(vmem,) * SIDE,
        compiler_params=room,
        cost_estimate=cost(1000000, 2000000),
        name="relay",
    )(at, *weights)
    relay = pass_on(relay, feature_groups)
    returned = lax.all_to_all(back, SP, 0, 0, tiled=True).reshape(slots, 128)

    grads = pl.pallas_call(
        grads_kernel,
        grid=(SIDE,),
        out_shape=(whole((192, 512), BF),) * SIDE,
        in_specs=[
            smem,
            pl.BlockSpec((SIDE, 192, slots), lambda i: (0, 0, 0)),
            pl.BlockSpec((1, slots, 256), lambda i: (i, 0, 0)),
        ],
        out_specs=(pl.BlockSpec((192, 128), lambda i: (0, i)),) * SIDE,
        compiler_params=room,
        cost_estimate=cost(800000000, 4400000),
        name="grads",
    )(at, hidden, rows)
    returned, grads = lax.optimization_barrier((returned, grads))

    act_part, mine, other, stats = pl.pallas_call(
        tail_kernel,
        out_shape=(
            whole((tp_count, 80, tokens), BF),
            whole((tp_count, 32, 128), BF),
            whole((tp_count, 32, 128), BF),
            whole((2, tokens), F32),
        ),
        in_specs=[smem] + [vmem] * 3 + [pl.BlockSpec(memory_space=pltpu.HBM)] * SIDE,
        out_specs=(vmem,) * 4,
        scratch_shapes=[VM((SIDE, 256, 512), BF), pltpu.SemaphoreType.DMA((SIDE,))],
        compiler_params=room,
        cost_estimate=cost(250000000, 4500000),
        name="tail",
    )(at, pick, returned, out_cotangent, *relay)
    act_part = lax.all_to_all(act_part, TP, 0, 0, tiled=True)
    other = lax.ppermute(other, "c", [(0, 1), (1, 0)])
    proj_part = pl.pallas_call(
        add_kernel,
        out_shape=whole((tp_count, 32, 128), BF),
        in_specs=[vmem] * 2,
        out_specs=vmem,
        compiler_params=room,
        cost_estimate=cost(100000, 400000),
        name="add_core",
    )(mine, other)
    act_part, proj_part, grads = lax.optimization_barrier((act_part, proj_part, grads))
    grads = pass_on(grads, unit_groups)
    proj_part = lax.all_to_all(proj_part, "z", 0, 0, tiled=True)
    proj_sum = pl.pallas_call(
        sum_kernel,
        out_shape=whole((64, 64), BF),
        in_specs=[vmem],
        out_specs=vmem,
        compiler_params=room,
        cost_estimate=cost(100000, 200000),
        name="sum_planes",
    )(proj_part)
    side = SIDE * SIDE
    swap = [
        (z * 2 * side + c * side + t, t * 2 * side + c * side + z)
        for z in range(side)
        for c in range(2)
        for t in range(side)
    ]
    grad_proj = lax.ppermute(proj_sum, ("z",) + PLANE, swap).astype(F32)

    conv_cot, head = pl.pallas_call(
        head_kernel,
        out_shape=(whole((64, tokens), F32), whole((64, 128), F32)),
        in_specs=[vmem] * 4,
        out_specs=(vmem, vmem),
        compiler_params=room,
        cost_estimate=cost(3000000, 1200000),
        name="conv_cot",
    )(act_part, conv_t, stats, gain)
    behind = [(i + 1, i) for i in range(sp_count - 1)]
    after = lax.ppermute(head, SP, behind)
    value, gate = pl.pallas_call(
        conv_kernel,
        out_shape=(whole((64, tokens), BF), whole((64, tokens), BF)),
        in_specs=[vmem] * 5,
        out_specs=(vmem, vmem),
        scratch_shapes=[VM((64, 384), F32)],
        compiler_params=room,
        cost_estimate=cost(4000000, 400000),
        name="conv",
    )(conv_cot, after, taps_t, glu_gate.T, glu_value.T)

    grad_gate, grad_up, grad_down = pl.pallas_call(
        merge_kernel,
        out_shape=(whole((64, 2048), F32),) * 3,
        in_specs=[smem] + [vmem] * SIDE,
        out_specs=(vmem,) * 3,
        compiler_params=room,
        cost_estimate=cost(1000000, 2400000),
        name="merge_grads",
    )(at, *grads)
    return (
        grad_gate[None],
        grad_up[None],
        grad_down[None],
        grad_proj,
        value.T,
        gate.T,
    )


def solution(mesh):
    split = Mesh(mesh.devices.reshape(16, 2, SIDE, SIDE), ("z", "c", "y", "x"))
    placed = (
        P(SP, TP),
        P(SP, TP),
        P(SP, None),
        P(SP, None),
        P(SP, TP, None),
        P(SP, TP, None),
        P(SP, TP, None),
        P(SP, TP),
        P(SP, TP),
        P(SP, TP),
        P(None, TP),
        P(TP),
        P(TP, None),
    )
    return jax.shard_map(
        body,
        mesh=split,
        in_specs=placed,
        out_specs=(
            P(SP, TP, None),
            P(SP, TP, None),
            P(SP, TP, None),
            P(SP, TP),
            P(SP, TP),
            P(SP, TP),
        ),
        check_vma=False,
    )
```

```python
import jax
import jax.numpy as jnp
import numpy as np
from jax import lax
from jax.experimental import pallas as pl
from jax.experimental.pallas import tpu as pltpu
from jax.sharding import Mesh
from jax.sharding import PartitionSpec as P

NORM_EPS = 0.25
SP = ("z", "c")
TP = ("y", "x")
PLANE = ("c", "y", "x")
SIDE = 4
SLOT = 32
ROOM = 12 << 20
BF = jnp.bfloat16
F32 = jnp.float32
VM = pltpu.VMEM

NT = (((1,), (1,)), ((), ()))
TN = (((0,), (0,)), ((), ()))
NN = (((1,), (0,)), ((), ()))


def place(core, row, col):
    return core * SIDE * SIDE + row * SIDE + col


def plane_groups():
    r = range(SIDE)
    down = [[[place(k, y, x) for y in r] for x in r] for k in (0, 1)]
    across = [[[place(k, y, x) for x in r] for y in r] for k in (0, 1)]
    return down[0] + across[1], across[0] + down[1]


def step_tables():
    features, units = plane_groups()
    of_features = {p: g for g in features for p in g}
    table = np.zeros((2 * SIDE * SIDE, 64), np.int32)
    for group in units:
        for me, p in enumerate(group):
            table[p, 0] = me
            table[p, 1] = of_features[p].index(p)
            table[p, 2] = p // (SIDE * SIDE)
            for k in range(SIDE):
                ahead = of_features[group[(me + k) % SIDE]]
                back = of_features[group[(me - k) % SIDE]]
                for a in range(SIDE):
                    table[p, 16 + k * SIDE + a] = ahead[a] % (SIDE * SIDE)
                    table[p, 32 + k * SIDE + a] = back[a] % (SIDE * SIDE)
    of_units = {p: g for g in units for p in g}
    for p in range(2 * SIDE * SIDE):
        group = of_features[p]
        for j in range(SIDE):
            source = group[(group.index(p) - j) % SIDE]
            their = of_units[source]
            for k in range(SIDE):
                first = their[(their.index(source) - k) % SIDE]
                table[p, 48 + j * SIDE + k] = first % (SIDE * SIDE)
    return table


def steps_ahead(groups, k):
    return [(g[i], g[(i + k) % SIDE]) for g in groups for i in range(SIDE)]


def pass_on(parts, groups):
    return (parts[0],) + tuple(
        lax.ppermute(parts[k], PLANE, steps_ahead(groups, k)) for k in range(1, SIDE)
    )


def mm(a, b, dims):
    return lax.dot_general(a, b, dims, preferred_element_type=F32)


def exchange(v, groups):
    return lax.all_to_all(v, PLANE, 0, 0, axis_index_groups=groups, tiled=True)


def cost(flops, nbytes):
    return pl.CostEstimate(flops=flops, bytes_accessed=nbytes, transcendentals=0)


def route_kernel(rt_ref, w_ref, x_ref, c_ref, s_ref, t_ref):
    tokens = rt_ref.shape[1]
    experts = s_ref.shape[0] // SLOT
    first, second = rt_ref[0:1, :], rt_ref[1:2, :]
    ids = lax.broadcasted_iota(jnp.int32, (experts, tokens), 0)
    o0, o1 = ids == first, ids == second
    both = jnp.where(o0 | o1, 1.0, 0.0).astype(BF)
    before = lax.broadcasted_iota(jnp.int32, (tokens, tokens), 0) < lax.broadcasted_iota(
        jnp.int32, (tokens, tokens), 1
    )
    earlier = mm(both, jnp.where(before, 1.0, 0.0).astype(BF), NN)
    rank0 = jnp.sum(jnp.where(o0, earlier, 0.0), axis=0, keepdims=True)
    rank1 = jnp.sum(jnp.where(o1, earlier, 0.0), axis=0, keepdims=True)
    t0 = first * SLOT + rank0.astype(jnp.int32)
    t1 = second * SLOT + rank1.astype(jnp.int32)
    t_ref[0:1, :] = t0
    t_ref[1:2, :] = t1
    w0, w1 = w_ref[0:1, :], w_ref[1:2, :]
    x, c = x_ref[...], c_ref[...]
    size = 128
    for k in range(s_ref.shape[0] // size):
        slots = lax.broadcasted_iota(jnp.int32, (size, tokens), 0) + k * size
        m0, m1 = slots == t0, slots == t1
        pick = jnp.where(m0 | m1, 1.0, 0.0).astype(BF)
        weight = jnp.sum(
            jnp.where(m0, w0, 0.0) + jnp.where(m1, w1, 0.0), axis=1, keepdims=True
        )
        rows = pl.ds(k * size, size)
        s_ref[rows, 0:128] = mm(pick, x, NN).astype(BF)
        s_ref[rows, 128:256] = (weight * mm(pick, c, NN)).astype(BF)


def pick_kernel(t_ref, p_ref):
    slots = lax.broadcasted_iota(jnp.int32, p_ref.shape, 0)
    held = (slots == t_ref[0:1, :]) | (slots == t_ref[1:2, :])
    p_ref[...] = jnp.where(held, 1.0, 0.0).astype(BF)


def split_kernel(at_ref, g_ref, u_ref, d_ref, p_ref, c_ref, *outs):
    for k, out in enumerate(outs):
        for a in range(SIDE):
            at = at_ref[16 + k * SIDE + a]
            cols = pl.ds(pl.multiple_of(at * 128, 128), 128)
            for q, ref in enumerate((g_ref, u_ref, d_ref, p_ref)):
                out[q * 64 : q * 64 + 64, a * 128 : a * 128 + 128] = ref[:, cols]
        out[256:320, :] = c_ref[...]


def relay_kernel(at_ref, r0, r1, r2, r3, *outs):
    for j, out in enumerate(outs):
        a = lax.rem(at_ref[1] + j, SIDE)
        cols = pl.ds(pl.multiple_of(a * 128, 128), 128)
        for k, r_ref in enumerate((r0, r1, r2, r3)):
            out[k * 64 : k * 64 + 64, 0:128] = r_ref[192:256, cols]
            out[k * 64 : k * 64 + 64, 128:512] = r_ref[256:320, 128:512]


def merge_kernel(at_ref, s0, s1, s2, s3, g_ref, u_ref, d_ref):
    for k, s_ref in enumerate((s0, s1, s2, s3)):
        for a in range(SIDE):
            at = at_ref[32 + k * SIDE + a]
            cols = pl.ds(pl.multiple_of(at * 128, 128), 128)
            for q, ref in enumerate((g_ref, u_ref, d_ref)):
                ref[:, cols] = s_ref[
                    q * 64 : q * 64 + 64, a * 128 : a * 128 + 128
                ].astype(F32)


def behind_of(at_ref, k):
    return lax.rem(at_ref[0] + (SIDE - k), SIDE)


def ahead_of(at_ref, k):
    return lax.rem(at_ref[0] + k, SIDE)


def pre_kernel(at_ref, a_ref, w0, w1, w2, w3, o_ref):
    ws = (w0, w1, w2, w3)
    x = jnp.concatenate([a_ref[i, :, 0:128] for i in range(SIDE)], axis=1)
    c = jnp.concatenate([a_ref[i, :, 128:256] for i in range(SIDE)], axis=1)
    pairs = mm(jnp.concatenate([w[0:128, :] for w in ws], axis=0), x, NT)
    downs = mm(jnp.concatenate([w[128:192, :] for w in ws], axis=0), c, NT)
    for k in range(SIDE):
        b = behind_of(at_ref, k)
        o_ref[b, 0:128, :] = pairs[k * 128 : k * 128 + 128].astype(BF)
        o_ref[b, 128:192, :] = downs[k * 64 : k * 64 + 64].astype(BF)


def gate_kernel(p_ref, o_ref):
    total = p_ref[0].astype(F32)
    for b in range(1, SIDE):
        total = total + p_ref[b].astype(F32)
    gate, up, cot = total[0:64], total[64:128], total[128:192]
    s = jax.nn.sigmoid(gate)
    act = gate * s
    hidden = (act * up).astype(BF)
    up_cot = (cot * act).astype(BF)
    gate_cot = (cot * up * s * (1.0 + gate * (1.0 - s))).astype(BF)
    for b in range(SIDE):
        o_ref[b, 0:64, :] = gate_cot
        o_ref[b, 64:128, :] = up_cot
        o_ref[b, 128:192, :] = hidden


def partial_kernel(at_ref, h_ref, w0, w1, w2, w3, o_ref):
    ws = (w0, w1, w2, w3)
    h = jnp.concatenate([h_ref[behind_of(at_ref, k), 0:128, :] for k in range(SIDE)], axis=0)
    w = jnp.concatenate([w_ref[0:128, :] for w_ref in ws], axis=0)
    total = mm(h, w, TN)
    for a in range(SIDE):
        o_ref[a] = total[:, a * 128 : a * 128 + 128].astype(BF)


def grads_kernel(at_ref, h_ref, a_ref, *outs):
    x, c = a_ref[0, :, 0:128], a_ref[0, :, 128:256]
    for k, out in enumerate(outs):
        b = ahead_of(at_ref, k)
        out[0:128, :] = mm(h_ref[b, 0:128, :], x, NN).astype(BF)
        out[128:192, :] = mm(h_ref[b, 128:192, :], c, NN).astype(BF)


def total_kernel(
    at_ref, p_ref, r_ref, c_ref, q0, q1, q2, q3, mine_ref, other_ref, total_ref, stats_ref
):
    qs = (q0, q1, q2, q3)
    moe = mm(p_ref[...], r_ref[...], TN)
    total = (c_ref[...].astype(F32) + moe).astype(BF)
    tokens = total.shape[0]
    total_ref[0:tokens, :] = total
    total_ref[tokens:, :] = jnp.zeros((total_ref.shape[0] - tokens, 128), BF)
    size = q0.shape[0]
    channels = SIDE * size
    mean = jnp.zeros((1, tokens), F32)
    for q in qs:
        conv = q[:, 128 : 128 + tokens].astype(F32)
        mean = mean + jnp.sum(conv, axis=0, keepdims=True)
    mean = mean / channels
    var = jnp.zeros((1, tokens), F32)
    for q in qs:
        off = q[:, 128 : 128 + tokens].astype(F32) - mean
        var = var + jnp.sum(off * off, axis=0, keepdims=True)
    inv = lax.rsqrt(var / channels + NORM_EPS)
    stats_ref[0:1, :] = mean
    stats_ref[1:2, :] = inv
    own = jnp.full((64, 128), at_ref[2], jnp.int32) == 0
    for j, q in enumerate(qs):
        normed = (q[:, 128 : 128 + tokens].astype(F32) - mean) * inv
        linear = normed * gain_of(q)
        act = (linear * jax.nn.sigmoid(linear)).astype(BF)
        grad = mm(act, total, NN)
        turned = pltpu.roll(grad, 64, 1)
        for k in range(SIDE):
            b = at_ref[48 + j * SIDE + k]
            rows = slice(k * 64, k * 64 + 64)
            mine_ref[b] = jnp.where(own, turned[rows], grad[rows]).astype(BF)
            other_ref[b] = jnp.where(own, grad[rows], turned[rows]).astype(BF)


def gain_of(q):
    lane = lax.broadcasted_iota(jnp.int32, (q.shape[0], 128), 1)
    pieces = jnp.where((lane >= 64) & (lane < 67), q[:, 384:512].astype(F32), 0.0)
    return jnp.sum(pieces, axis=1, keepdims=True)


def cot_kernel(at_ref, total_ref, stats_ref, q0, q1, q2, q3, o_ref):
    wide = total_ref.shape[0]
    tokens = stats_ref.shape[1]
    total = total_ref[...]
    mean, inv = stats_ref[0:1, :], stats_ref[1:2, :]
    first = jnp.zeros((1, tokens), F32)
    second = jnp.zeros((1, tokens), F32)
    for j, q in enumerate((q0, q1, q2, q3)):
        normed = (q[:, 128 : 128 + tokens].astype(F32) - mean) * inv
        gain = gain_of(q)
        linear = normed * gain
        s = jax.nn.sigmoid(linear)
        cot = mm(q[:, 0:128], total, NT)
        sloped = cot[:, 0:tokens] * (s * (1.0 + linear * (1.0 - s)) * gain)
        first = first + jnp.sum(sloped, axis=0, keepdims=True)
        second = second + jnp.sum(sloped * normed, axis=0, keepdims=True)
        for k in range(SIDE):
            o_ref[at_ref[48 + j * SIDE + k], 0:64, :] = cot[k * 64 : k * 64 + 64].astype(BF)
    row = lax.broadcasted_iota(jnp.int32, (16, tokens), 0)
    sums = jnp.zeros((16, tokens), F32)
    for i, v in enumerate((first, second)):
        head = v.astype(BF).astype(F32)
        sums = jnp.where(row == 2 * i, head, jnp.where(row == 2 * i + 1, v - head, sums))
    for b in range(o_ref.shape[0]):
        o_ref[b, 64:80, 0:tokens] = sums.astype(BF)
        o_ref[b, 64:80, tokens:wide] = jnp.zeros((16, wide - tokens), BF)


def join_kernel(a_ref, mine_ref, other_ref, o_ref):
    low = lax.broadcasted_iota(jnp.int32, (64, 128), 1) < 64
    for b in range(o_ref.shape[0]):
        piece = mine_ref[b].astype(F32) + other_ref[b].astype(F32)
        o_ref[b, 0:64, :] = jnp.where(low, a_ref[b, 0:64, :].astype(F32), piece).astype(BF)
        o_ref[b, 64:80, :] = a_ref[b, 64:80, :]


def part_kernel(r_ref, o_ref):
    low = lax.broadcasted_iota(jnp.int32, (32, 128), 1) < 64
    for b in range(o_ref.shape[0]):
        upper = pltpu.roll(r_ref[b, 0:32, 256:384].astype(F32), 64, 1)
        lower = r_ref[b, 32:64, 256:384].astype(F32)
        o_ref[b] = jnp.where(low, upper, lower).astype(BF)


def head_kernel(r_ref, conv_ref, stats_ref, gain_ref, o_ref, h_ref):
    tokens = conv_ref.shape[1]
    total = r_ref[0, :, 0:tokens].astype(F32)
    for b in range(1, r_ref.shape[0]):
        total = total + r_ref[b, :, 0:tokens].astype(F32)
    channels = 16 * conv_ref.shape[0]
    first = (total[64:65] + total[65:66]) / channels
    second = (total[66:67] + total[67:68]) / channels
    inv = stats_ref[1:2, :]
    normed = (conv_ref[...].astype(F32) - stats_ref[0:1, :]) * inv
    gain = gain_ref[...]
    linear = normed * gain
    s = jax.nn.sigmoid(linear)
    cot = total[0:64] * s * (1.0 + linear * (1.0 - s)) * gain
    cot = inv * (cot - first - normed * second)
    o_ref[...] = cot
    h_ref[...] = cot[:, 0:128]


def sum_kernel(a_ref, o_ref):
    total = a_ref[0].astype(F32)
    for b in range(1, a_ref.shape[0]):
        total = total + a_ref[b].astype(F32)
    turned = pltpu.roll(total, 64, 1)
    block = jnp.concatenate([total, turned], axis=0)
    o_ref[...] = block.T[0:64, :]


def sum_side_kernel(p_ref, o_ref):
    total = p_ref[0].astype(F32)
    for a in range(1, SIDE):
        total = total + p_ref[a].astype(F32)
    o_ref[...] = total.astype(BF)


def conv_kernel(cot_ref, next_ref, taps_ref, gate_ref, value_ref, v_ref, g_ref, buf):
    rows, tokens = cot_ref.shape
    wide = buf.shape[1]
    reach = taps_ref.shape[1] - 1
    buf[:, 0:128] = next_ref[...]
    buf[:, 128:wide] = jnp.zeros((rows, wide - 128), F32)
    after = pltpu.roll(buf[...], tokens, 1)
    buf[:, 0:tokens] = cot_ref[...]
    lane = lax.broadcasted_iota(jnp.int32, (rows, wide), 1)
    whole = jnp.where(lane < tokens, buf[...], after)
    taps = taps_ref[...]
    total = whole * taps[:, reach : reach + 1]
    for s in range(1, reach + 1):
        total = total + pltpu.roll(whole, wide - s, 1) * taps[:, reach - s : reach - s + 1]
    cot = total[:, 0:tokens]
    s = jax.nn.sigmoid(gate_ref[...].astype(F32))
    v_ref[...] = (cot * s).astype(BF)
    g_ref[...] = (cot * value_ref[...].astype(F32) * s * (1.0 - s)).astype(BF)


def whole(shape, dtype):
    return jax.ShapeDtypeStruct(shape, dtype)


def body(
    moe_input,
    out_cotangent,
    routes,
    route_weight,
    gate_weight,
    up_weight,
    down_weight,
    glu_value,
    glu_gate,
    conv_result,
    conv_taps,
    norm_gain,
    proj_weight,
):
    sp_count = lax.axis_size(SP)
    tp_count = lax.axis_size(TP)
    tokens = moe_input.shape[0]
    slots = sp_count * SLOT
    feature_groups, unit_groups = plane_groups()
    smem = pl.BlockSpec(memory_space=pltpu.SMEM)
    vmem = pl.BlockSpec(memory_space=VM)
    room = pltpu.CompilerParams(vmem_limit_bytes=ROOM)

    sent, target = pl.pallas_call(
        route_kernel,
        out_shape=(whole((slots, 256), BF), whole((2, tokens), jnp.int32)),
        in_specs=[vmem] * 4,
        out_specs=(vmem, vmem),
        cost_estimate=cost(400000000, 2000000),
        name="route",
    )(routes.T, route_weight.T, moe_input, out_cotangent)
    sent, target, table, gate_weight, conv_result, norm_gain = lax.optimization_barrier(
        (sent, target, jnp.asarray(step_tables()), gate_weight, conv_result, norm_gain)
    )
    at = table[lax.axis_index(PLANE)]
    pick = pl.pallas_call(
        pick_kernel,
        out_shape=whole((slots, tokens), BF),
        in_specs=[vmem],
        out_specs=vmem,
        compiler_params=room,
        cost_estimate=cost(1000000, 700000),
        name="pick",
    )(target)
    conv_t = conv_result.T
    gain = norm_gain.reshape(-1, 1)
    high = lax.reduce_precision(gain, 8, 7)
    middle = lax.reduce_precision(gain - high, 8, 7)
    pieces = jnp.concatenate([high, middle, gain - high - middle], axis=1).astype(BF)
    channel_part = jnp.concatenate(
        [jnp.zeros((64, 128), BF), conv_t, pieces, jnp.zeros((64, 61), BF)], axis=1
    )
    split = pl.pallas_call(
        split_kernel,
        out_shape=(whole((320, 512), BF),) * SIDE,
        in_specs=[smem] + [vmem] * 5,
        out_specs=(vmem,) * SIDE,
        compiler_params=room,
        cost_estimate=cost(1000000, 2600000),
        name="split_weights",
    )(at, gate_weight[0], up_weight[0], down_weight[0], proj_weight, channel_part)
    weights = pass_on(split, unit_groups)
    got = lax.all_to_all(sent.reshape(sp_count, SLOT, 256), SP, 0, 0, tiled=True)
    got = got.reshape(slots, 256)
    got, weights = lax.optimization_barrier((got, weights))
    taps_t = conv_taps.T

    rows = exchange(jnp.broadcast_to(got[None], (SIDE, slots, 256)), feature_groups)
    step = 256
    pre = pl.pallas_call(
        pre_kernel,
        grid=(slots // step,),
        out_shape=whole((SIDE, 192, slots), BF),
        in_specs=[smem, pl.BlockSpec((SIDE, step, 256), lambda i: (0, i, 0))]
        + [pl.BlockSpec((192, 512), lambda i: (0, 0))] * SIDE,
        out_specs=pl.BlockSpec((SIDE, 192, step), lambda i: (0, 0, i)),
        compiler_params=room,
        cost_estimate=cost(800000000, 4400000),
        name="pre",
    )(at, rows, *weights)
    pre = exchange(pre, unit_groups)
    hidden = pl.pallas_call(
        gate_kernel,
        grid=(slots // step,),
        out_shape=whole((SIDE, 192, slots), BF),
        in_specs=[pl.BlockSpec((SIDE, 192, step), lambda i: (0, 0, i))],
        out_specs=pl.BlockSpec((SIDE, 192, step), lambda i: (0, 0, i)),
        compiler_params=room,
        cost_estimate=cost(3000000, 3200000),
        name="gates",
    )(pre)
    hidden = exchange(hidden, unit_groups)
    part = pl.pallas_call(
        partial_kernel,
        grid=(slots // step,),
        out_shape=whole((SIDE, slots, 128), BF),
        in_specs=[smem, pl.BlockSpec((SIDE, 192, step), lambda i: (0, 0, i))]
        + [pl.BlockSpec((192, 512), lambda i: (0, 0))] * SIDE,
        out_specs=pl.BlockSpec((SIDE, step, 128), lambda i: (0, i, 0)),
        compiler_params=room,
        cost_estimate=cost(540000000, 3400000),
        name="partial",
    )(at, hidden, *weights)
    part = exchange(part, feature_groups)
    back = pl.pallas_call(
        sum_side_kernel,
        out_shape=whole((slots, 128), BF),
        in_specs=[vmem],
        out_specs=vmem,
        compiler_params=room,
        cost_estimate=cost(1000000, 1300000),
        name="sum_side",
    )(part).reshape(sp_count, SLOT, 128)
    back, weights = lax.optimization_barrier((back, weights))
    relay = pl.pallas_call(
        relay_kernel,
        out_shape=(whole((256, 512), BF),) * SIDE,
        in_specs=[smem] + [vmem] * SIDE,
        out_specs=(vmem,) * SIDE,
        compiler_params=room,
        cost_estimate=cost(1000000, 2000000),
        name="relay",
    )(at, *weights)
    relay = pass_on(relay, feature_groups)
    returned = lax.all_to_all(back, SP, 0, 0, tiled=True).reshape(slots, 128)

    grads = pl.pallas_call(
        grads_kernel,
        grid=(SIDE,),
        out_shape=(whole((192, 512), BF),) * SIDE,
        in_specs=[
            smem,
            pl.BlockSpec((SIDE, 192, slots), lambda i: (0, 0, 0)),
            pl.BlockSpec((1, slots, 256), lambda i: (i, 0, 0)),
        ],
        out_specs=(pl.BlockSpec((192, 128), lambda i: (0, i)),) * SIDE,
        compiler_params=room,
        cost_estimate=cost(800000000, 4400000),
        name="grads",
    )(at, hidden, rows)
    returned, grads = lax.optimization_barrier((returned, grads))

    wide = 384
    mine, other, total_cot, stats = pl.pallas_call(
        total_kernel,
        out_shape=(
            whole((tp_count, 64, 128), BF),
            whole((tp_count, 64, 128), BF),
            whole((wide, 128), BF),
            whole((2, tokens), F32),
        ),
        in_specs=[smem] + [vmem] * 7,
        out_specs=(vmem,) * 4,
        compiler_params=room,
        cost_estimate=cost(170000000, 2500000),
        name="total_cot",
    )(at, pick, returned, out_cotangent, *relay)
    other = lax.ppermute(other, "c", [(0, 1), (1, 0)])
    act_part = pl.pallas_call(
        cot_kernel,
        out_shape=whole((tp_count, 80, wide), BF),
        in_specs=[smem] + [vmem] * 6,
        out_specs=vmem,
        compiler_params=room,
        cost_estimate=cost(100000000, 2500000),
        name="act_cot",
    )(at, total_cot, stats, *relay)
    act_part = pl.pallas_call(
        join_kernel,
        grid=(1,),
        out_shape=whole((tp_count, 80, wide), BF),
        in_specs=[
            pl.BlockSpec((tp_count, 80, 128), lambda i: (0, 0, 2)),
            pl.BlockSpec((tp_count, 64, 128), lambda i: (0, 0, 0)),
            pl.BlockSpec((tp_count, 64, 128), lambda i: (0, 0, 0)),
        ],
        out_specs=pl.BlockSpec((tp_count, 80, 128), lambda i: (0, 0, 2)),
        input_output_aliases={0: 0},
        compiler_params=room,
        cost_estimate=cost(100000, 1200000),
        name="join_cores",
    )(act_part, mine, other)
    act_part = lax.all_to_all(act_part, TP, 0, 0, tiled=True)
    proj_part = pl.pallas_call(
        part_kernel,
        out_shape=whole((tp_count, 32, 128), BF),
        in_specs=[vmem],
        out_specs=vmem,
        compiler_params=room,
        cost_estimate=cost(100000, 400000),
        name="proj_part",
    )(act_part)
    act_part, proj_part, grads = lax.optimization_barrier((act_part, proj_part, grads))
    grads = pass_on(grads, unit_groups)
    proj_part = lax.all_to_all(proj_part, "z", 0, 0, tiled=True)
    grad_proj = pl.pallas_call(
        sum_kernel,
        out_shape=whole((64, 64), F32),
        in_specs=[vmem],
        out_specs=vmem,
        compiler_params=room,
        cost_estimate=cost(100000, 200000),
        name="sum_planes",
    )(proj_part)

    conv_cot, head = pl.pallas_call(
        head_kernel,
        out_shape=(whole((64, tokens), F32), whole((64, 128), F32)),
        in_specs=[vmem] * 4,
        out_specs=(vmem, vmem),
        compiler_params=room,
        cost_estimate=cost(3000000, 1200000),
        name="conv_cot",
    )(act_part, conv_t, stats, gain)
    behind = [(i + 1, i) for i in range(sp_count - 1)]
    after = lax.ppermute(head, SP, behind)
    value, gate = pl.pallas_call(
        conv_kernel,
        out_shape=(whole((64, tokens), BF), whole((64, tokens), BF)),
        in_specs=[vmem] * 5,
        out_specs=(vmem, vmem),
        scratch_shapes=[VM((64, 384), F32)],
        compiler_params=room,
        cost_estimate=cost(4000000, 400000),
        name="conv",
    )(conv_cot, after, taps_t, glu_gate.T, glu_value.T)

    grad_gate, grad_up, grad_down = pl.pallas_call(
        merge_kernel,
        out_shape=(whole((64, 2048), F32),) * 3,
        in_specs=[smem] + [vmem] * SIDE,
        out_specs=(vmem,) * 3,
        compiler_params=room,
        cost_estimate=cost(1000000, 2400000),
        name="merge_grads",
    )(at, *grads)
    return (
        grad_gate[None],
        grad_up[None],
        grad_down[None],
        grad_proj,
        value.T,
        gate.T,
    )


def solution(mesh):
    split = Mesh(mesh.devices.reshape(16, 2, SIDE, SIDE), ("z", "c", "y", "x"))
    placed = (
        P(SP, TP),
        P(SP, TP),
        P(SP, None),
        P(SP, None),
        P(SP, TP, None),
        P(SP, TP, None),
        P(SP, TP, None),
        P(SP, TP),
        P(SP, TP),
        P(SP, TP),
        P(None, TP),
        P(TP),
        P(TP, None),
    )
    return jax.shard_map(
        body,
        mesh=split,
        in_specs=placed,
        out_specs=(
            P(SP, TP, None),
            P(SP, TP, None),
            P(SP, TP, None),
            P(SP, TP),
            P(SP, TP),
            P(SP, TP),
        ),
        check_vma=False,
    )
```

```python
import jax
import jax.numpy as jnp
import numpy as np
from jax import lax
from jax.experimental import pallas as pl
from jax.experimental.pallas import tpu as pltpu
from jax.sharding import Mesh
from jax.sharding import PartitionSpec as P

NORM_EPS = 0.25
SP = ("z", "c")
TP = ("y", "x")
PLANE = ("c", "y", "x")
SIDE = 4
SLOT = 32
ROOM = 12 << 20
BF = jnp.bfloat16
F32 = jnp.float32
VM = pltpu.VMEM

NT = (((1,), (1,)), ((), ()))
TN = (((0,), (0,)), ((), ()))
NN = (((1,), (0,)), ((), ()))


def place(core, row, col):
    return core * SIDE * SIDE + row * SIDE + col


def plane_groups():
    r = range(SIDE)
    down = [[[place(k, y, x) for y in r] for x in r] for k in (0, 1)]
    across = [[[place(k, y, x) for x in r] for y in r] for k in (0, 1)]
    return down[0] + across[1], across[0] + down[1]


def step_tables():
    features, units = plane_groups()
    of_features = {p: g for g in features for p in g}
    table = np.zeros((2 * SIDE * SIDE, 64), np.int32)
    for group in units:
        for me, p in enumerate(group):
            table[p, 0] = me
            table[p, 1] = of_features[p].index(p)
            table[p, 2] = p // (SIDE * SIDE)
            for k in range(SIDE):
                ahead = of_features[group[(me + k) % SIDE]]
                back = of_features[group[(me - k) % SIDE]]
                for a in range(SIDE):
                    table[p, 16 + k * SIDE + a] = ahead[a] % (SIDE * SIDE)
                    table[p, 32 + k * SIDE + a] = back[a] % (SIDE * SIDE)
    of_units = {p: g for g in units for p in g}
    for p in range(2 * SIDE * SIDE):
        group = of_features[p]
        for j in range(SIDE):
            source = group[(group.index(p) - j) % SIDE]
            their = of_units[source]
            for k in range(SIDE):
                first = their[(their.index(source) - k) % SIDE]
                table[p, 48 + j * SIDE + k] = first % (SIDE * SIDE)
    return table


def steps_ahead(groups, k):
    return [(g[i], g[(i + k) % SIDE]) for g in groups for i in range(SIDE)]


def pass_on(parts, groups):
    return (parts[0],) + tuple(
        lax.ppermute(parts[k], PLANE, steps_ahead(groups, k)) for k in range(1, SIDE)
    )


def mm(a, b, dims):
    return lax.dot_general(a, b, dims, preferred_element_type=F32)


def exchange(v, groups):
    return lax.all_to_all(v, PLANE, 0, 0, axis_index_groups=groups, tiled=True)


def cost(flops, nbytes):
    return pl.CostEstimate(flops=flops, bytes_accessed=nbytes, transcendentals=0)


def route_kernel(rt_ref, w_ref, x_ref, c_ref, s_ref, t_ref):
    tokens = rt_ref.shape[1]
    experts = s_ref.shape[0] // SLOT
    first, second = rt_ref[0:1, :], rt_ref[1:2, :]
    ids = lax.broadcasted_iota(jnp.int32, (experts, tokens), 0)
    o0, o1 = ids == first, ids == second
    both = jnp.where(o0 | o1, 1.0, 0.0).astype(BF)
    before = lax.broadcasted_iota(jnp.int32, (tokens, tokens), 0) < lax.broadcasted_iota(
        jnp.int32, (tokens, tokens), 1
    )
    earlier = mm(both, jnp.where(before, 1.0, 0.0).astype(BF), NN)
    rank0 = jnp.sum(jnp.where(o0, earlier, 0.0), axis=0, keepdims=True)
    rank1 = jnp.sum(jnp.where(o1, earlier, 0.0), axis=0, keepdims=True)
    t0 = first * SLOT + rank0.astype(jnp.int32)
    t1 = second * SLOT + rank1.astype(jnp.int32)
    t_ref[0:1, :] = t0
    t_ref[1:2, :] = t1
    w0, w1 = w_ref[0:1, :], w_ref[1:2, :]
    x, c = x_ref[...], c_ref[...]
    size = 128
    for k in range(s_ref.shape[0] // size):
        slots = lax.broadcasted_iota(jnp.int32, (size, tokens), 0) + k * size
        m0, m1 = slots == t0, slots == t1
        pick = jnp.where(m0 | m1, 1.0, 0.0).astype(BF)
        weight = jnp.sum(
            jnp.where(m0, w0, 0.0) + jnp.where(m1, w1, 0.0), axis=1, keepdims=True
        )
        rows = pl.ds(k * size, size)
        s_ref[rows, 0:128] = mm(pick, x, NN).astype(BF)
        s_ref[rows, 128:256] = (weight * mm(pick, c, NN)).astype(BF)


def pick_kernel(t_ref, p_ref):
    slots = lax.broadcasted_iota(jnp.int32, p_ref.shape, 0)
    held = (slots == t_ref[0:1, :]) | (slots == t_ref[1:2, :])
    p_ref[...] = jnp.where(held, 1.0, 0.0).astype(BF)


def split_kernel(at_ref, g_ref, u_ref, d_ref, p_ref, c_ref, *outs):
    for k, out in enumerate(outs):
        for a in range(SIDE):
            at = at_ref[16 + k * SIDE + a]
            cols = pl.ds(pl.multiple_of(at * 128, 128), 128)
            for q, ref in enumerate((g_ref, u_ref, d_ref, p_ref)):
                out[q * 64 : q * 64 + 64, a * 128 : a * 128 + 128] = ref[:, cols]
        out[256:320, :] = c_ref[...]


def relay_kernel(at_ref, r0, r1, r2, r3, *outs):
    for j, out in enumerate(outs):
        a = lax.rem(at_ref[1] + j, SIDE)
        cols = pl.ds(pl.multiple_of(a * 128, 128), 128)
        for k, r_ref in enumerate((r0, r1, r2, r3)):
            out[k * 64 : k * 64 + 64, 0:128] = r_ref[192:256, cols]
            out[k * 64 : k * 64 + 64, 128:512] = r_ref[256:320, 128:512]


def merge_kernel(at_ref, s0, s1, s2, s3, g_ref, u_ref, d_ref):
    for k, s_ref in enumerate((s0, s1, s2, s3)):
        for a in range(SIDE):
            at = at_ref[32 + k * SIDE + a]
            cols = pl.ds(pl.multiple_of(at * 128, 128), 128)
            for q, ref in enumerate((g_ref, u_ref, d_ref)):
                ref[:, cols] = s_ref[
                    q * 64 : q * 64 + 64, a * 128 : a * 128 + 128
                ].astype(F32)


def behind_of(at_ref, k):
    return lax.rem(at_ref[0] + (SIDE - k), SIDE)


def ahead_of(at_ref, k):
    return lax.rem(at_ref[0] + k, SIDE)


def pre_kernel(at_ref, a_ref, w0, w1, w2, w3, o_ref):
    ws = (w0, w1, w2, w3)
    x = jnp.concatenate([a_ref[i, :, 0:128] for i in range(SIDE)], axis=1)
    c = jnp.concatenate([a_ref[i, :, 128:256] for i in range(SIDE)], axis=1)
    pairs = mm(jnp.concatenate([w[0:128, :] for w in ws], axis=0), x, NT)
    downs = mm(jnp.concatenate([w[128:192, :] for w in ws], axis=0), c, NT)
    for k in range(SIDE):
        b = behind_of(at_ref, k)
        o_ref[b, 0:128, :] = pairs[k * 128 : k * 128 + 128].astype(BF)
        o_ref[b, 128:192, :] = downs[k * 64 : k * 64 + 64].astype(BF)


def gate_kernel(p_ref, o_ref):
    total = p_ref[0].astype(F32)
    for b in range(1, SIDE):
        total = total + p_ref[b].astype(F32)
    gate, up, cot = total[0:64], total[64:128], total[128:192]
    s = jax.nn.sigmoid(gate)
    act = gate * s
    hidden = (act * up).astype(BF)
    up_cot = (cot * act).astype(BF)
    gate_cot = (cot * up * s * (1.0 + gate * (1.0 - s))).astype(BF)
    for b in range(SIDE):
        o_ref[b, 0:64, :] = gate_cot
        o_ref[b, 64:128, :] = up_cot
        o_ref[b, 128:192, :] = hidden


def partial_kernel(at_ref, h_ref, w0, w1, w2, w3, o_ref):
    ws = (w0, w1, w2, w3)
    h = jnp.concatenate([h_ref[behind_of(at_ref, k), 0:128, :] for k in range(SIDE)], axis=0)
    w = jnp.concatenate([w_ref[0:128, :] for w_ref in ws], axis=0)
    total = mm(h, w, TN)
    for a in range(SIDE):
        o_ref[a] = total[:, a * 128 : a * 128 + 128].astype(BF)


def grads_kernel(at_ref, h_ref, a_ref, *outs):
    x, c = a_ref[0, :, 0:128], a_ref[0, :, 128:256]
    for k, out in enumerate(outs):
        b = ahead_of(at_ref, k)
        out[0:128, :] = mm(h_ref[b, 0:128, :], x, NN).astype(BF)
        out[128:192, :] = mm(h_ref[b, 128:192, :], c, NN).astype(BF)


def total_kernel(
    at_ref, p_ref, r_ref, c_ref, q0, q1, q2, q3, mine_ref, other_ref, total_ref, stats_ref
):
    qs = (q0, q1, q2, q3)
    moe = mm(p_ref[...], r_ref[...], TN)
    total = (c_ref[...].astype(F32) + moe).astype(BF)
    tokens = total.shape[0]
    total_ref[0:tokens, :] = total
    total_ref[tokens:, :] = jnp.zeros((total_ref.shape[0] - tokens, 128), BF)
    size = q0.shape[0]
    channels = SIDE * size
    mean = jnp.zeros((1, tokens), F32)
    for q in qs:
        conv = q[:, 128 : 128 + tokens].astype(F32)
        mean = mean + jnp.sum(conv, axis=0, keepdims=True)
    mean = mean / channels
    var = jnp.zeros((1, tokens), F32)
    for q in qs:
        off = q[:, 128 : 128 + tokens].astype(F32) - mean
        var = var + jnp.sum(off * off, axis=0, keepdims=True)
    inv = lax.rsqrt(var / channels + NORM_EPS)
    stats_ref[0:1, :] = mean
    stats_ref[1:2, :] = inv
    own = jnp.full((64, 128), at_ref[2], jnp.int32) == 0
    for j, q in enumerate(qs):
        normed = (q[:, 128 : 128 + tokens].astype(F32) - mean) * inv
        linear = normed * gain_of(q)
        act = (linear * jax.nn.sigmoid(linear)).astype(BF)
        grad = mm(act, total, NN)
        turned = pltpu.roll(grad, 64, 1)
        for k in range(SIDE):
            b = at_ref[48 + j * SIDE + k]
            rows = slice(k * 64, k * 64 + 64)
            mine_ref[b] = jnp.where(own, turned[rows], grad[rows]).astype(BF)
            other_ref[b] = jnp.where(own, grad[rows], turned[rows]).astype(BF)


def gain_of(q):
    lane = lax.broadcasted_iota(jnp.int32, (q.shape[0], 128), 1)
    pieces = jnp.where((lane >= 64) & (lane < 67), q[:, 384:512].astype(F32), 0.0)
    return jnp.sum(pieces, axis=1, keepdims=True)


def cot_kernel(at_ref, total_ref, stats_ref, q0, q1, q2, q3, o_ref):
    wide = total_ref.shape[0]
    tokens = stats_ref.shape[1]
    total = total_ref[...]
    mean, inv = stats_ref[0:1, :], stats_ref[1:2, :]
    first = jnp.zeros((1, tokens), F32)
    second = jnp.zeros((1, tokens), F32)
    for j, q in enumerate((q0, q1, q2, q3)):
        normed = (q[:, 128 : 128 + tokens].astype(F32) - mean) * inv
        gain = gain_of(q)
        linear = normed * gain
        s = jax.nn.sigmoid(linear)
        cot = mm(q[:, 0:128], total, NT)
        sloped = cot[:, 0:tokens] * (s * (1.0 + linear * (1.0 - s)) * gain)
        first = first + jnp.sum(sloped, axis=0, keepdims=True)
        second = second + jnp.sum(sloped * normed, axis=0, keepdims=True)
        for k in range(SIDE):
            o_ref[at_ref[48 + j * SIDE + k], 0:64, :] = cot[k * 64 : k * 64 + 64].astype(BF)
    row = lax.broadcasted_iota(jnp.int32, (8, tokens), 0)
    sums = jnp.zeros((8, tokens), F32)
    for i, v in enumerate((first, second)):
        head = v.astype(BF).astype(F32)
        sums = jnp.where(row == 2 * i, head, jnp.where(row == 2 * i + 1, v - head, sums))
    for b in range(o_ref.shape[0]):
        o_ref[b, 64:72, 0:tokens] = sums.astype(BF)
        o_ref[b, 64:72, tokens:wide] = jnp.zeros((8, wide - tokens), BF)


def join_kernel(a_ref, mine_ref, other_ref, o_ref):
    low = lax.broadcasted_iota(jnp.int32, (64, 128), 1) < 64
    for b in range(o_ref.shape[0]):
        piece = mine_ref[b].astype(F32) + other_ref[b].astype(F32)
        o_ref[b, 0:64, :] = jnp.where(low, a_ref[b, 0:64, :].astype(F32), piece).astype(BF)
        o_ref[b, 64:72, :] = a_ref[b, 64:72, :]


def part_kernel(r_ref, o_ref):
    low = lax.broadcasted_iota(jnp.int32, (32, 128), 1) < 64
    for b in range(o_ref.shape[0]):
        upper = pltpu.roll(r_ref[b, 0:32, 256:384].astype(F32), 64, 1)
        lower = r_ref[b, 32:64, 256:384].astype(F32)
        o_ref[b] = jnp.where(low, upper, lower).astype(BF)


def head_kernel(r_ref, conv_ref, stats_ref, gain_ref, o_ref, h_ref):
    tokens = conv_ref.shape[1]
    total = r_ref[0, :, 0:tokens].astype(F32)
    for b in range(1, r_ref.shape[0]):
        total = total + r_ref[b, :, 0:tokens].astype(F32)
    channels = 16 * conv_ref.shape[0]
    first = (total[64:65] + total[65:66]) / channels
    second = (total[66:67] + total[67:68]) / channels
    inv = stats_ref[1:2, :]
    normed = (conv_ref[...].astype(F32) - stats_ref[0:1, :]) * inv
    gain = gain_ref[...]
    linear = normed * gain
    s = jax.nn.sigmoid(linear)
    cot = total[0:64] * s * (1.0 + linear * (1.0 - s)) * gain
    cot = inv * (cot - first - normed * second)
    o_ref[...] = cot
    h_ref[...] = cot[:, 0:128]


def sum_kernel(a_ref, o_ref):
    total = a_ref[0].astype(F32)
    for b in range(1, a_ref.shape[0]):
        total = total + a_ref[b].astype(F32)
    turned = pltpu.roll(total, 64, 1)
    block = jnp.concatenate([total, turned], axis=0)
    o_ref[...] = block.T[0:64, :]


def sum_side_kernel(p_ref, o_ref):
    total = p_ref[0].astype(F32)
    for a in range(1, SIDE):
        total = total + p_ref[a].astype(F32)
    o_ref[...] = total.astype(BF)


def conv_kernel(cot_ref, next_ref, taps_ref, gate_ref, value_ref, v_ref, g_ref, buf):
    rows, tokens = cot_ref.shape
    wide = buf.shape[1]
    reach = taps_ref.shape[1] - 1
    buf[:, 0:128] = next_ref[...]
    buf[:, 128:wide] = jnp.zeros((rows, wide - 128), F32)
    after = pltpu.roll(buf[...], tokens, 1)
    buf[:, 0:tokens] = cot_ref[...]
    lane = lax.broadcasted_iota(jnp.int32, (rows, wide), 1)
    whole = jnp.where(lane < tokens, buf[...], after)
    taps = taps_ref[...]
    total = whole * taps[:, reach : reach + 1]
    for s in range(1, reach + 1):
        total = total + pltpu.roll(whole, wide - s, 1) * taps[:, reach - s : reach - s + 1]
    cot = total[:, 0:tokens]
    s = jax.nn.sigmoid(gate_ref[...].astype(F32))
    v_ref[...] = (cot * s).astype(BF)
    g_ref[...] = (cot * value_ref[...].astype(F32) * s * (1.0 - s)).astype(BF)


def whole(shape, dtype):
    return jax.ShapeDtypeStruct(shape, dtype)


def body(
    moe_input,
    out_cotangent,
    routes,
    route_weight,
    gate_weight,
    up_weight,
    down_weight,
    glu_value,
    glu_gate,
    conv_result,
    conv_taps,
    norm_gain,
    proj_weight,
):
    sp_count = lax.axis_size(SP)
    tp_count = lax.axis_size(TP)
    tokens = moe_input.shape[0]
    slots = sp_count * SLOT
    feature_groups, unit_groups = plane_groups()
    smem = pl.BlockSpec(memory_space=pltpu.SMEM)
    vmem = pl.BlockSpec(memory_space=VM)
    room = pltpu.CompilerParams(vmem_limit_bytes=ROOM)

    sent, target = pl.pallas_call(
        route_kernel,
        out_shape=(whole((slots, 256), BF), whole((2, tokens), jnp.int32)),
        in_specs=[vmem] * 4,
        out_specs=(vmem, vmem),
        cost_estimate=cost(400000000, 2000000),
        name="route",
    )(routes.T, route_weight.T, moe_input, out_cotangent)
    sent, target, table, gate_weight, conv_result, norm_gain = lax.optimization_barrier(
        (sent, target, jnp.asarray(step_tables()), gate_weight, conv_result, norm_gain)
    )
    at = table[lax.axis_index(PLANE)]
    pick = pl.pallas_call(
        pick_kernel,
        out_shape=whole((slots, tokens), BF),
        in_specs=[vmem],
        out_specs=vmem,
        compiler_params=room,
        cost_estimate=cost(1000000, 700000),
        name="pick",
    )(target)
    conv_t = conv_result.T
    gain = norm_gain.reshape(-1, 1)
    high = lax.reduce_precision(gain, 8, 7)
    middle = lax.reduce_precision(gain - high, 8, 7)
    pieces = jnp.concatenate([high, middle, gain - high - middle], axis=1).astype(BF)
    channel_part = jnp.concatenate(
        [jnp.zeros((64, 128), BF), conv_t, pieces, jnp.zeros((64, 61), BF)], axis=1
    )
    split = pl.pallas_call(
        split_kernel,
        out_shape=(whole((320, 512), BF),) * SIDE,
        in_specs=[smem] + [vmem] * 5,
        out_specs=(vmem,) * SIDE,
        compiler_params=room,
        cost_estimate=cost(1000000, 2600000),
        name="split_weights",
    )(at, gate_weight[0], up_weight[0], down_weight[0], proj_weight, channel_part)
    weights = pass_on(split, unit_groups)
    got = lax.all_to_all(sent.reshape(sp_count, SLOT, 256), SP, 0, 0, tiled=True)
    got = got.reshape(slots, 256)
    got, weights = lax.optimization_barrier((got, weights))
    taps_t = conv_taps.T

    rows = exchange(jnp.broadcast_to(got[None], (SIDE, slots, 256)), feature_groups)
    step = 256
    pre = pl.pallas_call(
        pre_kernel,
        grid=(slots // step,),
        out_shape=whole((SIDE, 192, slots), BF),
        in_specs=[smem, pl.BlockSpec((SIDE, step, 256), lambda i: (0, i, 0))]
        + [pl.BlockSpec((192, 512), lambda i: (0, 0))] * SIDE,
        out_specs=pl.BlockSpec((SIDE, 192, step), lambda i: (0, 0, i)),
        compiler_params=room,
        cost_estimate=cost(800000000, 4400000),
        name="pre",
    )(at, rows, *weights)
    pre = exchange(pre, unit_groups)
    hidden = pl.pallas_call(
        gate_kernel,
        grid=(slots // step,),
        out_shape=whole((SIDE, 192, slots), BF),
        in_specs=[pl.BlockSpec((SIDE, 192, step), lambda i: (0, 0, i))],
        out_specs=pl.BlockSpec((SIDE, 192, step), lambda i: (0, 0, i)),
        compiler_params=room,
        cost_estimate=cost(3000000, 3200000),
        name="gates",
    )(pre)
    hidden = exchange(hidden, unit_groups)
    part = pl.pallas_call(
        partial_kernel,
        grid=(slots // step,),
        out_shape=whole((SIDE, slots, 128), BF),
        in_specs=[smem, pl.BlockSpec((SIDE, 192, step), lambda i: (0, 0, i))]
        + [pl.BlockSpec((192, 512), lambda i: (0, 0))] * SIDE,
        out_specs=pl.BlockSpec((SIDE, step, 128), lambda i: (0, i, 0)),
        compiler_params=room,
        cost_estimate=cost(540000000, 3400000),
        name="partial",
    )(at, hidden, *weights)
    part = exchange(part, feature_groups)
    back = pl.pallas_call(
        sum_side_kernel,
        out_shape=whole((slots, 128), BF),
        in_specs=[vmem],
        out_specs=vmem,
        compiler_params=room,
        cost_estimate=cost(1000000, 1300000),
        name="sum_side",
    )(part).reshape(sp_count, SLOT, 128)
    back, weights = lax.optimization_barrier((back, weights))
    relay = pl.pallas_call(
        relay_kernel,
        out_shape=(whole((256, 512), BF),) * SIDE,
        in_specs=[smem] + [vmem] * SIDE,
        out_specs=(vmem,) * SIDE,
        compiler_params=room,
        cost_estimate=cost(1000000, 2000000),
        name="relay",
    )(at, *weights)
    relay = pass_on(relay, feature_groups)
    returned = lax.all_to_all(back, SP, 0, 0, tiled=True).reshape(slots, 128)

    wide = 384
    mine, other, total_cot, stats = pl.pallas_call(
        total_kernel,
        out_shape=(
            whole((tp_count, 64, 128), BF),
            whole((tp_count, 64, 128), BF),
            whole((wide, 128), BF),
            whole((2, tokens), F32),
        ),
        in_specs=[smem] + [vmem] * 7,
        out_specs=(vmem,) * 4,
        compiler_params=room,
        cost_estimate=cost(170000000, 2500000),
        name="total_cot",
    )(at, pick, returned, out_cotangent, *relay)
    other = lax.ppermute(other, "c", [(0, 1), (1, 0)])
    act_part = pl.pallas_call(
        cot_kernel,
        out_shape=whole((tp_count, 72, wide), BF),
        in_specs=[smem] + [vmem] * 6,
        out_specs=vmem,
        compiler_params=room,
        cost_estimate=cost(100000000, 2500000),
        name="act_cot",
    )(at, total_cot, stats, *relay)
    act_part = pl.pallas_call(
        join_kernel,
        grid=(1,),
        out_shape=whole((tp_count, 72, wide), BF),
        in_specs=[
            pl.BlockSpec((tp_count, 72, 128), lambda i: (0, 0, 2)),
            pl.BlockSpec((tp_count, 64, 128), lambda i: (0, 0, 0)),
            pl.BlockSpec((tp_count, 64, 128), lambda i: (0, 0, 0)),
        ],
        out_specs=pl.BlockSpec((tp_count, 72, 128), lambda i: (0, 0, 2)),
        input_output_aliases={0: 0},
        compiler_params=room,
        cost_estimate=cost(100000, 1200000),
        name="join_cores",
    )(act_part, mine, other)
    act_part, hidden, rows = lax.optimization_barrier((act_part, hidden, rows))
    grads = pl.pallas_call(
        grads_kernel,
        grid=(SIDE,),
        out_shape=(whole((192, 512), BF),) * SIDE,
        in_specs=[
            smem,
            pl.BlockSpec((SIDE, 192, slots), lambda i: (0, 0, 0)),
            pl.BlockSpec((1, slots, 256), lambda i: (i, 0, 0)),
        ],
        out_specs=(pl.BlockSpec((192, 128), lambda i: (0, i)),) * SIDE,
        compiler_params=room,
        cost_estimate=cost(800000000, 4400000),
        name="grads",
    )(at, hidden, rows)
    grads = pass_on(grads, unit_groups)
    act_part = lax.all_to_all(act_part, TP, 0, 0, tiled=True)
    proj_part = pl.pallas_call(
        part_kernel,
        out_shape=whole((tp_count, 32, 128), BF),
        in_specs=[vmem],
        out_specs=vmem,
        compiler_params=room,
        cost_estimate=cost(100000, 400000),
        name="proj_part",
    )(act_part)
    act_part, proj_part = lax.optimization_barrier((act_part, proj_part))
    proj_part = lax.all_to_all(proj_part, "z", 0, 0, tiled=True)
    grad_proj = pl.pallas_call(
        sum_kernel,
        out_shape=whole((64, 64), F32),
        in_specs=[vmem],
        out_specs=vmem,
        compiler_params=room,
        cost_estimate=cost(100000, 200000),
        name="sum_planes",
    )(proj_part)

    conv_cot, head = pl.pallas_call(
        head_kernel,
        out_shape=(whole((64, tokens), F32), whole((64, 128), F32)),
        in_specs=[vmem] * 4,
        out_specs=(vmem, vmem),
        compiler_params=room,
        cost_estimate=cost(3000000, 1200000),
        name="conv_cot",
    )(act_part, conv_t, stats, gain)
    behind = [(i + 1, i) for i in range(sp_count - 1)]
    after = lax.ppermute(head, SP, behind)
    value, gate = pl.pallas_call(
        conv_kernel,
        out_shape=(whole((64, tokens), BF), whole((64, tokens), BF)),
        in_specs=[vmem] * 5,
        out_specs=(vmem, vmem),
        scratch_shapes=[VM((64, 384), F32)],
        compiler_params=room,
        cost_estimate=cost(4000000, 400000),
        name="conv",
    )(conv_cot, after, taps_t, glu_gate.T, glu_value.T)

    grad_gate, grad_up, grad_down = pl.pallas_call(
        merge_kernel,
        out_shape=(whole((64, 2048), F32),) * 3,
        in_specs=[smem] + [vmem] * SIDE,
        out_specs=(vmem,) * 3,
        compiler_params=room,
        cost_estimate=cost(1000000, 2400000),
        name="merge_grads",
    )(at, *grads)
    return (
        grad_gate[None],
        grad_up[None],
        grad_down[None],
        grad_proj,
        value.T,
        gate.T,
    )


def solution(mesh):
    split = Mesh(mesh.devices.reshape(16, 2, SIDE, SIDE), ("z", "c", "y", "x"))
    placed = (
        P(SP, TP),
        P(SP, TP),
        P(SP, None),
        P(SP, None),
        P(SP, TP, None),
        P(SP, TP, None),
        P(SP, TP, None),
        P(SP, TP),
        P(SP, TP),
        P(SP, TP),
        P(None, TP),
        P(TP),
        P(TP, None),
    )
    return jax.shard_map(
        body,
        mesh=split,
        in_specs=placed,
        out_specs=(
            P(SP, TP, None),
            P(SP, TP, None),
            P(SP, TP, None),
            P(SP, TP),
            P(SP, TP),
            P(SP, TP),
        ),
        check_vma=False,
    )
```

```python
import jax
import jax.numpy as jnp
import numpy as np
from jax import lax
from jax.experimental import pallas as pl
from jax.experimental.pallas import tpu as pltpu
from jax.sharding import Mesh
from jax.sharding import PartitionSpec as P

NORM_EPS = 0.25
SP = ("z", "c")
TP = ("y", "x")
PLANE = ("c", "y", "x")
SIDE = 4
SLOT = 32
ROOM = 12 << 20
BF = jnp.bfloat16
F32 = jnp.float32
VM = pltpu.VMEM

NT = (((1,), (1,)), ((), ()))
TN = (((0,), (0,)), ((), ()))
NN = (((1,), (0,)), ((), ()))


def place(core, row, col):
    return core * SIDE * SIDE + row * SIDE + col


def plane_groups():
    r = range(SIDE)
    down = [[[place(k, y, x) for y in r] for x in r] for k in (0, 1)]
    across = [[[place(k, y, x) for x in r] for y in r] for k in (0, 1)]
    return down[0] + across[1], across[0] + down[1]


def step_tables():
    features, units = plane_groups()
    of_features = {p: g for g in features for p in g}
    table = np.zeros((2 * SIDE * SIDE, 64), np.int32)
    for group in units:
        for me, p in enumerate(group):
            table[p, 0] = me
            table[p, 1] = of_features[p].index(p)
            table[p, 2] = p // (SIDE * SIDE)
            for k in range(SIDE):
                ahead = of_features[group[(me + k) % SIDE]]
                back = of_features[group[(me - k) % SIDE]]
                for a in range(SIDE):
                    table[p, 16 + k * SIDE + a] = ahead[a] % (SIDE * SIDE)
                    table[p, 32 + k * SIDE + a] = back[a] % (SIDE * SIDE)
    of_units = {p: g for g in units for p in g}
    for p in range(2 * SIDE * SIDE):
        group = of_features[p]
        for j in range(SIDE):
            source = group[(group.index(p) - j) % SIDE]
            their = of_units[source]
            for k in range(SIDE):
                first = their[(their.index(source) - k) % SIDE]
                table[p, 48 + j * SIDE + k] = first % (SIDE * SIDE)
    return table


def steps_ahead(groups, k):
    return [(g[i], g[(i + k) % SIDE]) for g in groups for i in range(SIDE)]


def shift(part, groups, k):
    return lax.ppermute(part, PLANE, steps_ahead(groups, k))


def pass_on(parts, groups):
    return (parts[0],) + tuple(shift(parts[k], groups, k) for k in range(1, SIDE))


def mm(a, b, dims):
    return lax.dot_general(a, b, dims, preferred_element_type=F32)


def exchange(v, groups):
    return lax.all_to_all(v, PLANE, 0, 0, axis_index_groups=groups, tiled=True)


def cost(flops, nbytes):
    return pl.CostEstimate(flops=flops, bytes_accessed=nbytes, transcendentals=0)


def route_kernel(rt_ref, w_ref, x_ref, c_ref, s_ref, t_ref):
    tokens = rt_ref.shape[1]
    experts = s_ref.shape[0] // SLOT
    first, second = rt_ref[0:1, :], rt_ref[1:2, :]
    ids = lax.broadcasted_iota(jnp.int32, (experts, tokens), 0)
    o0, o1 = ids == first, ids == second
    both = jnp.where(o0 | o1, 1.0, 0.0).astype(BF)
    before = lax.broadcasted_iota(jnp.int32, (tokens, tokens), 0) < lax.broadcasted_iota(
        jnp.int32, (tokens, tokens), 1
    )
    earlier = mm(both, jnp.where(before, 1.0, 0.0).astype(BF), NN)
    rank0 = jnp.sum(jnp.where(o0, earlier, 0.0), axis=0, keepdims=True)
    rank1 = jnp.sum(jnp.where(o1, earlier, 0.0), axis=0, keepdims=True)
    t0 = first * SLOT + rank0.astype(jnp.int32)
    t1 = second * SLOT + rank1.astype(jnp.int32)
    t_ref[0:1, :] = t0
    t_ref[1:2, :] = t1
    w0, w1 = w_ref[0:1, :], w_ref[1:2, :]
    x, c = x_ref[...], c_ref[...]
    size = 128
    for k in range(s_ref.shape[0] // size):
        slots = lax.broadcasted_iota(jnp.int32, (size, tokens), 0) + k * size
        m0, m1 = slots == t0, slots == t1
        pick = jnp.where(m0 | m1, 1.0, 0.0).astype(BF)
        weight = jnp.sum(
            jnp.where(m0, w0, 0.0) + jnp.where(m1, w1, 0.0), axis=1, keepdims=True
        )
        rows = pl.ds(k * size, size)
        s_ref[rows, 0:128] = mm(pick, x, NN).astype(BF)
        s_ref[rows, 128:256] = (weight * mm(pick, c, NN)).astype(BF)


def pick_kernel(t_ref, p_ref):
    slots = lax.broadcasted_iota(jnp.int32, p_ref.shape, 0)
    held = (slots == t_ref[0:1, :]) | (slots == t_ref[1:2, :])
    p_ref[...] = jnp.where(held, 1.0, 0.0).astype(BF)


def split_kernel(at_ref, g_ref, u_ref, d_ref, p_ref, c_ref, *outs):
    for k, out in enumerate(outs):
        for a in range(SIDE):
            at = at_ref[16 + k * SIDE + a]
            cols = pl.ds(pl.multiple_of(at * 128, 128), 128)
            for q, ref in enumerate((g_ref, u_ref, d_ref, p_ref)):
                out[q * 64 : q * 64 + 64, a * 128 : a * 128 + 128] = ref[:, cols]
        out[256:320, :] = c_ref[...]


def relay_kernel(at_ref, r0, r1, r2, r3, *outs):
    for j, out in enumerate(outs):
        a = lax.rem(at_ref[1] + j, SIDE)
        cols = pl.ds(pl.multiple_of(a * 128, 128), 128)
        for k, r_ref in enumerate((r0, r1, r2, r3)):
            out[k * 64 : k * 64 + 64, 0:128] = r_ref[192:256, cols]
            out[k * 64 : k * 64 + 64, 128:512] = r_ref[256:320, 128:512]


def merge_kernel(at_ref, s0, s1, s2, s3, g_ref, u_ref, d_ref):
    for k, s_ref in enumerate((s0, s1, s2, s3)):
        for a in range(SIDE):
            at = at_ref[32 + k * SIDE + a]
            cols = pl.ds(pl.multiple_of(at * 128, 128), 128)
            for q, ref in enumerate((g_ref, u_ref, d_ref)):
                ref[:, cols] = s_ref[
                    q * 64 : q * 64 + 64, a * 128 : a * 128 + 128
                ].astype(F32)


def behind_of(at_ref, k):
    return lax.rem(at_ref[0] + (SIDE - k), SIDE)


def ahead_of(at_ref, k):
    return lax.rem(at_ref[0] + k, SIDE)


def pre_kernel(at_ref, a_ref, w0, w1, w2, w3, o_ref):
    ws = (w0, w1, w2, w3)
    x = jnp.concatenate([a_ref[i, :, 0:128] for i in range(SIDE)], axis=1)
    c = jnp.concatenate([a_ref[i, :, 128:256] for i in range(SIDE)], axis=1)
    pairs = mm(jnp.concatenate([w[0:128, :] for w in ws], axis=0), x, NT)
    downs = mm(jnp.concatenate([w[128:192, :] for w in ws], axis=0), c, NT)
    for k in range(SIDE):
        b = behind_of(at_ref, k)
        o_ref[b, 0:128, :] = pairs[k * 128 : k * 128 + 128].astype(BF)
        o_ref[b, 128:192, :] = downs[k * 64 : k * 64 + 64].astype(BF)


def gate_kernel(p_ref, o_ref):
    total = p_ref[0].astype(F32)
    for b in range(1, SIDE):
        total = total + p_ref[b].astype(F32)
    gate, up, cot = total[0:64], total[64:128], total[128:192]
    s = jax.nn.sigmoid(gate)
    act = gate * s
    hidden = (act * up).astype(BF)
    up_cot = (cot * act).astype(BF)
    gate_cot = (cot * up * s * (1.0 + gate * (1.0 - s))).astype(BF)
    for b in range(SIDE):
        o_ref[b, 0:64, :] = gate_cot
        o_ref[b, 64:128, :] = up_cot
        o_ref[b, 128:192, :] = hidden


def partial_kernel(at_ref, h_ref, w0, w1, w2, w3, o_ref):
    ws = (w0, w1, w2, w3)
    h = jnp.concatenate([h_ref[behind_of(at_ref, k), 0:128, :] for k in range(SIDE)], axis=0)
    w = jnp.concatenate([w_ref[0:128, :] for w_ref in ws], axis=0)
    total = mm(h, w, TN)
    for a in range(SIDE):
        o_ref[a] = total[:, a * 128 : a * 128 + 128].astype(BF)


def grads_kernel(at_ref, h_ref, a_ref, *outs):
    x = jnp.concatenate([a_ref[0, :, 0:128], a_ref[1, :, 0:128]], axis=1)
    c = jnp.concatenate([a_ref[0, :, 128:256], a_ref[1, :, 128:256]], axis=1)
    order = [ahead_of(at_ref, k) for k in range(SIDE)]
    pairs = mm(jnp.concatenate([h_ref[b, 0:128, :] for b in order], axis=0), x, NN)
    downs = mm(jnp.concatenate([h_ref[b, 128:192, :] for b in order], axis=0), c, NN)
    for k, out in enumerate(outs):
        out[0:128, :] = pairs[k * 128 : k * 128 + 128].astype(BF)
        out[128:192, :] = downs[k * 64 : k * 64 + 64].astype(BF)


def total_kernel(
    at_ref, p_ref, r_ref, c_ref, q0, q1, q2, q3, mine_ref, other_ref, total_ref, stats_ref
):
    qs = (q0, q1, q2, q3)
    moe = mm(p_ref[...], r_ref[...], TN)
    total = (c_ref[...].astype(F32) + moe).astype(BF)
    tokens = total.shape[0]
    total_ref[0:tokens, :] = total
    total_ref[tokens:, :] = jnp.zeros((total_ref.shape[0] - tokens, 128), BF)
    size = q0.shape[0]
    channels = SIDE * size
    mean = jnp.zeros((1, tokens), F32)
    for q in qs:
        conv = q[:, 128 : 128 + tokens].astype(F32)
        mean = mean + jnp.sum(conv, axis=0, keepdims=True)
    mean = mean / channels
    var = jnp.zeros((1, tokens), F32)
    for q in qs:
        off = q[:, 128 : 128 + tokens].astype(F32) - mean
        var = var + jnp.sum(off * off, axis=0, keepdims=True)
    inv = lax.rsqrt(var / channels + NORM_EPS)
    stats_ref[0:1, :] = mean
    stats_ref[1:2, :] = inv
    own = jnp.full((64, 128), at_ref[2], jnp.int32) == 0
    for j, q in enumerate(qs):
        normed = (q[:, 128 : 128 + tokens].astype(F32) - mean) * inv
        linear = normed * gain_of(q)
        act = (linear * jax.nn.sigmoid(linear)).astype(BF)
        grad = mm(act, total, NN)
        turned = pltpu.roll(grad, 64, 1)
        for k in range(SIDE):
            b = at_ref[48 + j * SIDE + k]
            rows = slice(k * 64, k * 64 + 64)
            mine_ref[b] = jnp.where(own, turned[rows], grad[rows]).astype(BF)
            other_ref[b] = jnp.where(own, grad[rows], turned[rows]).astype(BF)


def gain_of(q):
    lane = lax.broadcasted_iota(jnp.int32, (q.shape[0], 128), 1)
    pieces = jnp.where((lane >= 64) & (lane < 67), q[:, 384:512].astype(F32), 0.0)
    return jnp.sum(pieces, axis=1, keepdims=True)


def cot_kernel(at_ref, total_ref, stats_ref, q0, q1, q2, q3, o_ref):
    wide = total_ref.shape[0]
    tokens = stats_ref.shape[1]
    total = total_ref[...]
    mean, inv = stats_ref[0:1, :], stats_ref[1:2, :]
    first = jnp.zeros((1, tokens), F32)
    second = jnp.zeros((1, tokens), F32)
    for j, q in enumerate((q0, q1, q2, q3)):
        normed = (q[:, 128 : 128 + tokens].astype(F32) - mean) * inv
        gain = gain_of(q)
        linear = normed * gain
        s = jax.nn.sigmoid(linear)
        cot = mm(q[:, 0:128], total, NT)
        sloped = cot[:, 0:tokens] * (s * (1.0 + linear * (1.0 - s)) * gain)
        first = first + jnp.sum(sloped, axis=0, keepdims=True)
        second = second + jnp.sum(sloped * normed, axis=0, keepdims=True)
        for k in range(SIDE):
            o_ref[at_ref[48 + j * SIDE + k], 0:64, :] = cot[k * 64 : k * 64 + 64].astype(BF)
    row = lax.broadcasted_iota(jnp.int32, (8, tokens), 0)
    sums = jnp.zeros((8, tokens), F32)
    for i, v in enumerate((first, second)):
        head = v.astype(BF).astype(F32)
        sums = jnp.where(row == 2 * i, head, jnp.where(row == 2 * i + 1, v - head, sums))
    for b in range(o_ref.shape[0]):
        o_ref[b, 64:72, 0:tokens] = sums.astype(BF)
        o_ref[b, 64:72, tokens:wide] = jnp.zeros((8, wide - tokens), BF)


def join_kernel(a_ref, mine_ref, other_ref, o_ref):
    low = lax.broadcasted_iota(jnp.int32, (64, 128), 1) < 64
    for b in range(o_ref.shape[0]):
        piece = mine_ref[b].astype(F32) + other_ref[b].astype(F32)
        o_ref[b, 0:64, :] = jnp.where(low, a_ref[b, 0:64, :].astype(F32), piece).astype(BF)
        o_ref[b, 64:72, :] = a_ref[b, 64:72, :]


def part_kernel(r_ref, o_ref):
    low = lax.broadcasted_iota(jnp.int32, (32, 128), 1) < 64
    for b in range(o_ref.shape[0]):
        upper = pltpu.roll(r_ref[b, 0:32, 256:384].astype(F32), 64, 1)
        lower = r_ref[b, 32:64, 256:384].astype(F32)
        o_ref[b] = jnp.where(low, upper, lower).astype(BF)


def head_kernel(r_ref, conv_ref, stats_ref, gain_ref, o_ref, h_ref):
    tokens = conv_ref.shape[1]
    total = r_ref[0, :, 0:tokens].astype(F32)
    for b in range(1, r_ref.shape[0]):
        total = total + r_ref[b, :, 0:tokens].astype(F32)
    channels = 16 * conv_ref.shape[0]
    first = (total[64:65] + total[65:66]) / channels
    second = (total[66:67] + total[67:68]) / channels
    inv = stats_ref[1:2, :]
    normed = (conv_ref[...].astype(F32) - stats_ref[0:1, :]) * inv
    gain = gain_ref[...]
    linear = normed * gain
    s = jax.nn.sigmoid(linear)
    cot = total[0:64] * s * (1.0 + linear * (1.0 - s)) * gain
    cot = inv * (cot - first - normed * second)
    o_ref[...] = cot
    h_ref[...] = cot[:, 0:128]


def sum_kernel(a_ref, o_ref):
    total = a_ref[0].astype(F32)
    for b in range(1, a_ref.shape[0]):
        total = total + a_ref[b].astype(F32)
    turned = pltpu.roll(total, 64, 1)
    block = jnp.concatenate([total, turned], axis=0)
    o_ref[...] = block.T[0:64, :]


def sum_side_kernel(p_ref, o_ref):
    total = p_ref[0].astype(F32)
    for a in range(1, SIDE):
        total = total + p_ref[a].astype(F32)
    o_ref[...] = total.astype(BF)


def conv_kernel(cot_ref, next_ref, taps_ref, gate_ref, value_ref, v_ref, g_ref, buf):
    rows, tokens = cot_ref.shape
    wide = buf.shape[1]
    reach = taps_ref.shape[1] - 1
    buf[:, 0:128] = next_ref[...]
    buf[:, 128:wide] = jnp.zeros((rows, wide - 128), F32)
    after = pltpu.roll(buf[...], tokens, 1)
    buf[:, 0:tokens] = cot_ref[...]
    lane = lax.broadcasted_iota(jnp.int32, (rows, wide), 1)
    whole = jnp.where(lane < tokens, buf[...], after)
    taps = taps_ref[...]
    total = whole * taps[:, reach : reach + 1]
    for s in range(1, reach + 1):
        total = total + pltpu.roll(whole, wide - s, 1) * taps[:, reach - s : reach - s + 1]
    cot = total[:, 0:tokens]
    s = jax.nn.sigmoid(gate_ref[...].astype(F32))
    v_ref[...] = (cot * s).astype(BF)
    g_ref[...] = (cot * value_ref[...].astype(F32) * s * (1.0 - s)).astype(BF)


def whole(shape, dtype):
    return jax.ShapeDtypeStruct(shape, dtype)


def body(
    moe_input,
    out_cotangent,
    routes,
    route_weight,
    gate_weight,
    up_weight,
    down_weight,
    glu_value,
    glu_gate,
    conv_result,
    conv_taps,
    norm_gain,
    proj_weight,
):
    sp_count = lax.axis_size(SP)
    tp_count = lax.axis_size(TP)
    tokens = moe_input.shape[0]
    slots = sp_count * SLOT
    feature_groups, unit_groups = plane_groups()
    smem = pl.BlockSpec(memory_space=pltpu.SMEM)
    vmem = pl.BlockSpec(memory_space=VM)
    room = pltpu.CompilerParams(vmem_limit_bytes=ROOM)

    sent, target = pl.pallas_call(
        route_kernel,
        out_shape=(whole((slots, 256), BF), whole((2, tokens), jnp.int32)),
        in_specs=[vmem] * 4,
        out_specs=(vmem, vmem),
        cost_estimate=cost(400000000, 2000000),
        name="route",
    )(routes.T, route_weight.T, moe_input, out_cotangent)
    sent, target, table, gate_weight, conv_result, norm_gain = lax.optimization_barrier(
        (sent, target, jnp.asarray(step_tables()), gate_weight, conv_result, norm_gain)
    )
    at = table[lax.axis_index(PLANE)]
    pick = pl.pallas_call(
        pick_kernel,
        out_shape=whole((slots, tokens), BF),
        in_specs=[vmem],
        out_specs=vmem,
        compiler_params=room,
        cost_estimate=cost(1000000, 700000),
        name="pick",
    )(target)
    conv_t = conv_result.T
    gain = norm_gain.reshape(-1, 1)
    high = lax.reduce_precision(gain, 8, 7)
    middle = lax.reduce_precision(gain - high, 8, 7)
    pieces = jnp.concatenate([high, middle, gain - high - middle], axis=1).astype(BF)
    channel_part = jnp.concatenate(
        [jnp.zeros((64, 128), BF), conv_t, pieces, jnp.zeros((64, 61), BF)], axis=1
    )
    split = pl.pallas_call(
        split_kernel,
        out_shape=(whole((320, 512), BF),) * SIDE,
        in_specs=[smem] + [vmem] * 5,
        out_specs=(vmem,) * SIDE,
        compiler_params=room,
        cost_estimate=cost(1000000, 2600000),
        name="split_weights",
    )(at, gate_weight[0], up_weight[0], down_weight[0], proj_weight, channel_part)
    weights = pass_on(split, unit_groups)
    relay = pl.pallas_call(
        relay_kernel,
        out_shape=(whole((256, 512), BF),) * SIDE,
        in_specs=[smem] + [vmem] * SIDE,
        out_specs=(vmem,) * SIDE,
        compiler_params=room,
        cost_estimate=cost(1000000, 2000000),
        name="relay",
    )(at, *weights)
    arrived = shift(relay[1], feature_groups, 1)
    got = lax.all_to_all(sent.reshape(sp_count, SLOT, 256), SP, 0, 0, tiled=True)
    got = got.reshape(slots, 256)
    got, weights, relay, arrived = lax.optimization_barrier((got, weights, relay, arrived))
    taps_t = conv_taps.T

    rows = exchange(jnp.broadcast_to(got[None], (SIDE, slots, 256)), feature_groups)
    step = 256
    pre = pl.pallas_call(
        pre_kernel,
        grid=(slots // step,),
        out_shape=whole((SIDE, 192, slots), BF),
        in_specs=[smem, pl.BlockSpec((SIDE, step, 256), lambda i: (0, i, 0))]
        + [pl.BlockSpec((192, 512), lambda i: (0, 0))] * SIDE,
        out_specs=pl.BlockSpec((SIDE, 192, step), lambda i: (0, 0, i)),
        compiler_params=room,
        cost_estimate=cost(800000000, 4400000),
        name="pre",
    )(at, rows, *weights)
    pre = exchange(pre, unit_groups)
    hidden = pl.pallas_call(
        gate_kernel,
        grid=(slots // step,),
        out_shape=whole((SIDE, 192, slots), BF),
        in_specs=[pl.BlockSpec((SIDE, 192, step), lambda i: (0, 0, i))],
        out_specs=pl.BlockSpec((SIDE, 192, step), lambda i: (0, 0, i)),
        compiler_params=room,
        cost_estimate=cost(3000000, 3200000),
        name="gates",
    )(pre)
    hidden = exchange(hidden, unit_groups)
    part = pl.pallas_call(
        partial_kernel,
        grid=(slots // step,),
        out_shape=whole((SIDE, slots, 128), BF),
        in_specs=[smem, pl.BlockSpec((SIDE, 192, step), lambda i: (0, 0, i))]
        + [pl.BlockSpec((192, 512), lambda i: (0, 0))] * SIDE,
        out_specs=pl.BlockSpec((SIDE, step, 128), lambda i: (0, i, 0)),
        compiler_params=room,
        cost_estimate=cost(540000000, 3400000),
        name="partial",
    )(at, hidden, *weights)
    part = exchange(part, feature_groups)
    back = pl.pallas_call(
        sum_side_kernel,
        out_shape=whole((slots, 128), BF),
        in_specs=[vmem],
        out_specs=vmem,
        compiler_params=room,
        cost_estimate=cost(1000000, 1300000),
        name="sum_side",
    )(part).reshape(sp_count, SLOT, 128)
    back, relay = lax.optimization_barrier((back, relay))
    relay = (relay[0], arrived, shift(relay[2], feature_groups, 2), shift(relay[3], feature_groups, 3))
    returned = lax.all_to_all(back, SP, 0, 0, tiled=True).reshape(slots, 128)

    grads = pl.pallas_call(
        grads_kernel,
        grid=(SIDE // 2,),
        out_shape=(whole((192, 512), BF),) * SIDE,
        in_specs=[
            smem,
            pl.BlockSpec((SIDE, 192, slots), lambda i: (0, 0, 0)),
            pl.BlockSpec((2, slots, 256), lambda i: (i, 0, 0)),
        ],
        out_specs=(pl.BlockSpec((192, 256), lambda i: (0, i)),) * SIDE,
        compiler_params=room,
        cost_estimate=cost(800000000, 4400000),
        name="grads",
    )(at, hidden, rows)
    first_grad = shift(grads[1], unit_groups, 1)
    returned, grads, first_grad = lax.optimization_barrier((returned, grads, first_grad))

    wide = 384
    mine, other, total_cot, stats = pl.pallas_call(
        total_kernel,
        out_shape=(
            whole((tp_count, 64, 128), BF),
            whole((tp_count, 64, 128), BF),
            whole((wide, 128), BF),
            whole((2, tokens), F32),
        ),
        in_specs=[smem] + [vmem] * 7,
        out_specs=(vmem,) * 4,
        compiler_params=room,
        cost_estimate=cost(170000000, 2500000),
        name="total_cot",
    )(at, pick, returned, out_cotangent, *relay)
    other = lax.ppermute(other, "c", [(0, 1), (1, 0)])
    act_part = pl.pallas_call(
        cot_kernel,
        out_shape=whole((tp_count, 72, wide), BF),
        in_specs=[smem] + [vmem] * 6,
        out_specs=vmem,
        compiler_params=room,
        cost_estimate=cost(100000000, 2500000),
        name="act_cot",
    )(at, total_cot, stats, *relay)
    act_part = pl.pallas_call(
        join_kernel,
        grid=(1,),
        out_shape=whole((tp_count, 72, wide), BF),
        in_specs=[
            pl.BlockSpec((tp_count, 72, 128), lambda i: (0, 0, 2)),
            pl.BlockSpec((tp_count, 64, 128), lambda i: (0, 0, 0)),
            pl.BlockSpec((tp_count, 64, 128), lambda i: (0, 0, 0)),
        ],
        out_specs=pl.BlockSpec((tp_count, 72, 128), lambda i: (0, 0, 2)),
        input_output_aliases={0: 0},
        compiler_params=room,
        cost_estimate=cost(100000, 1200000),
        name="join_cores",
    )(act_part, mine, other)
    act_part = lax.all_to_all(act_part, TP, 0, 0, tiled=True)
    proj_part = pl.pallas_call(
        part_kernel,
        out_shape=whole((tp_count, 32, 128), BF),
        in_specs=[vmem],
        out_specs=vmem,
        compiler_params=room,
        cost_estimate=cost(100000, 400000),
        name="proj_part",
    )(act_part)
    act_part, proj_part, grads = lax.optimization_barrier((act_part, proj_part, grads))
    grads = (grads[0], first_grad, shift(grads[2], unit_groups, 2), shift(grads[3], unit_groups, 3))
    proj_part = lax.all_to_all(proj_part, "z", 0, 0, tiled=True)
    grad_proj = pl.pallas_call(
        sum_kernel,
        out_shape=whole((64, 64), F32),
        in_specs=[vmem],
        out_specs=vmem,
        compiler_params=room,
        cost_estimate=cost(100000, 200000),
        name="sum_planes",
    )(proj_part)

    conv_cot, head = pl.pallas_call(
        head_kernel,
        out_shape=(whole((64, tokens), F32), whole((64, 128), F32)),
        in_specs=[vmem] * 4,
        out_specs=(vmem, vmem),
        compiler_params=room,
        cost_estimate=cost(3000000, 1200000),
        name="conv_cot",
    )(act_part, conv_t, stats, gain)
    behind = [(i + 1, i) for i in range(sp_count - 1)]
    after = lax.ppermute(head, SP, behind)
    value, gate = pl.pallas_call(
        conv_kernel,
        out_shape=(whole((64, tokens), BF), whole((64, tokens), BF)),
        in_specs=[vmem] * 5,
        out_specs=(vmem, vmem),
        scratch_shapes=[VM((64, 384), F32)],
        compiler_params=room,
        cost_estimate=cost(4000000, 400000),
        name="conv",
    )(conv_cot, after, taps_t, glu_gate.T, glu_value.T)

    grad_gate, grad_up, grad_down = pl.pallas_call(
        merge_kernel,
        out_shape=(whole((64, 2048), F32),) * 3,
        in_specs=[smem] + [vmem] * SIDE,
        out_specs=(vmem,) * 3,
        compiler_params=room,
        cost_estimate=cost(1000000, 2400000),
        name="merge_grads",
    )(at, *grads)
    return (
        grad_gate[None],
        grad_up[None],
        grad_down[None],
        grad_proj,
        value.T,
        gate.T,
    )


def solution(mesh):
    split = Mesh(mesh.devices.reshape(16, 2, SIDE, SIDE), ("z", "c", "y", "x"))
    placed = (
        P(SP, TP),
        P(SP, TP),
        P(SP, None),
        P(SP, None),
        P(SP, TP, None),
        P(SP, TP, None),
        P(SP, TP, None),
        P(SP, TP),
        P(SP, TP),
        P(SP, TP),
        P(None, TP),
        P(TP),
        P(TP, None),
    )
    return jax.shard_map(
        body,
        mesh=split,
        in_specs=placed,
        out_specs=(
            P(SP, TP, None),
            P(SP, TP, None),
            P(SP, TP, None),
            P(SP, TP),
            P(SP, TP),
            P(SP, TP),
        ),
        check_vma=False,
    )
```

```python
import jax
import jax.numpy as jnp
import numpy as np
from jax import lax
from jax.experimental import pallas as pl
from jax.experimental.pallas import tpu as pltpu
from jax.sharding import Mesh
from jax.sharding import PartitionSpec as P

NORM_EPS = 0.25
SP = ("z", "c")
TP = ("y", "x")
PLANE = ("c", "y", "x")
SIDE = 4
SLOT = 32
ROOM = 12 << 20
BF = jnp.bfloat16
F32 = jnp.float32
VM = pltpu.VMEM

NT = (((1,), (1,)), ((), ()))
TN = (((0,), (0,)), ((), ()))
NN = (((1,), (0,)), ((), ()))


def place(core, row, col):
    return core * SIDE * SIDE + row * SIDE + col


def plane_groups():
    r = range(SIDE)
    down = [[[place(k, y, x) for y in r] for x in r] for k in (0, 1)]
    across = [[[place(k, y, x) for x in r] for y in r] for k in (0, 1)]
    return down[0] + across[1], across[0] + down[1]


def step_tables():
    features, units = plane_groups()
    of_features = {p: g for g in features for p in g}
    table = np.zeros((2 * SIDE * SIDE, 64), np.int32)
    for group in units:
        for me, p in enumerate(group):
            table[p, 0] = me
            table[p, 1] = of_features[p].index(p)
            table[p, 2] = p // (SIDE * SIDE)
            for k in range(SIDE):
                ahead = of_features[group[(me + k) % SIDE]]
                back = of_features[group[(me - k) % SIDE]]
                for a in range(SIDE):
                    table[p, 16 + k * SIDE + a] = ahead[a] % (SIDE * SIDE)
                    table[p, 32 + k * SIDE + a] = back[a] % (SIDE * SIDE)
    of_units = {p: g for g in units for p in g}
    for p in range(2 * SIDE * SIDE):
        group = of_features[p]
        for j in range(SIDE):
            source = group[(group.index(p) - j) % SIDE]
            their = of_units[source]
            for k in range(SIDE):
                first = their[(their.index(source) - k) % SIDE]
                table[p, 48 + j * SIDE + k] = first % (SIDE * SIDE)
    return table


def steps_ahead(groups, k):
    return [(g[i], g[(i + k) % SIDE]) for g in groups for i in range(SIDE)]


def shift(part, groups, k):
    return lax.ppermute(part, PLANE, steps_ahead(groups, k))


def pass_on(parts, groups):
    return (parts[0],) + tuple(shift(parts[k], groups, k) for k in range(1, SIDE))


def mm(a, b, dims):
    return lax.dot_general(a, b, dims, preferred_element_type=F32)


def exchange(v, groups):
    return lax.all_to_all(v, PLANE, 0, 0, axis_index_groups=groups, tiled=True)


def cost(flops, nbytes):
    return pl.CostEstimate(flops=flops, bytes_accessed=nbytes, transcendentals=0)


def route_kernel(rt_ref, w_ref, x_ref, c_ref, s_ref, t_ref):
    tokens = rt_ref.shape[1]
    experts = s_ref.shape[0] // SLOT
    first, second = rt_ref[0:1, :], rt_ref[1:2, :]
    ids = lax.broadcasted_iota(jnp.int32, (experts, tokens), 0)
    o0, o1 = ids == first, ids == second
    both = jnp.where(o0 | o1, 1.0, 0.0).astype(BF)
    before = lax.broadcasted_iota(jnp.int32, (tokens, tokens), 0) < lax.broadcasted_iota(
        jnp.int32, (tokens, tokens), 1
    )
    earlier = mm(both, jnp.where(before, 1.0, 0.0).astype(BF), NN)
    rank0 = jnp.sum(jnp.where(o0, earlier, 0.0), axis=0, keepdims=True)
    rank1 = jnp.sum(jnp.where(o1, earlier, 0.0), axis=0, keepdims=True)
    t0 = first * SLOT + rank0.astype(jnp.int32)
    t1 = second * SLOT + rank1.astype(jnp.int32)
    t_ref[0:1, :] = t0
    t_ref[1:2, :] = t1
    w0, w1 = w_ref[0:1, :], w_ref[1:2, :]
    x, c = x_ref[...], c_ref[...]
    size = 128
    for k in range(s_ref.shape[0] // size):
        slots = lax.broadcasted_iota(jnp.int32, (size, tokens), 0) + k * size
        m0, m1 = slots == t0, slots == t1
        pick = jnp.where(m0 | m1, 1.0, 0.0).astype(BF)
        weight = jnp.sum(
            jnp.where(m0, w0, 0.0) + jnp.where(m1, w1, 0.0), axis=1, keepdims=True
        )
        rows = pl.ds(k * size, size)
        s_ref[rows, 0:128] = mm(pick, x, NN).astype(BF)
        s_ref[rows, 128:256] = (weight * mm(pick, c, NN)).astype(BF)


def pick_kernel(t_ref, p_ref):
    slots = lax.broadcasted_iota(jnp.int32, p_ref.shape, 0)
    held = (slots == t_ref[0:1, :]) | (slots == t_ref[1:2, :])
    p_ref[...] = jnp.where(held, 1.0, 0.0).astype(BF)


def split_kernel(at_ref, g_ref, u_ref, d_ref, p_ref, c_ref, *outs):
    for k, out in enumerate(outs):
        for a in range(SIDE):
            at = at_ref[16 + k * SIDE + a]
            cols = pl.ds(pl.multiple_of(at * 128, 128), 128)
            for q, ref in enumerate((g_ref, u_ref, d_ref, p_ref)):
                out[q * 64 : q * 64 + 64, a * 128 : a * 128 + 128] = ref[:, cols]
        out[256:320, :] = c_ref[...]


def relay_kernel(at_ref, r0, r1, r2, r3, *outs):
    for j, out in enumerate(outs):
        a = lax.rem(at_ref[1] + j, SIDE)
        cols = pl.ds(pl.multiple_of(a * 128, 128), 128)
        for k, r_ref in enumerate((r0, r1, r2, r3)):
            out[k * 64 : k * 64 + 64, 0:128] = r_ref[192:256, cols]
            out[k * 64 : k * 64 + 64, 128:512] = r_ref[256:320, 128:512]


def merge_kernel(at_ref, s0, s1, s2, s3, g_ref, u_ref, d_ref):
    for k, s_ref in enumerate((s0, s1, s2, s3)):
        for a in range(SIDE):
            at = at_ref[32 + k * SIDE + a]
            cols = pl.ds(pl.multiple_of(at * 128, 128), 128)
            for q, ref in enumerate((g_ref, u_ref, d_ref)):
                ref[:, cols] = s_ref[
                    q * 64 : q * 64 + 64, a * 128 : a * 128 + 128
                ].astype(F32)


def behind_of(at_ref, k):
    return lax.rem(at_ref[0] + (SIDE - k), SIDE)


def ahead_of(at_ref, k):
    return lax.rem(at_ref[0] + k, SIDE)


def pre_kernel(at_ref, a_ref, w0, w1, w2, w3, o_ref):
    ws = (w0, w1, w2, w3)
    x = jnp.concatenate([a_ref[i, :, 0:128] for i in range(SIDE)], axis=1)
    c = jnp.concatenate([a_ref[i, :, 128:256] for i in range(SIDE)], axis=1)
    pairs = mm(jnp.concatenate([w[0:128, :] for w in ws], axis=0), x, NT)
    downs = mm(jnp.concatenate([w[128:192, :] for w in ws], axis=0), c, NT)
    for k in range(SIDE):
        b = behind_of(at_ref, k)
        o_ref[b, 0:128, :] = pairs[k * 128 : k * 128 + 128].astype(BF)
        o_ref[b, 128:192, :] = downs[k * 64 : k * 64 + 64].astype(BF)


def gate_kernel(p_ref, o_ref):
    total = p_ref[0].astype(F32)
    for b in range(1, SIDE):
        total = total + p_ref[b].astype(F32)
    gate, up, cot = total[0:64], total[64:128], total[128:192]
    s = jax.nn.sigmoid(gate)
    act = gate * s
    hidden = (act * up).astype(BF)
    up_cot = (cot * act).astype(BF)
    gate_cot = (cot * up * s * (1.0 + gate * (1.0 - s))).astype(BF)
    for b in range(SIDE):
        o_ref[b, 0:64, :] = gate_cot
        o_ref[b, 64:128, :] = up_cot
        o_ref[b, 128:192, :] = hidden


def partial_kernel(at_ref, h_ref, w0, w1, w2, w3, o_ref):
    ws = (w0, w1, w2, w3)
    h = jnp.concatenate([h_ref[behind_of(at_ref, k), 0:128, :] for k in range(SIDE)], axis=0)
    w = jnp.concatenate([w_ref[0:128, :] for w_ref in ws], axis=0)
    total = mm(h, w, TN)
    for a in range(SIDE):
        o_ref[a] = total[:, a * 128 : a * 128 + 128].astype(BF)


def grads_kernel(at_ref, h_ref, a_ref, *outs):
    x = jnp.concatenate([a_ref[0, :, 0:128], a_ref[1, :, 0:128]], axis=1)
    c = jnp.concatenate([a_ref[0, :, 128:256], a_ref[1, :, 128:256]], axis=1)
    order = [ahead_of(at_ref, k) for k in range(SIDE)]
    pairs = mm(jnp.concatenate([h_ref[b, 0:128, :] for b in order], axis=0), x, NN)
    downs = mm(jnp.concatenate([h_ref[b, 128:192, :] for b in order], axis=0), c, NN)
    for k, out in enumerate(outs):
        out[0:128, :] = pairs[k * 128 : k * 128 + 128].astype(BF)
        out[128:192, :] = downs[k * 64 : k * 64 + 64].astype(BF)


def total_kernel(
    at_ref, p_ref, r_ref, c_ref, q0, q1, q2, q3, mine_ref, other_ref, total_ref, stats_ref
):
    qs = (q0, q1, q2, q3)
    moe = mm(p_ref[...], r_ref[...], TN)
    total = (c_ref[...].astype(F32) + moe).astype(BF)
    tokens = total.shape[0]
    total_ref[0:tokens, :] = total
    total_ref[tokens:, :] = jnp.zeros((total_ref.shape[0] - tokens, 128), BF)
    size = q0.shape[0]
    channels = SIDE * size
    mean = jnp.zeros((1, tokens), F32)
    for q in qs:
        conv = q[:, 128 : 128 + tokens].astype(F32)
        mean = mean + jnp.sum(conv, axis=0, keepdims=True)
    mean = mean / channels
    var = jnp.zeros((1, tokens), F32)
    for q in qs:
        off = q[:, 128 : 128 + tokens].astype(F32) - mean
        var = var + jnp.sum(off * off, axis=0, keepdims=True)
    inv = lax.rsqrt(var / channels + NORM_EPS)
    stats_ref[0:1, :] = mean
    stats_ref[1:2, :] = inv
    own = jnp.full((64, 128), at_ref[2], jnp.int32) == 0
    for j, q in enumerate(qs):
        normed = (q[:, 128 : 128 + tokens].astype(F32) - mean) * inv
        linear = normed * gain_of(q)
        act = (linear * jax.nn.sigmoid(linear)).astype(BF)
        grad = mm(act, total, NN)
        turned = pltpu.roll(grad, 64, 1)
        for k in range(SIDE):
            b = at_ref[48 + j * SIDE + k]
            rows = slice(k * 64, k * 64 + 64)
            mine_ref[b] = jnp.where(own, turned[rows], grad[rows]).astype(BF)
            other_ref[b] = jnp.where(own, grad[rows], turned[rows]).astype(BF)


def gain_of(q):
    lane = lax.broadcasted_iota(jnp.int32, (q.shape[0], 128), 1)
    pieces = jnp.where((lane >= 64) & (lane < 67), q[:, 384:512].astype(F32), 0.0)
    return jnp.sum(pieces, axis=1, keepdims=True)


def cot_kernel(at_ref, total_ref, stats_ref, q0, q1, q2, q3, o_ref):
    wide = total_ref.shape[0]
    tokens = stats_ref.shape[1]
    total = total_ref[...]
    mean, inv = stats_ref[0:1, :], stats_ref[1:2, :]
    first = jnp.zeros((1, tokens), F32)
    second = jnp.zeros((1, tokens), F32)
    for j, q in enumerate((q0, q1, q2, q3)):
        normed = (q[:, 128 : 128 + tokens].astype(F32) - mean) * inv
        gain = gain_of(q)
        linear = normed * gain
        s = jax.nn.sigmoid(linear)
        cot = mm(q[:, 0:128], total, NT)
        sloped = cot[:, 0:tokens] * (s * (1.0 + linear * (1.0 - s)) * gain)
        first = first + jnp.sum(sloped, axis=0, keepdims=True)
        second = second + jnp.sum(sloped * normed, axis=0, keepdims=True)
        for k in range(SIDE):
            o_ref[at_ref[48 + j * SIDE + k], 0:64, :] = cot[k * 64 : k * 64 + 64].astype(BF)
    row = lax.broadcasted_iota(jnp.int32, (8, tokens), 0)
    sums = jnp.zeros((8, tokens), F32)
    for i, v in enumerate((first, second)):
        head = v.astype(BF).astype(F32)
        sums = jnp.where(row == 2 * i, head, jnp.where(row == 2 * i + 1, v - head, sums))
    for b in range(o_ref.shape[0]):
        o_ref[b, 64:72, 0:tokens] = sums.astype(BF)
        o_ref[b, 64:72, tokens:wide] = jnp.zeros((8, wide - tokens), BF)


def join_kernel(a_ref, mine_ref, other_ref, o_ref):
    low = lax.broadcasted_iota(jnp.int32, (64, 128), 1) < 64
    for b in range(o_ref.shape[0]):
        piece = mine_ref[b].astype(F32) + other_ref[b].astype(F32)
        o_ref[b, 0:64, :] = jnp.where(low, a_ref[b, 0:64, :].astype(F32), piece).astype(BF)
        o_ref[b, 64:72, :] = a_ref[b, 64:72, :]


def part_kernel(r_ref, o_ref):
    low = lax.broadcasted_iota(jnp.int32, (32, 128), 1) < 64
    for b in range(o_ref.shape[0]):
        upper = pltpu.roll(r_ref[b, 0:32, 256:384].astype(F32), 64, 1)
        lower = r_ref[b, 32:64, 256:384].astype(F32)
        o_ref[b] = jnp.where(low, upper, lower).astype(BF)


def head_kernel(r_ref, conv_ref, stats_ref, gain_ref, o_ref, h_ref):
    tokens = conv_ref.shape[1]
    total = r_ref[0, :, 0:tokens].astype(F32)
    for b in range(1, r_ref.shape[0]):
        total = total + r_ref[b, :, 0:tokens].astype(F32)
    channels = 16 * conv_ref.shape[0]
    first = (total[64:65] + total[65:66]) / channels
    second = (total[66:67] + total[67:68]) / channels
    inv = stats_ref[1:2, :]
    normed = (conv_ref[...].astype(F32) - stats_ref[0:1, :]) * inv
    gain = gain_ref[...]
    linear = normed * gain
    s = jax.nn.sigmoid(linear)
    cot = total[0:64] * s * (1.0 + linear * (1.0 - s)) * gain
    cot = inv * (cot - first - normed * second)
    o_ref[...] = cot
    h_ref[...] = cot[:, 0:128]


def sum_kernel(a_ref, o_ref):
    total = a_ref[0].astype(F32)
    for b in range(1, a_ref.shape[0]):
        total = total + a_ref[b].astype(F32)
    turned = pltpu.roll(total, 64, 1)
    block = jnp.concatenate([total, turned], axis=0)
    o_ref[...] = block.T[0:64, :]


def sum_side_kernel(p_ref, o_ref):
    total = p_ref[0].astype(F32)
    for a in range(1, SIDE):
        total = total + p_ref[a].astype(F32)
    o_ref[...] = total.astype(BF)


def conv_kernel(cot_ref, next_ref, taps_ref, gate_ref, value_ref, v_ref, g_ref, buf):
    rows, tokens = cot_ref.shape
    wide = buf.shape[1]
    reach = taps_ref.shape[1] - 1
    buf[:, 0:128] = next_ref[...]
    buf[:, 128:wide] = jnp.zeros((rows, wide - 128), F32)
    after = pltpu.roll(buf[...], tokens, 1)
    buf[:, 0:tokens] = cot_ref[...]
    lane = lax.broadcasted_iota(jnp.int32, (rows, wide), 1)
    whole = jnp.where(lane < tokens, buf[...], after)
    taps = taps_ref[...]
    total = whole * taps[:, reach : reach + 1]
    for s in range(1, reach + 1):
        total = total + pltpu.roll(whole, wide - s, 1) * taps[:, reach - s : reach - s + 1]
    cot = total[:, 0:tokens]
    s = jax.nn.sigmoid(gate_ref[...].astype(F32))
    v_ref[...] = (cot * s).astype(BF)
    g_ref[...] = (cot * value_ref[...].astype(F32) * s * (1.0 - s)).astype(BF)


def whole(shape, dtype):
    return jax.ShapeDtypeStruct(shape, dtype)


def body(
    moe_input,
    out_cotangent,
    routes,
    route_weight,
    gate_weight,
    up_weight,
    down_weight,
    glu_value,
    glu_gate,
    conv_result,
    conv_taps,
    norm_gain,
    proj_weight,
):
    sp_count = lax.axis_size(SP)
    tp_count = lax.axis_size(TP)
    tokens = moe_input.shape[0]
    slots = sp_count * SLOT
    feature_groups, unit_groups = plane_groups()
    smem = pl.BlockSpec(memory_space=pltpu.SMEM)
    vmem = pl.BlockSpec(memory_space=VM)
    room = pltpu.CompilerParams(vmem_limit_bytes=ROOM)

    sent, target = pl.pallas_call(
        route_kernel,
        out_shape=(whole((slots, 256), BF), whole((2, tokens), jnp.int32)),
        in_specs=[vmem] * 4,
        out_specs=(vmem, vmem),
        cost_estimate=cost(400000000, 2000000),
        name="route",
    )(routes.T, route_weight.T, moe_input, out_cotangent)
    sent, target, table, gate_weight, conv_result, norm_gain = lax.optimization_barrier(
        (sent, target, jnp.asarray(step_tables()), gate_weight, conv_result, norm_gain)
    )
    at = table[lax.axis_index(PLANE)]
    pick = pl.pallas_call(
        pick_kernel,
        out_shape=whole((slots, tokens), BF),
        in_specs=[vmem],
        out_specs=vmem,
        compiler_params=room,
        cost_estimate=cost(1000000, 700000),
        name="pick",
    )(target)
    conv_t = conv_result.T
    gain = norm_gain.reshape(-1, 1)
    high = lax.reduce_precision(gain, 8, 7)
    middle = lax.reduce_precision(gain - high, 8, 7)
    pieces = jnp.concatenate([high, middle, gain - high - middle], axis=1).astype(BF)
    channel_part = jnp.concatenate(
        [jnp.zeros((64, 128), BF), conv_t, pieces, jnp.zeros((64, 61), BF)], axis=1
    )
    split = pl.pallas_call(
        split_kernel,
        out_shape=(whole((320, 512), BF),) * SIDE,
        in_specs=[smem] + [vmem] * 5,
        out_specs=(vmem,) * SIDE,
        compiler_params=room,
        cost_estimate=cost(1000000, 2600000),
        name="split_weights",
    )(at, gate_weight[0], up_weight[0], down_weight[0], proj_weight, channel_part)
    weights = pass_on(split, unit_groups)
    relay = pl.pallas_call(
        relay_kernel,
        out_shape=(whole((256, 512), BF),) * SIDE,
        in_specs=[smem] + [vmem] * SIDE,
        out_specs=(vmem,) * SIDE,
        compiler_params=room,
        cost_estimate=cost(1000000, 2000000),
        name="relay",
    )(at, *weights)
    got = lax.all_to_all(sent.reshape(sp_count, SLOT, 256), SP, 0, 0, tiled=True)
    got = got.reshape(slots, 256)
    got, weights, relay = lax.optimization_barrier((got, weights, relay))
    taps_t = conv_taps.T

    rows = exchange(jnp.broadcast_to(got[None], (SIDE, slots, 256)), feature_groups)
    step = 256
    pre = pl.pallas_call(
        pre_kernel,
        grid=(slots // step,),
        out_shape=whole((SIDE, 192, slots), BF),
        in_specs=[smem, pl.BlockSpec((SIDE, step, 256), lambda i: (0, i, 0))]
        + [pl.BlockSpec((192, 512), lambda i: (0, 0))] * SIDE,
        out_specs=pl.BlockSpec((SIDE, 192, step), lambda i: (0, 0, i)),
        compiler_params=room,
        cost_estimate=cost(800000000, 4400000),
        name="pre",
    )(at, rows, *weights)
    pre = exchange(pre, unit_groups)
    hidden = pl.pallas_call(
        gate_kernel,
        grid=(slots // step,),
        out_shape=whole((SIDE, 192, slots), BF),
        in_specs=[pl.BlockSpec((SIDE, 192, step), lambda i: (0, 0, i))],
        out_specs=pl.BlockSpec((SIDE, 192, step), lambda i: (0, 0, i)),
        compiler_params=room,
        cost_estimate=cost(3000000, 3200000),
        name="gates",
    )(pre)
    hidden = exchange(hidden, unit_groups)
    part = pl.pallas_call(
        partial_kernel,
        grid=(slots // step,),
        out_shape=whole((SIDE, slots, 128), BF),
        in_specs=[smem, pl.BlockSpec((SIDE, 192, step), lambda i: (0, 0, i))]
        + [pl.BlockSpec((192, 512), lambda i: (0, 0))] * SIDE,
        out_specs=pl.BlockSpec((SIDE, step, 128), lambda i: (0, i, 0)),
        compiler_params=room,
        cost_estimate=cost(540000000, 3400000),
        name="partial",
    )(at, hidden, *weights)
    part = exchange(part, feature_groups)
    back = pl.pallas_call(
        sum_side_kernel,
        out_shape=whole((slots, 128), BF),
        in_specs=[vmem],
        out_specs=vmem,
        compiler_params=room,
        cost_estimate=cost(1000000, 1300000),
        name="sum_side",
    )(part).reshape(sp_count, SLOT, 128)
    back, relay = lax.optimization_barrier((back, relay))
    relay = pass_on(relay, feature_groups)
    returned = lax.all_to_all(back, SP, 0, 0, tiled=True).reshape(slots, 128)

    grads = pl.pallas_call(
        grads_kernel,
        grid=(SIDE // 2,),
        out_shape=(whole((192, 512), BF),) * SIDE,
        in_specs=[
            smem,
            pl.BlockSpec((SIDE, 192, slots), lambda i: (0, 0, 0)),
            pl.BlockSpec((2, slots, 256), lambda i: (i, 0, 0)),
        ],
        out_specs=(pl.BlockSpec((192, 256), lambda i: (0, i)),) * SIDE,
        compiler_params=room,
        cost_estimate=cost(800000000, 4400000),
        name="grads",
    )(at, hidden, rows)
    returned, grads = lax.optimization_barrier((returned, grads))

    wide = 384
    mine, other, total_cot, stats = pl.pallas_call(
        total_kernel,
        out_shape=(
            whole((tp_count, 64, 128), BF),
            whole((tp_count, 64, 128), BF),
            whole((wide, 128), BF),
            whole((2, tokens), F32),
        ),
        in_specs=[smem] + [vmem] * 7,
        out_specs=(vmem,) * 4,
        compiler_params=room,
        cost_estimate=cost(170000000, 2500000),
        name="total_cot",
    )(at, pick, returned, out_cotangent, *relay)
    other = lax.ppermute(other, "c", [(0, 1), (1, 0)])
    act_part = pl.pallas_call(
        cot_kernel,
        out_shape=whole((tp_count, 72, wide), BF),
        in_specs=[smem] + [vmem] * 6,
        out_specs=vmem,
        compiler_params=room,
        cost_estimate=cost(100000000, 2500000),
        name="act_cot",
    )(at, total_cot, stats, *relay)
    act_part = pl.pallas_call(
        join_kernel,
        grid=(1,),
        out_shape=whole((tp_count, 72, wide), BF),
        in_specs=[
            pl.BlockSpec((tp_count, 72, 128), lambda i: (0, 0, 2)),
            pl.BlockSpec((tp_count, 64, 128), lambda i: (0, 0, 0)),
            pl.BlockSpec((tp_count, 64, 128), lambda i: (0, 0, 0)),
        ],
        out_specs=pl.BlockSpec((tp_count, 72, 128), lambda i: (0, 0, 2)),
        input_output_aliases={0: 0},
        compiler_params=room,
        cost_estimate=cost(100000, 1200000),
        name="join_cores",
    )(act_part, mine, other)
    act_part, grads = lax.optimization_barrier((act_part, grads))
    act_part = lax.all_to_all(act_part, TP, 0, 0, tiled=True)
    proj_part = pl.pallas_call(
        part_kernel,
        out_shape=whole((tp_count, 32, 128), BF),
        in_specs=[vmem],
        out_specs=vmem,
        compiler_params=room,
        cost_estimate=cost(100000, 400000),
        name="proj_part",
    )(act_part)
    near = [shift(grads[k], unit_groups, k) for k in (1, 3)]
    act_part, proj_part, last = lax.optimization_barrier((act_part, proj_part, grads[2]))
    grads = (grads[0], near[0], shift(last, unit_groups, 2), near[1])
    proj_part = lax.all_to_all(proj_part, "z", 0, 0, tiled=True)
    grad_proj = pl.pallas_call(
        sum_kernel,
        out_shape=whole((64, 64), F32),
        in_specs=[vmem],
        out_specs=vmem,
        compiler_params=room,
        cost_estimate=cost(100000, 200000),
        name="sum_planes",
    )(proj_part)

    conv_cot, head = pl.pallas_call(
        head_kernel,
        out_shape=(whole((64, tokens), F32), whole((64, 128), F32)),
        in_specs=[vmem] * 4,
        out_specs=(vmem, vmem),
        compiler_params=room,
        cost_estimate=cost(3000000, 1200000),
        name="conv_cot",
    )(act_part, conv_t, stats, gain)
    behind = [(i + 1, i) for i in range(sp_count - 1)]
    after = lax.ppermute(head, SP, behind)
    value, gate = pl.pallas_call(
        conv_kernel,
        out_shape=(whole((64, tokens), BF), whole((64, tokens), BF)),
        in_specs=[vmem] * 5,
        out_specs=(vmem, vmem),
        scratch_shapes=[VM((64, 384), F32)],
        compiler_params=room,
        cost_estimate=cost(4000000, 400000),
        name="conv",
    )(conv_cot, after, taps_t, glu_gate.T, glu_value.T)

    grad_gate, grad_up, grad_down = pl.pallas_call(
        merge_kernel,
        out_shape=(whole((64, 2048), F32),) * 3,
        in_specs=[smem] + [vmem] * SIDE,
        out_specs=(vmem,) * 3,
        compiler_params=room,
        cost_estimate=cost(1000000, 2400000),
        name="merge_grads",
    )(at, *grads)
    return (
        grad_gate[None],
        grad_up[None],
        grad_down[None],
        grad_proj,
        value.T,
        gate.T,
    )


def solution(mesh):
    split = Mesh(mesh.devices.reshape(16, 2, SIDE, SIDE), ("z", "c", "y", "x"))
    placed = (
        P(SP, TP),
        P(SP, TP),
        P(SP, None),
        P(SP, None),
        P(SP, TP, None),
        P(SP, TP, None),
        P(SP, TP, None),
        P(SP, TP),
        P(SP, TP),
        P(SP, TP),
        P(None, TP),
        P(TP),
        P(TP, None),
    )
    return jax.shard_map(
        body,
        mesh=split,
        in_specs=placed,
        out_specs=(
            P(SP, TP, None),
            P(SP, TP, None),
            P(SP, TP, None),
            P(SP, TP),
            P(SP, TP),
            P(SP, TP),
        ),
        check_vma=False,
    )
```

```python
import jax
import jax.numpy as jnp
import numpy as np
from jax import lax
from jax.experimental import pallas as pl
from jax.experimental.pallas import tpu as pltpu
from jax.sharding import Mesh
from jax.sharding import PartitionSpec as P

NORM_EPS = 0.25
SP = ("z", "c")
TP = ("y", "x")
PLANE = ("c", "y", "x")
SIDE = 4
SLOT = 32
ROOM = 12 << 20
BF = jnp.bfloat16
F32 = jnp.float32
VM = pltpu.VMEM

NT = (((1,), (1,)), ((), ()))
TN = (((0,), (0,)), ((), ()))
NN = (((1,), (0,)), ((), ()))


def place(core, row, col):
    return core * SIDE * SIDE + row * SIDE + col


def plane_groups():
    r = range(SIDE)
    down = [[[place(k, y, x) for y in r] for x in r] for k in (0, 1)]
    across = [[[place(k, y, x) for x in r] for y in r] for k in (0, 1)]
    return down[0] + across[1], across[0] + down[1]


def step_tables():
    features, units = plane_groups()
    of_features = {p: g for g in features for p in g}
    table = np.zeros((2 * SIDE * SIDE, 64), np.int32)
    for group in units:
        for me, p in enumerate(group):
            table[p, 0] = me
            table[p, 1] = of_features[p].index(p)
            table[p, 2] = p // (SIDE * SIDE)
            for k in range(SIDE):
                ahead = of_features[group[(me + k) % SIDE]]
                back = of_features[group[(me - k) % SIDE]]
                for a in range(SIDE):
                    table[p, 16 + k * SIDE + a] = ahead[a] % (SIDE * SIDE)
                    table[p, 32 + k * SIDE + a] = back[a] % (SIDE * SIDE)
    of_units = {p: g for g in units for p in g}
    for p in range(2 * SIDE * SIDE):
        group = of_features[p]
        for j in range(SIDE):
            source = group[(group.index(p) - j) % SIDE]
            their = of_units[source]
            for k in range(SIDE):
                first = their[(their.index(source) - k) % SIDE]
                table[p, 48 + j * SIDE + k] = first % (SIDE * SIDE)
    return table


def steps_ahead(groups, k):
    return [(g[i], g[(i + k) % SIDE]) for g in groups for i in range(SIDE)]


def shift(part, groups, k):
    return lax.ppermute(part, PLANE, steps_ahead(groups, k))


def pass_on(parts, groups):
    return (parts[0],) + tuple(shift(parts[k], groups, k) for k in range(1, SIDE))


def mm(a, b, dims):
    return lax.dot_general(a, b, dims, preferred_element_type=F32)


def exchange(v, groups):
    return lax.all_to_all(v, PLANE, 0, 0, axis_index_groups=groups, tiled=True)


def cost(flops, nbytes):
    return pl.CostEstimate(flops=flops, bytes_accessed=nbytes, transcendentals=0)


def route_kernel(rt_ref, w_ref, x_ref, c_ref, s_ref, t_ref):
    tokens = rt_ref.shape[1]
    experts = s_ref.shape[0] // SLOT
    first, second = rt_ref[0:1, :], rt_ref[1:2, :]
    ids = lax.broadcasted_iota(jnp.int32, (experts, tokens), 0)
    o0, o1 = ids == first, ids == second
    both = jnp.where(o0 | o1, 1.0, 0.0).astype(BF)
    before = lax.broadcasted_iota(jnp.int32, (tokens, tokens), 0) < lax.broadcasted_iota(
        jnp.int32, (tokens, tokens), 1
    )
    earlier = mm(both, jnp.where(before, 1.0, 0.0).astype(BF), NN)
    rank0 = jnp.sum(jnp.where(o0, earlier, 0.0), axis=0, keepdims=True)
    rank1 = jnp.sum(jnp.where(o1, earlier, 0.0), axis=0, keepdims=True)
    t0 = first * SLOT + rank0.astype(jnp.int32)
    t1 = second * SLOT + rank1.astype(jnp.int32)
    t_ref[0:1, :] = t0
    t_ref[1:2, :] = t1
    w0, w1 = w_ref[0:1, :], w_ref[1:2, :]
    x, c = x_ref[...], c_ref[...]
    size = 128
    for k in range(s_ref.shape[0] // size):
        slots = lax.broadcasted_iota(jnp.int32, (size, tokens), 0) + k * size
        m0, m1 = slots == t0, slots == t1
        pick = jnp.where(m0 | m1, 1.0, 0.0).astype(BF)
        weight = jnp.sum(
            jnp.where(m0, w0, 0.0) + jnp.where(m1, w1, 0.0), axis=1, keepdims=True
        )
        rows = pl.ds(k * size, size)
        s_ref[rows, 0:128] = mm(pick, x, NN).astype(BF)
        s_ref[rows, 128:256] = (weight * mm(pick, c, NN)).astype(BF)


def pick_kernel(t_ref, p_ref):
    slots = lax.broadcasted_iota(jnp.int32, p_ref.shape, 0)
    held = (slots == t_ref[0:1, :]) | (slots == t_ref[1:2, :])
    p_ref[...] = jnp.where(held, 1.0, 0.0).astype(BF)


def split_kernel(at_ref, g_ref, u_ref, d_ref, p_ref, c_ref, *outs):
    for k, out in enumerate(outs):
        for a in range(SIDE):
            at = at_ref[16 + k * SIDE + a]
            cols = pl.ds(pl.multiple_of(at * 128, 128), 128)
            for q, ref in enumerate((g_ref, u_ref, d_ref, p_ref)):
                out[q * 64 : q * 64 + 64, a * 128 : a * 128 + 128] = ref[:, cols]
        out[256:320, :] = c_ref[...]


def relay_kernel(at_ref, r0, r1, r2, r3, *outs):
    for j, out in enumerate(outs):
        a = lax.rem(at_ref[1] + j, SIDE)
        cols = pl.ds(pl.multiple_of(a * 128, 128), 128)
        for k, r_ref in enumerate((r0, r1, r2, r3)):
            out[k * 64 : k * 64 + 64, 0:128] = r_ref[192:256, cols]
            out[k * 64 : k * 64 + 64, 128:512] = r_ref[256:320, 128:512]


def merge_kernel(at_ref, s0, s1, s2, s3, g_ref, u_ref, d_ref):
    for k, s_ref in enumerate((s0, s1, s2, s3)):
        for a in range(SIDE):
            at = at_ref[32 + k * SIDE + a]
            cols = pl.ds(pl.multiple_of(at * 128, 128), 128)
            for q, ref in enumerate((g_ref, u_ref, d_ref)):
                ref[:, cols] = s_ref[
                    q * 64 : q * 64 + 64, a * 128 : a * 128 + 128
                ].astype(F32)


def behind_of(at_ref, k):
    return lax.rem(at_ref[0] + (SIDE - k), SIDE)


def ahead_of(at_ref, k):
    return lax.rem(at_ref[0] + k, SIDE)


def pre_kernel(at_ref, a_ref, w0, w1, w2, w3, o_ref):
    ws = (w0, w1, w2, w3)
    x = jnp.concatenate([a_ref[i, :, 0:128] for i in range(SIDE)], axis=1)
    c = jnp.concatenate([a_ref[i, :, 128:256] for i in range(SIDE)], axis=1)
    pairs = mm(jnp.concatenate([w[0:128, :] for w in ws], axis=0), x, NT)
    downs = mm(jnp.concatenate([w[128:192, :] for w in ws], axis=0), c, NT)
    for k in range(SIDE):
        b = behind_of(at_ref, k)
        o_ref[b, 0:128, :] = pairs[k * 128 : k * 128 + 128].astype(BF)
        o_ref[b, 128:192, :] = downs[k * 64 : k * 64 + 64].astype(BF)


def gate_kernel(p_ref, o_ref):
    total = p_ref[0].astype(F32)
    for b in range(1, SIDE):
        total = total + p_ref[b].astype(F32)
    gate, up, cot = total[0:64], total[64:128], total[128:192]
    s = jax.nn.sigmoid(gate)
    act = gate * s
    hidden = (act * up).astype(BF)
    up_cot = (cot * act).astype(BF)
    gate_cot = (cot * up * s * (1.0 + gate * (1.0 - s))).astype(BF)
    for b in range(SIDE):
        o_ref[b, 0:64, :] = gate_cot
        o_ref[b, 64:128, :] = up_cot
        o_ref[b, 128:192, :] = hidden


def partial_kernel(at_ref, h_ref, w0, w1, w2, w3, o_ref):
    ws = (w0, w1, w2, w3)
    h = jnp.concatenate([h_ref[behind_of(at_ref, k), 0:128, :] for k in range(SIDE)], axis=0)
    w = jnp.concatenate([w_ref[0:128, :] for w_ref in ws], axis=0)
    total = mm(h, w, TN)
    for a in range(SIDE):
        o_ref[a] = total[:, a * 128 : a * 128 + 128].astype(BF)


def grads_kernel(at_ref, h_ref, a_ref, *outs):
    x = jnp.concatenate([a_ref[0, :, 0:128], a_ref[1, :, 0:128]], axis=1)
    c = jnp.concatenate([a_ref[0, :, 128:256], a_ref[1, :, 128:256]], axis=1)
    order = [ahead_of(at_ref, k) for k in range(SIDE)]
    pairs = mm(jnp.concatenate([h_ref[b, 0:128, :] for b in order], axis=0), x, NN)
    downs = mm(jnp.concatenate([h_ref[b, 128:192, :] for b in order], axis=0), c, NN)
    for k, out in enumerate(outs):
        out[0:128, :] = pairs[k * 128 : k * 128 + 128].astype(BF)
        out[128:192, :] = downs[k * 64 : k * 64 + 64].astype(BF)


def total_kernel(
    at_ref, p_ref, r_ref, c_ref, q0, q1, q2, q3, mine_ref, other_ref, total_ref, stats_ref
):
    qs = (q0, q1, q2, q3)
    moe = mm(p_ref[...], r_ref[...], TN)
    total = (c_ref[...].astype(F32) + moe).astype(BF)
    tokens = total.shape[0]
    total_ref[0:tokens, :] = total
    total_ref[tokens:, :] = jnp.zeros((total_ref.shape[0] - tokens, 128), BF)
    size = q0.shape[0]
    channels = SIDE * size
    mean = jnp.zeros((1, tokens), F32)
    for q in qs:
        conv = q[:, 128 : 128 + tokens].astype(F32)
        mean = mean + jnp.sum(conv, axis=0, keepdims=True)
    mean = mean / channels
    var = jnp.zeros((1, tokens), F32)
    for q in qs:
        off = q[:, 128 : 128 + tokens].astype(F32) - mean
        var = var + jnp.sum(off * off, axis=0, keepdims=True)
    inv = lax.rsqrt(var / channels + NORM_EPS)
    stats_ref[0:1, :] = mean
    stats_ref[1:2, :] = inv
    own = jnp.full((64, 128), at_ref[2], jnp.int32) == 0
    for j, q in enumerate(qs):
        normed = (q[:, 128 : 128 + tokens].astype(F32) - mean) * inv
        linear = normed * gain_of(q)
        act = (linear * jax.nn.sigmoid(linear)).astype(BF)
        grad = mm(act, total, NN)
        turned = pltpu.roll(grad, 64, 1)
        for k in range(SIDE):
            b = at_ref[48 + j * SIDE + k]
            rows = slice(k * 64, k * 64 + 64)
            mine_ref[b] = jnp.where(own, turned[rows], grad[rows]).astype(BF)
            other_ref[b] = jnp.where(own, grad[rows], turned[rows]).astype(BF)


def gain_of(q):
    lane = lax.broadcasted_iota(jnp.int32, (q.shape[0], 128), 1)
    pieces = jnp.where((lane >= 64) & (lane < 67), q[:, 384:512].astype(F32), 0.0)
    return jnp.sum(pieces, axis=1, keepdims=True)


def cot_kernel(at_ref, total_ref, stats_ref, q0, q1, q2, q3, o_ref):
    wide = total_ref.shape[0]
    tokens = stats_ref.shape[1]
    total = total_ref[...]
    mean, inv = stats_ref[0:1, :], stats_ref[1:2, :]
    first = jnp.zeros((1, tokens), F32)
    second = jnp.zeros((1, tokens), F32)
    for j, q in enumerate((q0, q1, q2, q3)):
        normed = (q[:, 128 : 128 + tokens].astype(F32) - mean) * inv
        gain = gain_of(q)
        linear = normed * gain
        s = jax.nn.sigmoid(linear)
        cot = mm(q[:, 0:128], total, NT)
        sloped = cot[:, 0:tokens] * (s * (1.0 + linear * (1.0 - s)) * gain)
        first = first + jnp.sum(sloped, axis=0, keepdims=True)
        second = second + jnp.sum(sloped * normed, axis=0, keepdims=True)
        for k in range(SIDE):
            o_ref[at_ref[48 + j * SIDE + k], 0:64, :] = cot[k * 64 : k * 64 + 64].astype(BF)
    row = lax.broadcasted_iota(jnp.int32, (8, tokens), 0)
    sums = jnp.zeros((8, tokens), F32)
    for i, v in enumerate((first, second)):
        head = v.astype(BF).astype(F32)
        sums = jnp.where(row == 2 * i, head, jnp.where(row == 2 * i + 1, v - head, sums))
    for b in range(o_ref.shape[0]):
        o_ref[b, 64:72, 0:tokens] = sums.astype(BF)
        o_ref[b, 64:72, tokens:wide] = jnp.zeros((8, wide - tokens), BF)


def join_kernel(a_ref, mine_ref, other_ref, o_ref):
    low = lax.broadcasted_iota(jnp.int32, (64, 128), 1) < 64
    for b in range(o_ref.shape[0]):
        piece = mine_ref[b].astype(F32) + other_ref[b].astype(F32)
        o_ref[b, :, 0:256] = a_ref[b, :, 0:256]
        o_ref[b, 0:64, 256:384] = jnp.where(
            low, a_ref[b, 0:64, 256:384].astype(F32), piece
        ).astype(BF)
        o_ref[b, 64:72, 256:384] = a_ref[b, 64:72, 256:384]


def part_kernel(r_ref, o_ref):
    low = lax.broadcasted_iota(jnp.int32, (32, 128), 1) < 64
    for b in range(o_ref.shape[0]):
        upper = pltpu.roll(r_ref[b, 0:32, 256:384].astype(F32), 64, 1)
        lower = r_ref[b, 32:64, 256:384].astype(F32)
        o_ref[b] = jnp.where(low, upper, lower).astype(BF)


def head_kernel(r_ref, conv_ref, stats_ref, gain_ref, o_ref, h_ref):
    tokens = conv_ref.shape[1]
    total = r_ref[0, :, 0:tokens].astype(F32)
    for b in range(1, r_ref.shape[0]):
        total = total + r_ref[b, :, 0:tokens].astype(F32)
    channels = 16 * conv_ref.shape[0]
    first = (total[64:65] + total[65:66]) / channels
    second = (total[66:67] + total[67:68]) / channels
    inv = stats_ref[1:2, :]
    normed = (conv_ref[...].astype(F32) - stats_ref[0:1, :]) * inv
    gain = gain_ref[...]
    linear = normed * gain
    s = jax.nn.sigmoid(linear)
    cot = total[0:64] * s * (1.0 + linear * (1.0 - s)) * gain
    cot = inv * (cot - first - normed * second)
    o_ref[...] = cot
    h_ref[...] = cot[:, 0:128]


def sum_kernel(a_ref, o_ref):
    total = a_ref[0].astype(F32)
    for b in range(1, a_ref.shape[0]):
        total = total + a_ref[b].astype(F32)
    turned = pltpu.roll(total, 64, 1)
    block = jnp.concatenate([total, turned], axis=0)
    o_ref[...] = block.T[0:64, :]


def sum_side_kernel(p_ref, o_ref):
    total = p_ref[0].astype(F32)
    for a in range(1, SIDE):
        total = total + p_ref[a].astype(F32)
    o_ref[...] = total.astype(BF)


def conv_kernel(cot_ref, next_ref, taps_ref, gate_ref, value_ref, v_ref, g_ref, buf):
    rows, tokens = cot_ref.shape
    wide = buf.shape[1]
    reach = taps_ref.shape[1] - 1
    buf[:, 0:128] = next_ref[...]
    buf[:, 128:wide] = jnp.zeros((rows, wide - 128), F32)
    after = pltpu.roll(buf[...], tokens, 1)
    buf[:, 0:tokens] = cot_ref[...]
    lane = lax.broadcasted_iota(jnp.int32, (rows, wide), 1)
    whole = jnp.where(lane < tokens, buf[...], after)
    taps = taps_ref[...]
    total = whole * taps[:, reach : reach + 1]
    for s in range(1, reach + 1):
        total = total + pltpu.roll(whole, wide - s, 1) * taps[:, reach - s : reach - s + 1]
    cot = total[:, 0:tokens]
    s = jax.nn.sigmoid(gate_ref[...].astype(F32))
    v_ref[...] = (cot * s).astype(BF)
    g_ref[...] = (cot * value_ref[...].astype(F32) * s * (1.0 - s)).astype(BF)


def whole(shape, dtype):
    return jax.ShapeDtypeStruct(shape, dtype)


def body(
    moe_input,
    out_cotangent,
    routes,
    route_weight,
    gate_weight,
    up_weight,
    down_weight,
    glu_value,
    glu_gate,
    conv_result,
    conv_taps,
    norm_gain,
    proj_weight,
):
    sp_count = lax.axis_size(SP)
    tp_count = lax.axis_size(TP)
    tokens = moe_input.shape[0]
    slots = sp_count * SLOT
    feature_groups, unit_groups = plane_groups()
    smem = pl.BlockSpec(memory_space=pltpu.SMEM)
    vmem = pl.BlockSpec(memory_space=VM)
    room = pltpu.CompilerParams(vmem_limit_bytes=ROOM)

    sent, target = pl.pallas_call(
        route_kernel,
        out_shape=(whole((slots, 256), BF), whole((2, tokens), jnp.int32)),
        in_specs=[vmem] * 4,
        out_specs=(vmem, vmem),
        cost_estimate=cost(400000000, 2000000),
        name="route",
    )(routes.T, route_weight.T, moe_input, out_cotangent)
    sent, target, table, gate_weight, conv_result, norm_gain = lax.optimization_barrier(
        (sent, target, jnp.asarray(step_tables()), gate_weight, conv_result, norm_gain)
    )
    at = table[lax.axis_index(PLANE)]
    pick = pl.pallas_call(
        pick_kernel,
        out_shape=whole((slots, tokens), BF),
        in_specs=[vmem],
        out_specs=vmem,
        compiler_params=room,
        cost_estimate=cost(1000000, 700000),
        name="pick",
    )(target)
    conv_t = conv_result.T
    gain = norm_gain.reshape(-1, 1)
    high = lax.reduce_precision(gain, 8, 7)
    middle = lax.reduce_precision(gain - high, 8, 7)
    pieces = jnp.concatenate([high, middle, gain - high - middle], axis=1).astype(BF)
    channel_part = jnp.concatenate(
        [jnp.zeros((64, 128), BF), conv_t, pieces, jnp.zeros((64, 61), BF)], axis=1
    )
    split = pl.pallas_call(
        split_kernel,
        out_shape=(whole((320, 512), BF),) * SIDE,
        in_specs=[smem] + [vmem] * 5,
        out_specs=(vmem,) * SIDE,
        compiler_params=room,
        cost_estimate=cost(1000000, 2600000),
        name="split_weights",
    )(at, gate_weight[0], up_weight[0], down_weight[0], proj_weight, channel_part)
    weights = pass_on(split, unit_groups)
    relay = pl.pallas_call(
        relay_kernel,
        out_shape=(whole((256, 512), BF),) * SIDE,
        in_specs=[smem] + [vmem] * SIDE,
        out_specs=(vmem,) * SIDE,
        compiler_params=room,
        cost_estimate=cost(1000000, 2000000),
        name="relay",
    )(at, *weights)
    got = lax.all_to_all(sent.reshape(sp_count, SLOT, 256), SP, 0, 0, tiled=True)
    got = got.reshape(slots, 256)
    got, weights, relay = lax.optimization_barrier((got, weights, relay))
    taps_t = conv_taps.T

    rows = exchange(jnp.broadcast_to(got[None], (SIDE, slots, 256)), feature_groups)
    step = 256
    pre = pl.pallas_call(
        pre_kernel,
        grid=(slots // step,),
        out_shape=whole((SIDE, 192, slots), BF),
        in_specs=[smem, pl.BlockSpec((SIDE, step, 256), lambda i: (0, i, 0))]
        + [pl.BlockSpec((192, 512), lambda i: (0, 0))] * SIDE,
        out_specs=pl.BlockSpec((SIDE, 192, step), lambda i: (0, 0, i)),
        compiler_params=room,
        cost_estimate=cost(800000000, 4400000),
        name="pre",
    )(at, rows, *weights)
    pre = exchange(pre, unit_groups)
    hidden = pl.pallas_call(
        gate_kernel,
        grid=(slots // step,),
        out_shape=whole((SIDE, 192, slots), BF),
        in_specs=[pl.BlockSpec((SIDE, 192, step), lambda i: (0, 0, i))],
        out_specs=pl.BlockSpec((SIDE, 192, step), lambda i: (0, 0, i)),
        compiler_params=room,
        cost_estimate=cost(3000000, 3200000),
        name="gates",
    )(pre)
    hidden = exchange(hidden, unit_groups)
    part = pl.pallas_call(
        partial_kernel,
        grid=(slots // step,),
        out_shape=whole((SIDE, slots, 128), BF),
        in_specs=[smem, pl.BlockSpec((SIDE, 192, step), lambda i: (0, 0, i))]
        + [pl.BlockSpec((192, 512), lambda i: (0, 0))] * SIDE,
        out_specs=pl.BlockSpec((SIDE, step, 128), lambda i: (0, i, 0)),
        compiler_params=room,
        cost_estimate=cost(540000000, 3400000),
        name="partial",
    )(at, hidden, *weights)
    part = exchange(part, feature_groups)
    back = pl.pallas_call(
        sum_side_kernel,
        out_shape=whole((slots, 128), BF),
        in_specs=[vmem],
        out_specs=vmem,
        compiler_params=room,
        cost_estimate=cost(1000000, 1300000),
        name="sum_side",
    )(part).reshape(sp_count, SLOT, 128)
    back, relay = lax.optimization_barrier((back, relay))
    relay = pass_on(relay, feature_groups)
    returned = lax.all_to_all(back, SP, 0, 0, tiled=True).reshape(slots, 128)

    grads = pl.pallas_call(
        grads_kernel,
        grid=(SIDE // 2,),
        out_shape=(whole((192, 512), BF),) * SIDE,
        in_specs=[
            smem,
            pl.BlockSpec((SIDE, 192, slots), lambda i: (0, 0, 0)),
            pl.BlockSpec((2, slots, 256), lambda i: (i, 0, 0)),
        ],
        out_specs=(pl.BlockSpec((192, 256), lambda i: (0, i)),) * SIDE,
        compiler_params=room,
        cost_estimate=cost(800000000, 4400000),
        name="grads",
    )(at, hidden, rows)
    returned, grads = lax.optimization_barrier((returned, grads))

    wide = 384
    mine, other, total_cot, stats = pl.pallas_call(
        total_kernel,
        out_shape=(
            whole((tp_count, 64, 128), BF),
            whole((tp_count, 64, 128), BF),
            whole((wide, 128), BF),
            whole((2, tokens), F32),
        ),
        in_specs=[smem] + [vmem] * 7,
        out_specs=(vmem,) * 4,
        compiler_params=room,
        cost_estimate=cost(170000000, 2500000),
        name="total_cot",
    )(at, pick, returned, out_cotangent, *relay)
    other = lax.ppermute(other, "c", [(0, 1), (1, 0)])
    act_part = pl.pallas_call(
        cot_kernel,
        out_shape=whole((tp_count, 72, wide), BF),
        in_specs=[smem] + [vmem] * 6,
        out_specs=vmem,
        compiler_params=room,
        cost_estimate=cost(100000000, 2500000),
        name="act_cot",
    )(at, total_cot, stats, *relay)
    act_part = pl.pallas_call(
        join_kernel,
        grid=(2,),
        out_shape=whole((tp_count, 72, wide), BF),
        in_specs=[
            pl.BlockSpec((8, 72, wide), lambda i: (i, 0, 0)),
            pl.BlockSpec((8, 64, 128), lambda i: (i, 0, 0)),
            pl.BlockSpec((8, 64, 128), lambda i: (i, 0, 0)),
        ],
        out_specs=pl.BlockSpec((8, 72, wide), lambda i: (i, 0, 0)),
        compiler_params=room,
        cost_estimate=cost(100000, 2200000),
        name="join_cores",
    )(act_part, mine, other)
    act_part, grads = lax.optimization_barrier((act_part, grads))
    act_part = lax.all_to_all(act_part, TP, 0, 0, tiled=True)
    proj_part = pl.pallas_call(
        part_kernel,
        out_shape=whole((tp_count, 32, 128), BF),
        in_specs=[vmem],
        out_specs=vmem,
        compiler_params=room,
        cost_estimate=cost(100000, 400000),
        name="proj_part",
    )(act_part)
    near = [shift(grads[k], unit_groups, k) for k in (1, 3)]
    act_part, proj_part, last = lax.optimization_barrier((act_part, proj_part, grads[2]))
    grads = (grads[0], near[0], shift(last, unit_groups, 2), near[1])
    proj_part = lax.all_to_all(proj_part, "z", 0, 0, tiled=True)
    grad_proj = pl.pallas_call(
        sum_kernel,
        out_shape=whole((64, 64), F32),
        in_specs=[vmem],
        out_specs=vmem,
        compiler_params=room,
        cost_estimate=cost(100000, 200000),
        name="sum_planes",
    )(proj_part)

    conv_cot, head = pl.pallas_call(
        head_kernel,
        out_shape=(whole((64, tokens), F32), whole((64, 128), F32)),
        in_specs=[vmem] * 4,
        out_specs=(vmem, vmem),
        compiler_params=room,
        cost_estimate=cost(3000000, 1200000),
        name="conv_cot",
    )(act_part, conv_t, stats, gain)
    behind = [(i + 1, i) for i in range(sp_count - 1)]
    after = lax.ppermute(head, SP, behind)
    value, gate = pl.pallas_call(
        conv_kernel,
        out_shape=(whole((64, tokens), BF), whole((64, tokens), BF)),
        in_specs=[vmem] * 5,
        out_specs=(vmem, vmem),
        scratch_shapes=[VM((64, 384), F32)],
        compiler_params=room,
        cost_estimate=cost(4000000, 400000),
        name="conv",
    )(conv_cot, after, taps_t, glu_gate.T, glu_value.T)

    grad_gate, grad_up, grad_down = pl.pallas_call(
        merge_kernel,
        out_shape=(whole((64, 2048), F32),) * 3,
        in_specs=[smem] + [vmem] * SIDE,
        out_specs=(vmem,) * 3,
        compiler_params=room,
        cost_estimate=cost(1000000, 2400000),
        name="merge_grads",
    )(at, *grads)
    return (
        grad_gate[None],
        grad_up[None],
        grad_down[None],
        grad_proj,
        value.T,
        gate.T,
    )


def solution(mesh):
    split = Mesh(mesh.devices.reshape(16, 2, SIDE, SIDE), ("z", "c", "y", "x"))
    placed = (
        P(SP, TP),
        P(SP, TP),
        P(SP, None),
        P(SP, None),
        P(SP, TP, None),
        P(SP, TP, None),
        P(SP, TP, None),
        P(SP, TP),
        P(SP, TP),
        P(SP, TP),
        P(None, TP),
        P(TP),
        P(TP, None),
    )
    return jax.shard_map(
        body,
        mesh=split,
        in_specs=placed,
        out_specs=(
            P(SP, TP, None),
            P(SP, TP, None),
            P(SP, TP, None),
            P(SP, TP),
            P(SP, TP),
            P(SP, TP),
        ),
        check_vma=False,
    )
```

```python
import jax
import jax.numpy as jnp
import numpy as np
from jax import lax
from jax.experimental import pallas as pl
from jax.experimental.pallas import tpu as pltpu
from jax.sharding import Mesh
from jax.sharding import PartitionSpec as P

NORM_EPS = 0.25
SP = ("z", "c")
TP = ("y", "x")
PLANE = ("c", "y", "x")
SIDE = 4
SLOT = 32
ROOM = 12 << 20
STEP = 512
BF = jnp.bfloat16
F32 = jnp.float32
VM = pltpu.VMEM

NT = (((1,), (1,)), ((), ()))
TN = (((0,), (0,)), ((), ()))
NN = (((1,), (0,)), ((), ()))


def place(core, row, col):
    return core * SIDE * SIDE + row * SIDE + col


def plane_groups():
    r = range(SIDE)
    down = [[[place(k, y, x) for y in r] for x in r] for k in (0, 1)]
    across = [[[place(k, y, x) for x in r] for y in r] for k in (0, 1)]
    return down[0] + across[1], across[0] + down[1]


def step_tables():
    features, units = plane_groups()
    of_features = {p: g for g in features for p in g}
    table = np.zeros((2 * SIDE * SIDE, 64), np.int32)
    for group in units:
        for me, p in enumerate(group):
            table[p, 0] = me
            table[p, 1] = of_features[p].index(p)
            table[p, 2] = p // (SIDE * SIDE)
            for k in range(SIDE):
                ahead = of_features[group[(me + k) % SIDE]]
                back = of_features[group[(me - k) % SIDE]]
                for a in range(SIDE):
                    table[p, 16 + k * SIDE + a] = ahead[a] % (SIDE * SIDE)
                    table[p, 32 + k * SIDE + a] = back[a] % (SIDE * SIDE)
    of_units = {p: g for g in units for p in g}
    for p in range(2 * SIDE * SIDE):
        group = of_features[p]
        for j in range(SIDE):
            source = group[(group.index(p) - j) % SIDE]
            their = of_units[source]
            for k in range(SIDE):
                first = their[(their.index(source) - k) % SIDE]
                table[p, 48 + j * SIDE + k] = first % (SIDE * SIDE)
    return table


def steps_ahead(groups, k):
    return [(g[i], g[(i + k) % SIDE]) for g in groups for i in range(SIDE)]


def shift(part, groups, k):
    return lax.ppermute(part, PLANE, steps_ahead(groups, k))


def pass_on(parts, groups):
    return (parts[0],) + tuple(shift(parts[k], groups, k) for k in range(1, SIDE))


def mm(a, b, dims):
    return lax.dot_general(a, b, dims, preferred_element_type=F32)


def exchange(v, groups):
    return lax.all_to_all(v, PLANE, 0, 0, axis_index_groups=groups, tiled=True)


def cost(flops, nbytes):
    return pl.CostEstimate(flops=flops, bytes_accessed=nbytes, transcendentals=0)


def route_kernel(rt_ref, w_ref, x_ref, c_ref, s_ref, t_ref):
    tokens = rt_ref.shape[1]
    experts = s_ref.shape[0] // SLOT
    first, second = rt_ref[0:1, :], rt_ref[1:2, :]
    ids = lax.broadcasted_iota(jnp.int32, (experts, tokens), 0)
    o0, o1 = ids == first, ids == second
    both = jnp.where(o0 | o1, 1.0, 0.0).astype(BF)
    before = lax.broadcasted_iota(jnp.int32, (tokens, tokens), 0) < lax.broadcasted_iota(
        jnp.int32, (tokens, tokens), 1
    )
    earlier = mm(both, jnp.where(before, 1.0, 0.0).astype(BF), NN)
    rank0 = jnp.sum(jnp.where(o0, earlier, 0.0), axis=0, keepdims=True)
    rank1 = jnp.sum(jnp.where(o1, earlier, 0.0), axis=0, keepdims=True)
    t0 = first * SLOT + rank0.astype(jnp.int32)
    t1 = second * SLOT + rank1.astype(jnp.int32)
    t_ref[0:1, :] = t0
    t_ref[1:2, :] = t1
    w0, w1 = w_ref[0:1, :], w_ref[1:2, :]
    x, c = x_ref[...], c_ref[...]
    size = 128
    for k in range(s_ref.shape[0] // size):
        slots = lax.broadcasted_iota(jnp.int32, (size, tokens), 0) + k * size
        m0, m1 = slots == t0, slots == t1
        pick = jnp.where(m0 | m1, 1.0, 0.0).astype(BF)
        weight = jnp.sum(
            jnp.where(m0, w0, 0.0) + jnp.where(m1, w1, 0.0), axis=1, keepdims=True
        )
        rows = pl.ds(k * size, size)
        s_ref[rows, 0:128] = mm(pick, x, NN).astype(BF)
        s_ref[rows, 128:256] = (weight * mm(pick, c, NN)).astype(BF)


def pick_kernel(t_ref, p_ref):
    slots = lax.broadcasted_iota(jnp.int32, p_ref.shape, 0)
    held = (slots == t_ref[0:1, :]) | (slots == t_ref[1:2, :])
    p_ref[...] = jnp.where(held, 1.0, 0.0).astype(BF)


def split_kernel(at_ref, g_ref, u_ref, d_ref, p_ref, c_ref, *outs):
    for k, out in enumerate(outs):
        for a in range(SIDE):
            at = at_ref[16 + k * SIDE + a]
            cols = pl.ds(pl.multiple_of(at * 128, 128), 128)
            for q, ref in enumerate((g_ref, u_ref, d_ref, p_ref)):
                out[q * 64 : q * 64 + 64, a * 128 : a * 128 + 128] = ref[:, cols]
        out[256:320, :] = c_ref[...]


def relay_kernel(at_ref, r0, r1, r2, r3, *outs):
    for j, out in enumerate(outs):
        a = lax.rem(at_ref[1] + j, SIDE)
        cols = pl.ds(pl.multiple_of(a * 128, 128), 128)
        for k, r_ref in enumerate((r0, r1, r2, r3)):
            out[k * 64 : k * 64 + 64, 0:128] = r_ref[192:256, cols]
            out[k * 64 : k * 64 + 64, 128:512] = r_ref[256:320, 128:512]


def merge_kernel(at_ref, s0, s1, s2, s3, g_ref, u_ref, d_ref):
    for k, s_ref in enumerate((s0, s1, s2, s3)):
        for a in range(SIDE):
            at = at_ref[32 + k * SIDE + a]
            cols = pl.ds(pl.multiple_of(at * 128, 128), 128)
            for q, ref in enumerate((g_ref, u_ref, d_ref)):
                ref[:, cols] = s_ref[
                    q * 64 : q * 64 + 64, a * 128 : a * 128 + 128
                ].astype(F32)


def behind_of(at_ref, k):
    return lax.rem(at_ref[0] + (SIDE - k), SIDE)


def ahead_of(at_ref, k):
    return lax.rem(at_ref[0] + k, SIDE)


def pre_kernel(at_ref, a_ref, w0, w1, w2, w3, o_ref):
    ws = (w0, w1, w2, w3)

    @pl.loop(0, a_ref.shape[1] // STEP)
    def _(i):
        rows = pl.ds(pl.multiple_of(i * STEP, STEP), STEP)
        x = jnp.concatenate([a_ref[a, rows, 0:128] for a in range(SIDE)], axis=1)
        c = jnp.concatenate([a_ref[a, rows, 128:256] for a in range(SIDE)], axis=1)
        pairs = mm(jnp.concatenate([w[0:128, :] for w in ws], axis=0), x, NT)
        downs = mm(jnp.concatenate([w[128:192, :] for w in ws], axis=0), c, NT)
        for k in range(SIDE):
            b = behind_of(at_ref, k)
            o_ref[b, 0:128, rows] = pairs[k * 128 : k * 128 + 128].astype(BF)
            o_ref[b, 128:192, rows] = downs[k * 64 : k * 64 + 64].astype(BF)


def gate_kernel(p_ref, o_ref):
    total = p_ref[0].astype(F32)
    for b in range(1, SIDE):
        total = total + p_ref[b].astype(F32)
    gate, up, cot = total[0:64], total[64:128], total[128:192]
    s = jax.nn.sigmoid(gate)
    act = gate * s
    hidden = (act * up).astype(BF)
    up_cot = (cot * act).astype(BF)
    gate_cot = (cot * up * s * (1.0 + gate * (1.0 - s))).astype(BF)
    for b in range(SIDE):
        o_ref[b, 0:64, :] = gate_cot
        o_ref[b, 64:128, :] = up_cot
        o_ref[b, 128:192, :] = hidden


def partial_kernel(at_ref, h_ref, w0, w1, w2, w3, o_ref):
    ws = (w0, w1, w2, w3)

    @pl.loop(0, h_ref.shape[2] // STEP)
    def _(i):
        rows = pl.ds(pl.multiple_of(i * STEP, STEP), STEP)
        h = jnp.concatenate(
            [h_ref[behind_of(at_ref, k), 0:128, rows] for k in range(SIDE)], axis=0
        )
        w = jnp.concatenate([w_ref[0:128, :] for w_ref in ws], axis=0)
        total = mm(h, w, TN)
        for a in range(SIDE):
            o_ref[a, rows, :] = total[:, a * 128 : a * 128 + 128].astype(BF)


def grads_kernel(at_ref, h_ref, a_ref, *outs):
    x = jnp.concatenate([a_ref[0, :, 0:128], a_ref[1, :, 0:128]], axis=1)
    c = jnp.concatenate([a_ref[0, :, 128:256], a_ref[1, :, 128:256]], axis=1)
    order = [ahead_of(at_ref, k) for k in range(SIDE)]
    pairs = mm(jnp.concatenate([h_ref[b, 0:128, :] for b in order], axis=0), x, NN)
    downs = mm(jnp.concatenate([h_ref[b, 128:192, :] for b in order], axis=0), c, NN)
    for k, out in enumerate(outs):
        out[0:128, :] = pairs[k * 128 : k * 128 + 128].astype(BF)
        out[128:192, :] = downs[k * 64 : k * 64 + 64].astype(BF)


def total_kernel(
    at_ref, p_ref, r_ref, c_ref, q0, q1, q2, q3, mine_ref, other_ref, total_ref, stats_ref
):
    qs = (q0, q1, q2, q3)
    moe = mm(p_ref[...], r_ref[...], TN)
    total = (c_ref[...].astype(F32) + moe).astype(BF)
    tokens = total.shape[0]
    total_ref[0:tokens, :] = total
    total_ref[tokens:, :] = jnp.zeros((total_ref.shape[0] - tokens, 128), BF)
    size = q0.shape[0]
    channels = SIDE * size
    mean = jnp.zeros((1, tokens), F32)
    for q in qs:
        conv = q[:, 128 : 128 + tokens].astype(F32)
        mean = mean + jnp.sum(conv, axis=0, keepdims=True)
    mean = mean / channels
    var = jnp.zeros((1, tokens), F32)
    for q in qs:
        off = q[:, 128 : 128 + tokens].astype(F32) - mean
        var = var + jnp.sum(off * off, axis=0, keepdims=True)
    inv = lax.rsqrt(var / channels + NORM_EPS)
    stats_ref[0:1, :] = mean
    stats_ref[1:2, :] = inv
    own = jnp.full((64, 128), at_ref[2], jnp.int32) == 0
    for j, q in enumerate(qs):
        normed = (q[:, 128 : 128 + tokens].astype(F32) - mean) * inv
        linear = normed * gain_of(q)
        act = (linear * jax.nn.sigmoid(linear)).astype(BF)
        grad = mm(act, total, NN)
        turned = pltpu.roll(grad, 64, 1)
        for k in range(SIDE):
            b = at_ref[48 + j * SIDE + k]
            rows = slice(k * 64, k * 64 + 64)
            mine_ref[b] = jnp.where(own, turned[rows], grad[rows]).astype(BF)
            other_ref[b] = jnp.where(own, grad[rows], turned[rows]).astype(BF)


def gain_of(q):
    lane = lax.broadcasted_iota(jnp.int32, (q.shape[0], 128), 1)
    pieces = jnp.where((lane >= 64) & (lane < 67), q[:, 384:512].astype(F32), 0.0)
    return jnp.sum(pieces, axis=1, keepdims=True)


def cot_kernel(at_ref, total_ref, stats_ref, q0, q1, q2, q3, o_ref):
    wide = total_ref.shape[0]
    tokens = stats_ref.shape[1]
    total = total_ref[...]
    mean, inv = stats_ref[0:1, :], stats_ref[1:2, :]
    first = jnp.zeros((1, tokens), F32)
    second = jnp.zeros((1, tokens), F32)
    for j, q in enumerate((q0, q1, q2, q3)):
        normed = (q[:, 128 : 128 + tokens].astype(F32) - mean) * inv
        gain = gain_of(q)
        linear = normed * gain
        s = jax.nn.sigmoid(linear)
        cot = mm(q[:, 0:128], total, NT)
        sloped = cot[:, 0:tokens] * (s * (1.0 + linear * (1.0 - s)) * gain)
        first = first + jnp.sum(sloped, axis=0, keepdims=True)
        second = second + jnp.sum(sloped * normed, axis=0, keepdims=True)
        for k in range(SIDE):
            o_ref[at_ref[48 + j * SIDE + k], 0:64, :] = cot[k * 64 : k * 64 + 64].astype(BF)
    row = lax.broadcasted_iota(jnp.int32, (8, tokens), 0)
    sums = jnp.zeros((8, tokens), F32)
    for i, v in enumerate((first, second)):
        head = v.astype(BF).astype(F32)
        sums = jnp.where(row == 2 * i, head, jnp.where(row == 2 * i + 1, v - head, sums))
    for b in range(o_ref.shape[0]):
        o_ref[b, 64:72, 0:tokens] = sums.astype(BF)
        o_ref[b, 64:72, tokens:wide] = jnp.zeros((8, wide - tokens), BF)


def join_kernel(a_ref, mine_ref, other_ref, o_ref):
    low = lax.broadcasted_iota(jnp.int32, (64, 128), 1) < 64
    for b in range(o_ref.shape[0]):
        piece = mine_ref[b].astype(F32) + other_ref[b].astype(F32)
        o_ref[b, :, 0:256] = a_ref[b, :, 0:256]
        o_ref[b, 0:64, 256:384] = jnp.where(
            low, a_ref[b, 0:64, 256:384].astype(F32), piece
        ).astype(BF)
        o_ref[b, 64:72, 256:384] = a_ref[b, 64:72, 256:384]


def part_kernel(r_ref, o_ref):
    low = lax.broadcasted_iota(jnp.int32, (32, 128), 1) < 64
    for b in range(o_ref.shape[0]):
        upper = pltpu.roll(r_ref[b, 0:32, 256:384].astype(F32), 64, 1)
        lower = r_ref[b, 32:64, 256:384].astype(F32)
        o_ref[b] = jnp.where(low, upper, lower).astype(BF)


def head_kernel(r_ref, conv_ref, stats_ref, gain_ref, o_ref, h_ref):
    tokens = conv_ref.shape[1]
    total = r_ref[0, :, 0:tokens].astype(F32)
    for b in range(1, r_ref.shape[0]):
        total = total + r_ref[b, :, 0:tokens].astype(F32)
    channels = 16 * conv_ref.shape[0]
    first = (total[64:65] + total[65:66]) / channels
    second = (total[66:67] + total[67:68]) / channels
    inv = stats_ref[1:2, :]
    normed = (conv_ref[...].astype(F32) - stats_ref[0:1, :]) * inv
    gain = gain_ref[...]
    linear = normed * gain
    s = jax.nn.sigmoid(linear)
    cot = total[0:64] * s * (1.0 + linear * (1.0 - s)) * gain
    cot = inv * (cot - first - normed * second)
    o_ref[...] = cot
    h_ref[...] = cot[:, 0:128]


def sum_kernel(a_ref, o_ref):
    total = a_ref[0].astype(F32)
    for b in range(1, a_ref.shape[0]):
        total = total + a_ref[b].astype(F32)
    turned = pltpu.roll(total, 64, 1)
    block = jnp.concatenate([total, turned], axis=0)
    o_ref[...] = block.T[0:64, :]


def sum_side_kernel(p_ref, o_ref):
    total = p_ref[0].astype(F32)
    for a in range(1, SIDE):
        total = total + p_ref[a].astype(F32)
    o_ref[...] = total.astype(BF)


def conv_kernel(cot_ref, next_ref, taps_ref, gate_ref, value_ref, v_ref, g_ref, buf):
    rows, tokens = cot_ref.shape
    wide = buf.shape[1]
    reach = taps_ref.shape[1] - 1
    buf[:, 0:128] = next_ref[...]
    buf[:, 128:wide] = jnp.zeros((rows, wide - 128), F32)
    after = pltpu.roll(buf[...], tokens, 1)
    buf[:, 0:tokens] = cot_ref[...]
    lane = lax.broadcasted_iota(jnp.int32, (rows, wide), 1)
    whole = jnp.where(lane < tokens, buf[...], after)
    taps = taps_ref[...]
    total = whole * taps[:, reach : reach + 1]
    for s in range(1, reach + 1):
        total = total + pltpu.roll(whole, wide - s, 1) * taps[:, reach - s : reach - s + 1]
    cot = total[:, 0:tokens]
    s = jax.nn.sigmoid(gate_ref[...].astype(F32))
    v_ref[...] = (cot * s).astype(BF)
    g_ref[...] = (cot * value_ref[...].astype(F32) * s * (1.0 - s)).astype(BF)


def whole(shape, dtype):
    return jax.ShapeDtypeStruct(shape, dtype)


def body(
    moe_input,
    out_cotangent,
    routes,
    route_weight,
    gate_weight,
    up_weight,
    down_weight,
    glu_value,
    glu_gate,
    conv_result,
    conv_taps,
    norm_gain,
    proj_weight,
):
    sp_count = lax.axis_size(SP)
    tp_count = lax.axis_size(TP)
    tokens = moe_input.shape[0]
    slots = sp_count * SLOT
    feature_groups, unit_groups = plane_groups()
    smem = pl.BlockSpec(memory_space=pltpu.SMEM)
    vmem = pl.BlockSpec(memory_space=VM)
    room = pltpu.CompilerParams(vmem_limit_bytes=ROOM)

    sent, target = pl.pallas_call(
        route_kernel,
        out_shape=(whole((slots, 256), BF), whole((2, tokens), jnp.int32)),
        in_specs=[vmem] * 4,
        out_specs=(vmem, vmem),
        cost_estimate=cost(400000000, 2000000),
        name="route",
    )(routes.T, route_weight.T, moe_input, out_cotangent)
    sent, target, table, gate_weight, conv_result, norm_gain = lax.optimization_barrier(
        (sent, target, jnp.asarray(step_tables()), gate_weight, conv_result, norm_gain)
    )
    at = table[lax.axis_index(PLANE)]
    pick = pl.pallas_call(
        pick_kernel,
        out_shape=whole((slots, tokens), BF),
        in_specs=[vmem],
        out_specs=vmem,
        compiler_params=room,
        cost_estimate=cost(1000000, 700000),
        name="pick",
    )(target)
    conv_t = conv_result.T
    gain = norm_gain.reshape(-1, 1)
    high = lax.reduce_precision(gain, 8, 7)
    middle = lax.reduce_precision(gain - high, 8, 7)
    pieces = jnp.concatenate([high, middle, gain - high - middle], axis=1).astype(BF)
    channel_part = jnp.concatenate(
        [jnp.zeros((64, 128), BF), conv_t, pieces, jnp.zeros((64, 61), BF)], axis=1
    )
    split = pl.pallas_call(
        split_kernel,
        out_shape=(whole((320, 512), BF),) * SIDE,
        in_specs=[smem] + [vmem] * 5,
        out_specs=(vmem,) * SIDE,
        compiler_params=room,
        cost_estimate=cost(1000000, 2600000),
        name="split_weights",
    )(at, gate_weight[0], up_weight[0], down_weight[0], proj_weight, channel_part)
    weights = pass_on(split, unit_groups)
    relay = pl.pallas_call(
        relay_kernel,
        out_shape=(whole((256, 512), BF),) * SIDE,
        in_specs=[smem] + [vmem] * SIDE,
        out_specs=(vmem,) * SIDE,
        compiler_params=room,
        cost_estimate=cost(1000000, 2000000),
        name="relay",
    )(at, *weights)
    got = lax.all_to_all(sent.reshape(sp_count, SLOT, 256), SP, 0, 0, tiled=True)
    got = got.reshape(slots, 256)
    got, weights, relay = lax.optimization_barrier((got, weights, relay))
    taps_t = conv_taps.T

    rows = exchange(jnp.broadcast_to(got[None], (SIDE, slots, 256)), feature_groups)
    step = 256
    pre = pl.pallas_call(
        pre_kernel,
        out_shape=whole((SIDE, 192, slots), BF),
        in_specs=[smem] + [vmem] * (1 + SIDE),
        out_specs=vmem,
        compiler_params=room,
        cost_estimate=cost(800000000, 4400000),
        name="pre",
    )(at, rows, *weights)
    pre = exchange(pre, unit_groups)
    hidden = pl.pallas_call(
        gate_kernel,
        grid=(slots // step,),
        out_shape=whole((SIDE, 192, slots), BF),
        in_specs=[pl.BlockSpec((SIDE, 192, step), lambda i: (0, 0, i))],
        out_specs=pl.BlockSpec((SIDE, 192, step), lambda i: (0, 0, i)),
        compiler_params=room,
        cost_estimate=cost(3000000, 3200000),
        name="gates",
    )(pre)
    hidden = exchange(hidden, unit_groups)
    part = pl.pallas_call(
        partial_kernel,
        out_shape=whole((SIDE, slots, 128), BF),
        in_specs=[smem] + [vmem] * (1 + SIDE),
        out_specs=vmem,
        compiler_params=room,
        cost_estimate=cost(540000000, 3400000),
        name="partial",
    )(at, hidden, *weights)
    part = exchange(part, feature_groups)
    back = pl.pallas_call(
        sum_side_kernel,
        out_shape=whole((slots, 128), BF),
        in_specs=[vmem],
        out_specs=vmem,
        compiler_params=room,
        cost_estimate=cost(1000000, 1300000),
        name="sum_side",
    )(part).reshape(sp_count, SLOT, 128)
    back, relay = lax.optimization_barrier((back, relay))
    relay = pass_on(relay, feature_groups)
    returned = lax.all_to_all(back, SP, 0, 0, tiled=True).reshape(slots, 128)

    grads = pl.pallas_call(
        grads_kernel,
        grid=(SIDE // 2,),
        out_shape=(whole((192, 512), BF),) * SIDE,
        in_specs=[
            smem,
            pl.BlockSpec((SIDE, 192, slots), lambda i: (0, 0, 0)),
            pl.BlockSpec((2, slots, 256), lambda i: (i, 0, 0)),
        ],
        out_specs=(pl.BlockSpec((192, 256), lambda i: (0, i)),) * SIDE,
        compiler_params=room,
        cost_estimate=cost(800000000, 4400000),
        name="grads",
    )(at, hidden, rows)
    returned, grads = lax.optimization_barrier((returned, grads))

    wide = 384
    mine, other, total_cot, stats = pl.pallas_call(
        total_kernel,
        out_shape=(
            whole((tp_count, 64, 128), BF),
            whole((tp_count, 64, 128), BF),
            whole((wide, 128), BF),
            whole((2, tokens), F32),
        ),
        in_specs=[smem] + [vmem] * 7,
        out_specs=(vmem,) * 4,
        compiler_params=room,
        cost_estimate=cost(170000000, 2500000),
        name="total_cot",
    )(at, pick, returned, out_cotangent, *relay)
    other = lax.ppermute(other, "c", [(0, 1), (1, 0)])
    act_part = pl.pallas_call(
        cot_kernel,
        out_shape=whole((tp_count, 72, wide), BF),
        in_specs=[smem] + [vmem] * 6,
        out_specs=vmem,
        compiler_params=room,
        cost_estimate=cost(100000000, 2500000),
        name="act_cot",
    )(at, total_cot, stats, *relay)
    act_part = pl.pallas_call(
        join_kernel,
        grid=(2,),
        out_shape=whole((tp_count, 72, wide), BF),
        in_specs=[
            pl.BlockSpec((8, 72, wide), lambda i: (i, 0, 0)),
            pl.BlockSpec((8, 64, 128), lambda i: (i, 0, 0)),
            pl.BlockSpec((8, 64, 128), lambda i: (i, 0, 0)),
        ],
        out_specs=pl.BlockSpec((8, 72, wide), lambda i: (i, 0, 0)),
        compiler_params=room,
        cost_estimate=cost(100000, 2200000),
        name="join_cores",
    )(act_part, mine, other)
    act_part, grads = lax.optimization_barrier((act_part, grads))
    act_part = lax.all_to_all(act_part, TP, 0, 0, tiled=True)
    proj_part = pl.pallas_call(
        part_kernel,
        out_shape=whole((tp_count, 32, 128), BF),
        in_specs=[vmem],
        out_specs=vmem,
        compiler_params=room,
        cost_estimate=cost(100000, 400000),
        name="proj_part",
    )(act_part)
    near = [shift(grads[k], unit_groups, k) for k in (1, 3)]
    act_part, proj_part, last = lax.optimization_barrier((act_part, proj_part, grads[2]))
    grads = (grads[0], near[0], shift(last, unit_groups, 2), near[1])
    proj_part = lax.all_to_all(proj_part, "z", 0, 0, tiled=True)
    grad_proj = pl.pallas_call(
        sum_kernel,
        out_shape=whole((64, 64), F32),
        in_specs=[vmem],
        out_specs=vmem,
        compiler_params=room,
        cost_estimate=cost(100000, 200000),
        name="sum_planes",
    )(proj_part)

    conv_cot, head = pl.pallas_call(
        head_kernel,
        out_shape=(whole((64, tokens), F32), whole((64, 128), F32)),
        in_specs=[vmem] * 4,
        out_specs=(vmem, vmem),
        compiler_params=room,
        cost_estimate=cost(3000000, 1200000),
        name="conv_cot",
    )(act_part, conv_t, stats, gain)
    behind = [(i + 1, i) for i in range(sp_count - 1)]
    after = lax.ppermute(head, SP, behind)
    value, gate = pl.pallas_call(
        conv_kernel,
        out_shape=(whole((64, tokens), BF), whole((64, tokens), BF)),
        in_specs=[vmem] * 5,
        out_specs=(vmem, vmem),
        scratch_shapes=[VM((64, 384), F32)],
        compiler_params=room,
        cost_estimate=cost(4000000, 400000),
        name="conv",
    )(conv_cot, after, taps_t, glu_gate.T, glu_value.T)

    grad_gate, grad_up, grad_down = pl.pallas_call(
        merge_kernel,
        out_shape=(whole((64, 2048), F32),) * 3,
        in_specs=[smem] + [vmem] * SIDE,
        out_specs=(vmem,) * 3,
        compiler_params=room,
        cost_estimate=cost(1000000, 2400000),
        name="merge_grads",
    )(at, *grads)
    return (
        grad_gate[None],
        grad_up[None],
        grad_down[None],
        grad_proj,
        value.T,
        gate.T,
    )


def solution(mesh):
    split = Mesh(mesh.devices.reshape(16, 2, SIDE, SIDE), ("z", "c", "y", "x"))
    placed = (
        P(SP, TP),
        P(SP, TP),
        P(SP, None),
        P(SP, None),
        P(SP, TP, None),
        P(SP, TP, None),
        P(SP, TP, None),
        P(SP, TP),
        P(SP, TP),
        P(SP, TP),
        P(None, TP),
        P(TP),
        P(TP, None),
    )
    return jax.shard_map(
        body,
        mesh=split,
        in_specs=placed,
        out_specs=(
            P(SP, TP, None),
            P(SP, TP, None),
            P(SP, TP, None),
            P(SP, TP),
            P(SP, TP),
            P(SP, TP),
        ),
        check_vma=False,
    )
```
